768 devices in a mesh: fs: 96 (over z, y), tp: 8 (over x, core).
Axes of the slice: x: 4, y: 8, z: 12, core: 2. Of those that a mesh axis runs over, the one named last changes fastest.
Arguments:
- saved_inputs: bfloat16 [49152, 3072], P('fs'), may hold values from -6 to 6
- query_cotangent: bfloat16 [49152, 3072], P('fs', 'tp'), may hold values from -0.21875 to 0.21875
- attn_outputs: bfloat16 [49152, 3072], P('fs', 'tp'), may hold values from -6 to 6
- out_cotangent: bfloat16 [49152, 3072], P('fs'), may hold values from -0.21875 to 0.21875
- left_factor: bfloat16 [3072, 384], P('fs', 'tp'), may hold values from -0.109375 to 0.109375
- right_factor: bfloat16 [3072, 384], P('fs', 'tp'), may hold values from -0.109375 to 0.109375
- query_master: float32 [3072, 3072], P('fs', 'tp'), may hold values from -0.109375 to 0.109375
- out_master: float32 [3072, 3072], P('tp', 'fs'), may hold values from -0.109375 to 0.109375
- first_moment: float32 [2, 384, 3072], P(None, 'fs', 'tp'), may hold values from -14 to 14
- second_moment: float32 [2, 384, 3072], P(None, 'fs', 'tp'), may hold values from 0.3 to 3
Outputs:
- query_new: float32 [3072, 3072], P('fs', 'tp')
- out_new: float32 [3072, 3072], P('tp', 'fs')
- query_copy: bfloat16 [3072, 3072], P(None, 'tp')
- out_copy: bfloat16 [3072, 3072], P('tp')
- first_new: float32 [2, 384, 3072], P(None, 'fs', 'tp')
- second_new: float32 [2, 384, 3072], P(None, 'fs', 'tp')
The draws below stay inside these ranges and needn't reach their ends.
All inputs are finite; a program needn't handle non-finite values.
Results may differ from the reference program's by a relative error of at most 0.0025.
Values may be sent and summed in bfloat16 or wider, within the bound.
No kernel may reach another device: no remote copies, remote signals or barrier semaphores. Data moves between devices by JAX's collectives and lax.ppermute only.
A program may use at most 64 MiB of HBM per device.

```python
import math
import jax
import jax.numpy as jnp
from jax import lax

D = 3072
RANK = 384
QW = 3072
TOKENS = 49152


def draw_first_moment(key, part):
    row_pos = jnp.arange(RANK, dtype=jnp.float32) / RANK
    col_pos = jnp.arange(QW, dtype=jnp.float32) / QW
    base = jnp.clip(jax.random.normal(key, (2, RANK, QW), jnp.float32), -4.0, 4.0)
    growth = 3.0
    spread = growth ** row_pos[:, None] * growth ** col_pos[None, :] / growth
    return (base * spread[None]).astype(jnp.float32)


def shard_levels(own_key, extent, shards, least, high):
    gain = 1.0
    for position, blocks in shards:
        heights = jax.random.uniform(jax.random.fold_in(jax.random.fold_in(own_key, 6), position), (blocks,), jnp.float32, least / len(shards), high / len(shards))
        gain = gain * jnp.repeat(jnp.exp(heights), extent[position] // blocks).reshape((-1,) + (1,) * (len(extent) - 1 - position))
    return gain


def normal_values(own_key, dims, scale, reach, shards=(), held_as=jnp.bfloat16):
    drawn = jax.random.normal(own_key, dims, jnp.float32) * scale
    if len(shards) > 0:
        drawn = shard_levels(own_key, dims, shards, -0.22, 0.18) * drawn
    return jnp.clip(drawn, min=-reach, max=reach).astype(held_as)


def setup_inputs(seed: int = 0) -> dict:
    key_list = jax.random.split(jax.random.key(seed), 11)
    return {
        "saved_inputs": normal_values(key_list[0], (TOKENS, D), 1.0, 6.0, ((0, 96),)),
        "query_cotangent": normal_values(key_list[1], (TOKENS, QW), (8.0 / TOKENS ** 0.5), 0.21875, ((0, 96), (1, 8))),
        "attn_outputs": normal_values(key_list[2], (TOKENS, QW), 1.0, 6.0, ((0, 96), (1, 8))),
        "out_cotangent": normal_values(key_list[3], (TOKENS, D), (8.0 / TOKENS ** 0.5), 0.21875, ((0, 96),)),
        "left_factor": normal_values(key_list[4], (D, RANK), D ** -0.5, 0.109375, ((0, 96), (1, 8))),
        "right_factor": normal_values(key_list[5], (D, RANK), D ** -0.5, 0.109375, ((0, 96), (1, 8))),
        "query_master": normal_values(key_list[6], (D, QW), D ** -0.5, 0.109375, ((0, 96), (1, 8)), jnp.float32),
        "out_master": normal_values(key_list[7], (QW, D), QW ** -0.5, 0.109375, ((0, 8), (1, 96)), jnp.float32),
        "first_moment": draw_first_moment(jax.random.fold_in(key_list[10], 71), 0),
        "second_moment": jnp.clip(jnp.exp(math.log(3.0) - 2.3025851 * jax.random.uniform(key_list[9], (2, RANK, QW), jnp.float32) ** shard_levels(key_list[9], (2, RANK, QW), ((1, 96), (2, 8)), -0.2, 0.2)), 0.3, 3.0),
    }


def reference(saved_inputs, query_cotangent, attn_outputs, out_cotangent, left_factor, right_factor, query_master, out_master, first_moment, second_moment):
    left_proj = jnp.dot(saved_inputs, left_factor, preferred_element_type=jnp.float32).astype(jnp.bfloat16)
    right_proj = jnp.dot(out_cotangent, right_factor, preferred_element_type=jnp.float32).astype(jnp.bfloat16)
    grad_query = jnp.dot(left_proj.T, query_cotangent, preferred_element_type=jnp.float32)
    grad_output = jnp.dot(right_proj.T, attn_outputs, preferred_element_type=jnp.float32)
    grads = jnp.stack([grad_query, grad_output], axis=0)
    first_new = 0.9 * first_moment + 0.1 * grads
    second_new = 0.99 * second_moment + 0.01 * grads * grads
    direction = first_new / (jnp.sqrt(second_new) + 1e-08)
    scale = lax.rsqrt(lax.optimization_barrier(jnp.mean(direction * direction, axis=(1, 2))) + 1e-06)
    direction_low = direction.astype(jnp.bfloat16)
    step_query = scale[0] * jnp.dot(left_factor, direction_low[0], preferred_element_type=jnp.float32)
    step_output = scale[1] * jnp.dot(direction_low[1].T, right_factor.T, preferred_element_type=jnp.float32)
    query_new = query_master - 0.01 * step_query
    out_new = out_master - 0.01 * step_output
    return (query_new, out_new, query_new.astype(jnp.bfloat16), out_new.astype(jnp.bfloat16), first_new, second_new)
```

```python
import functools

import jax
import jax.numpy as jnp
from jax import lax
from jax.experimental import pallas as pl
from jax.experimental.pallas import tpu as pltpu
from jax.sharding import PartitionSpec as P


bf16 = jnp.bfloat16
f32 = jnp.float32
VMEM = pl.BlockSpec(memory_space=pltpu.VMEM)
SMEM = pl.BlockSpec(memory_space=pltpu.SMEM)


def cost(flops, nbytes):
    return pl.CostEstimate(flops=flops, bytes_accessed=nbytes, transcendentals=0)


def to_all(value, axis):
    n = lax.axis_size(axis)
    return lax.all_to_all(jnp.broadcast_to(value[None], (n, *value.shape)), axis, 0, 0)


def grad_kernel(proj, query_cotangent, attn_outputs, out):
    tokens = query_cotangent.shape[0]
    cols = query_cotangent.shape[1]
    first = jnp.dot(proj[:, :tokens], query_cotangent[...], preferred_element_type=f32)
    second = jnp.dot(proj[:, tokens:], attn_outputs[...], preferred_element_type=f32)
    first = first.reshape(-1, 8, cols)
    second = second.reshape(-1, 8, cols)
    both = jnp.concatenate([first[:, :4], second[:, :4], first[:, 4:], second[:, 4:]], axis=1)
    out[...] = both.astype(bf16)


def moment_kernel(pieces, first, second, first_new, second_new, low):
    rows = first.shape[1]
    grads = jnp.sum(pieces[...].astype(f32), axis=0)
    new_first = 0.9 * jnp.concatenate([first[0], first[1]], axis=0) + 0.1 * grads
    new_second = 0.99 * jnp.concatenate([second[0], second[1]], axis=0) + 0.01 * grads * grads
    direction = new_first / (jnp.sqrt(new_second) + 1e-08)
    first_new[0] = new_first[:rows]
    first_new[1] = new_first[rows:]
    second_new[0] = new_second[:rows]
    second_new[1] = new_second[rows:]
    squares = direction * direction
    lane = lax.broadcasted_iota(jnp.int32, (rows, 128), 1)
    sums = jnp.zeros((rows, 128), f32)
    for k in range(2):
        rest = jnp.sum(squares[k * rows : (k + 1) * rows], axis=(0, 1), keepdims=True)
        for part in range(3):
            rounded = rest.astype(bf16).astype(f32)
            sums = jnp.where(lane == 3 * k + part, rounded, sums)
            rest = rest - rounded
    sent = jnp.concatenate([direction[:rows], direction[rows:], sums], axis=1).astype(bf16)
    low[...] = jnp.broadcast_to(sent[None], low.shape)


def squares_kernel(low, out):
    sums = jnp.sum(low[:, :, -128:].astype(f32), axis=0)[:1]
    out[...] = jnp.broadcast_to(sums[None], out.shape)


def final_kernel(
    entries,
    place,
    low,
    squares,
    masters,
    held,
    other,
    query_copy,
    out_copy,
    query_new,
    out_new,
    direction,
    factors,
    tile,
):
    step = pl.program_id(0)
    tp, rank_cols, cols = direction.shape[1:]
    rows = low.shape[1]
    per_block = rank_cols // rows
    own = query_new.shape[0]
    span = query_copy.shape[0]

    @pl.when(step == 0)
    def _():
        for b in range(tp):
            chip, core = b % (tp // 2), b // (tp // 2)
            at = (place[1] + 2 * chip) % tp
            at = at + core * (1 - 2 * (at % 2))
            block = low[pl.ds(at * per_block, per_block)].astype(f32)
            for k in range(2):
                part = block[:, :, k * cols : (k + 1) * cols]
                part = jnp.concatenate([part[j] for j in range(per_block)], axis=0)
                direction[k, b] = part.astype(bf16)

    sums = jnp.sum(squares[...], axis=0)[:1]
    lane = lax.broadcasted_iota(jnp.int32, sums.shape, 1)
    for k, copy, new in ((0, query_copy, query_new), (1, out_copy, out_new)):
        total = jnp.sum(jnp.where(lane // 3 == k, sums, 0.0), axis=1, keepdims=True)
        scale = 0.01 * lax.rsqrt(total / entries + 1e-06)
        for c, half in enumerate((held, other)):
            for s in range(tp // 2):
                at = (c * (tp // 2) + s) * rank_cols
                factors[k, :, at : at + rank_cols] = half[s, :, k * rank_cols : (k + 1) * rank_cols]
        moved = jnp.dot(
            factors[k], direction[k].reshape(tp * rank_cols, cols), preferred_element_type=f32
        )
        kept = masters[:, k * own : (k + 1) * own].reshape(span, cols)
        fresh = kept - scale * moved
        if k == 0:
            copy[...] = fresh.astype(bf16)
        else:
            copy[...] = fresh.T.astype(bf16)

        @pl.when(step == place[0] // (span // own))
        def _():
            tile[...] = fresh
            new[...] = tile[pl.ds(pl.multiple_of(place[0] % (span // own) * own, own), own)]


def body(
    saved_inputs,
    query_cotangent,
    attn_outputs,
    out_cotangent,
    left_factor,
    right_factor,
    query_master,
    out_master,
    first_moment,
    second_moment,
):
    fs = lax.axis_size("fs")
    tp = lax.axis_size("tp")
    own, rank_cols = left_factor.shape
    rows = first_moment.shape[1]
    cols = first_moment.shape[2]
    width = fs * own
    ranks = tp * rank_cols

    masters = lax.all_gather(jnp.concatenate([query_master, out_master.T], axis=0), "fs")

    lanes = jnp.zeros((own, 128 - 2 * rank_cols), bf16)
    factors = to_all(jnp.concatenate([left_factor, right_factor, lanes], axis=1), "fs")
    factors = factors.reshape(width, 128)
    turned = (((0,), (1,)), ((), ()))
    left_part = lax.dot_general(
        factors[:, :rank_cols], saved_inputs, turned, preferred_element_type=f32
    )
    right_part = lax.dot_general(
        factors[:, rank_cols : 2 * rank_cols], out_cotangent, turned, preferred_element_type=f32
    )
    proj = jnp.concatenate([left_part.astype(bf16), right_part.astype(bf16)], axis=1)
    proj = lax.all_gather(proj, "tp", axis=0, tiled=True)

    proj, mine = lax.optimization_barrier((proj, factors))
    held = [mine]
    for step in range(1, tp // 2):
        held.append(lax.ppermute(mine, "tp", [((t + 2 * step) % tp, t) for t in range(tp)]))
    held = jnp.stack(held)

    partial = pl.pallas_call(
        grad_kernel,
        out_shape=jax.ShapeDtypeStruct((fs // 2, 4 * rows, cols), bf16),
        in_specs=[VMEM] * 3,
        out_specs=VMEM,
        cost_estimate=cost(4 * ranks * saved_inputs.shape[0] * cols, 2 << 20),
    )(proj, query_cotangent, attn_outputs)
    pieces = lax.all_to_all(partial.reshape(fs, 2 * rows, cols), "fs", 0, 0)
    other = lax.ppermute(held, "tp", [(t ^ 1, t) for t in range(tp)])
    first_new, second_new, low = pl.pallas_call(
        moment_kernel,
        out_shape=(
            jax.ShapeDtypeStruct(first_moment.shape, f32),
            jax.ShapeDtypeStruct(second_moment.shape, f32),
            jax.ShapeDtypeStruct((fs, rows, 2 * cols + 128), bf16),
        ),
        in_specs=[VMEM] * 3,
        out_specs=(VMEM, VMEM, VMEM),
        cost_estimate=cost(1 << 20, 2 << 20),
    )(pieces, first_moment, second_moment)
    low = lax.all_to_all(low, "fs", 0, 0)
    squares = pl.pallas_call(
        squares_kernel,
        out_shape=jax.ShapeDtypeStruct((tp, 8, 128), f32),
        in_specs=[VMEM],
        out_specs=VMEM,
        cost_estimate=cost(1 << 16, 1 << 16),
    )(low)
    squares = lax.all_to_all(squares, "tp", 0, 0)

    span = 256
    per = span // own
    place = jnp.stack([lax.axis_index("fs"), lax.axis_index("tp")]).astype(jnp.int32)
    query_copy, out_copy, query_new, out_new = pl.pallas_call(
        functools.partial(final_kernel, float(rows * fs * cols * tp)),
        grid=(width // span,),
        out_shape=(
            jax.ShapeDtypeStruct((width, cols), bf16),
            jax.ShapeDtypeStruct((cols, width), bf16),
            jax.ShapeDtypeStruct((own, cols), f32),
            jax.ShapeDtypeStruct((own, cols), f32),
        ),
        in_specs=[
            SMEM,
            VMEM,
            VMEM,
            pl.BlockSpec((per, 2 * own, cols), lambda i: (i, 0, 0)),
            pl.BlockSpec((tp // 2, span, 128), lambda i: (0, i, 0)),
            pl.BlockSpec((tp // 2, span, 128), lambda i: (0, i, 0)),
        ],
        out_specs=(
            pl.BlockSpec((span, cols), lambda i: (i, 0)),
            pl.BlockSpec((cols, span), lambda i: (0, i)),
            pl.BlockSpec((own, cols), lambda i: (0, 0)),
            pl.BlockSpec((own, cols), lambda i: (0, 0)),
        ),
        scratch_shapes=[
            pltpu.VMEM((2, tp, rank_cols, cols), bf16),
            pltpu.VMEM((2, span, ranks), bf16),
            pltpu.VMEM((span, cols), f32),
        ],
        cost_estimate=cost(4 * width * ranks * cols, 20 << 20),
    )(place, low, squares, masters, held, other)
    return (query_new, out_new.T, query_copy, out_copy, first_new, second_new)


def solution(mesh):
    both = P("fs", "tp")
    moment = P(None, "fs", "tp")

    return jax.shard_map(
        body,
        mesh=mesh,
        in_specs=(P("fs", None), both, both, P("fs", None), both, both, both, P("tp", "fs"), moment, moment),
        out_specs=(both, P("tp", "fs"), P(None, "tp"), P("tp", None), moment, moment),
        check_vma=False,
    )
```

```python
import functools

import jax
import jax.numpy as jnp
from jax import lax
from jax.experimental import pallas as pl
from jax.experimental.pallas import tpu as pltpu
from jax.sharding import Mesh
from jax.sharding import PartitionSpec as P


bf16 = jnp.bfloat16
f32 = jnp.float32
FS = ("z", "y")
VMEM = pl.BlockSpec(memory_space=pltpu.VMEM)
SMEM = pl.BlockSpec(memory_space=pltpu.SMEM)
REACH = 2.0**19
SMALL = pltpu.CompilerParams(vmem_limit_bytes=16 << 20)


def cost(flops, nbytes):
    return pl.CostEstimate(flops=flops, bytes_accessed=nbytes, transcendentals=0)


def send_kernel(left, right, query_master, out_master, out, masters):
    own = query_master.shape[0]
    masters[:own] = query_master[...]
    masters[own : 2 * own] = out_master[...]
    masters[2 * own :] = jnp.zeros((masters.shape[0] - 2 * own, masters.shape[1]), f32)
    both = jnp.concatenate([left[...].astype(f32), right[...].astype(f32)], axis=1)
    used = both.shape[1]
    free = 128 - used
    kept = out.shape[1]
    rest = both[kept:]
    tail = jnp.concatenate([rest[:, j : j + free] for j in range(0, used, free)], axis=0)
    packed = jnp.concatenate([both[:kept], tail], axis=1).astype(bf16)
    out[...] = jnp.broadcast_to(packed[None], out.shape)


def unpacked(packed, used):
    free = 128 - used
    parts = used // free
    height = packed.shape[1] // parts
    wide = packed.astype(f32)
    tail = [wide[:, j * height : (j + 1) * height, used:] for j in range(parts)]
    tail = jnp.concatenate(tail + [jnp.zeros_like(tail[0])], axis=2)
    return jnp.concatenate([wide, tail], axis=1)


def proj_kernel(used, packed, saved_inputs, out_cotangent, out, left, right):
    step = pl.program_id(0)
    rows = saved_inputs.shape[1]

    @pl.when(step == 0)
    def _():
        left[...] = jnp.zeros_like(left)
        right[...] = jnp.zeros_like(right)

    factors = unpacked(packed[...], used).reshape(rows, 128).astype(bf16)
    left[...] += jnp.dot(saved_inputs[...], factors, preferred_element_type=f32)
    right[...] += jnp.dot(out_cotangent[...], factors, preferred_element_type=f32)

    @pl.when(step == pl.num_programs(0) - 1)
    def _():
        lane = lax.broadcasted_iota(jnp.int32, left.shape, 1)
        both = jnp.where(lane < used // 2, left[...], right[...])
        out[...] = both.T[:used].astype(bf16)


def grad_kernel(rank_cols, proj, query_cotangent, attn_outputs, out):
    cols = query_cotangent.shape[1]
    parts = []
    for k, other in enumerate((query_cotangent, attn_outputs)):
        starts = range(k * rank_cols, proj.shape[0], 2 * rank_cols)
        ranks = jnp.concatenate([proj[at : at + rank_cols] for at in starts], axis=0)
        parts.append(jnp.dot(ranks, other[...], preferred_element_type=f32).reshape(-1, 8, cols))
    first, second = parts
    both = jnp.concatenate([first[:, :4], second[:, :4], first[:, 4:], second[:, 4:]], axis=1)
    out[...] = both.astype(bf16)


def moment_kernel(pieces, first, second, first_new, second_new, low):
    rows = first.shape[1]
    grads = jnp.sum(pieces[...].astype(f32), axis=0)
    new_first = 0.9 * jnp.concatenate([first[0], first[1]], axis=0) + 0.1 * grads
    new_second = 0.99 * jnp.concatenate([second[0], second[1]], axis=0) + 0.01 * grads * grads
    direction = new_first / (jnp.sqrt(new_second) + 1e-08)
    first_new[0] = new_first[:rows]
    first_new[1] = new_first[rows:]
    second_new[0] = new_second[:rows]
    second_new[1] = new_second[rows:]
    squares = direction * direction
    lane = lax.broadcasted_iota(jnp.int32, (rows, 128), 1)
    sums = jnp.zeros((rows, 128), f32)
    for k in range(2):
        rest = jnp.sum(squares[k * rows : (k + 1) * rows], axis=(0, 1), keepdims=True)
        for part in range(3):
            rounded = rest.astype(bf16).astype(f32)
            sums = jnp.where(lane == 3 * k + part, rounded, sums)
            rest = rest - rounded
    sent = jnp.concatenate([direction[:rows], direction[rows:], sums], axis=1).astype(bf16)
    low[...] = jnp.broadcast_to(sent[None], low.shape)


def coded(value):
    size = jnp.abs(value) * REACH
    size = size * size
    size = size * size
    size = size * size
    return jnp.where(value < 0.0, -size, size).astype(bf16)


def decoded(code):
    wide = code.astype(f32)
    size = jnp.sqrt(jnp.sqrt(jnp.sqrt(jnp.abs(wide)))) * (1.0 / REACH)
    return jnp.where(wide < 0.0, -size, size)


def prep_kernel(rank_cols, place, masters, held, other, left, right, query_master, out_master, own_left, own_right, tile):
    own = masters.shape[1] // 2
    span = left.shape[0]
    cols = masters.shape[2]
    query_master[...] = decoded(masters[:, :own].reshape(span, cols))
    out_master[...] = decoded(masters[:, own:].reshape(span, cols)).T
    sides = [[], []]
    for half in (held, other):
        for s in range(half.shape[0]):
            block = unpacked(half[s], 2 * rank_cols).reshape(span, 128)
            for k in range(2):
                sides[k].append(block[:, k * rank_cols : (k + 1) * rank_cols])
    both = [jnp.concatenate(side, axis=1) for side in sides]
    left[...] = both[0].astype(bf16)
    right[...] = both[1].T.astype(bf16)

    @pl.when(pl.program_id(0) == place[0] // (span // own))
    def _():
        rows = pl.ds(pl.multiple_of(place[0] % (span // own) * own, own), own)
        for side, out in zip(both, (own_left, own_right)):
            tile[...] = side
            out[...] = tile[rows].astype(bf16)


def sums_kernel(rank_cols, place, low, squares, first, second):
    tp = squares.shape[0]
    cols = first.shape[1]
    per_block = rank_cols // low.shape[1]
    sums = jnp.sum(low[:, :, -128:].astype(f32), axis=0)[:1]
    squares[...] = jnp.broadcast_to(sums[None], squares.shape)
    for b in range(tp):
        chip, core = b % (tp // 2), b // (tp // 2)
        at = (place[1] + 2 * chip) % tp
        at = at + core * (1 - 2 * (at % 2))
        block = low[pl.ds(at * per_block, per_block)].astype(f32)
        for k, out in enumerate((first, second)):
            part = block[:, :, k * cols : (k + 1) * cols]
            part = jnp.concatenate([part[j] for j in range(per_block)], axis=0)
            out[b * rank_cols : (b + 1) * rank_cols] = part.astype(bf16)


def final_kernel(
    entries,
    squares,
    first,
    second,
    left,
    right,
    query_all,
    out_all,
    own_left,
    own_right,
    query_master,
    out_master,
    query_copy,
    out_copy,
    query_new,
    out_new,
):
    step = pl.program_id(0)
    sums = jnp.sum(squares[...], axis=0)[:1]
    lane = lax.broadcasted_iota(jnp.int32, sums.shape, 1)
    scales = []
    for k in range(2):
        total = jnp.sum(jnp.where(lane // 3 == k, sums, 0.0), axis=1, keepdims=True)
        scales.append(0.01 * lax.rsqrt(total / entries + 1e-06))
    moved = jnp.dot(left[...], first[...], preferred_element_type=f32)
    query_copy[...] = (query_all[...] - scales[0] * moved).astype(bf16)
    across = (((0,), (0,)), ((), ()))
    moved = lax.dot_general(second[...], right[...], across, preferred_element_type=f32)
    out_copy[...] = (out_all[...] - scales[1] * moved).astype(bf16)

    @pl.when(step == 0)
    def _():
        moved = jnp.dot(own_left[...], first[...], preferred_element_type=f32)
        query_new[...] = query_master[...] - scales[0] * moved
        moved = jnp.dot(own_right[...], second[...], preferred_element_type=f32)
        out_new[...] = out_master[...] - scales[1] * moved


def far(value):
    return pltpu.with_memory_space_constraint(value, pltpu.HBM)


def body(
    saved_inputs,
    query_cotangent,
    attn_outputs,
    out_cotangent,
    left_factor,
    right_factor,
    query_master,
    out_master,
    first_moment,
    second_moment,
):
    depth = lax.axis_size("z")
    fs = lax.axis_size(FS)
    tp = lax.axis_size("tp")
    own, rank_cols = left_factor.shape
    rows = first_moment.shape[1]
    cols = first_moment.shape[2]
    tokens = saved_inputs.shape[0]
    width = fs * own
    ranks = tp * rank_cols
    used = 2 * rank_cols
    kept = own * used // 128

    place = jnp.stack([lax.axis_index(FS), lax.axis_index("tp")]).astype(jnp.int32)
    packed, masters = pl.pallas_call(
        send_kernel,
        out_shape=(
            jax.ShapeDtypeStruct((fs, kept, 128), bf16),
            pltpu.HBM((88, cols), f32),
        ),
        in_specs=[pl.BlockSpec()] * 4,
        out_specs=(VMEM, VMEM),
        compiler_params=SMALL,
        cost_estimate=cost(1 << 16, 1 << 20),
    )(far(left_factor), far(right_factor), far(query_master), far(out_master.T))
    masters = lax.all_gather(masters, "y")
    packed = lax.all_to_all(packed, FS, 0, 0)
    packed, masters = lax.optimization_barrier((packed, masters))
    masters = masters[:, : 2 * own]
    masters = lax.all_gather(coded(masters), "z").reshape(fs, 2 * own, cols)
    parts = 6
    proj = pl.pallas_call(
        functools.partial(proj_kernel, used),
        grid=(parts,),
        out_shape=jax.ShapeDtypeStruct((used, tokens), bf16),
        in_specs=[
            pl.BlockSpec((fs // parts, kept, 128), lambda i: (i, 0, 0)),
            pl.BlockSpec((tokens, width // parts), lambda i: (0, i)),
            pl.BlockSpec((tokens, width // parts), lambda i: (0, i)),
        ],
        out_specs=pl.BlockSpec((used, tokens), lambda i: (0, 0)),
        scratch_shapes=[pltpu.VMEM((tokens, 128), f32)] * 2,
        compiler_params=SMALL,
        cost_estimate=cost(4 * tokens * width * 128, 8 << 20),
    )(packed, far(saved_inputs), far(out_cotangent))
    proj = lax.all_gather(proj, "tp", axis=0, tiled=True)

    partial = pl.pallas_call(
        functools.partial(grad_kernel, rank_cols),
        out_shape=pltpu.HBM((fs // 2, 4 * rows, cols), bf16),
        in_specs=[VMEM] * 3,
        out_specs=VMEM,
        compiler_params=SMALL,
        cost_estimate=cost(4 * ranks * tokens * cols, 2 << 20),
    )(proj, query_cotangent, attn_outputs)
    pieces = lax.all_to_all(partial.reshape(fs, 2 * rows, cols), FS, 0, 0)

    held = [packed]
    for step in range(1, tp // 2):
        held.append(lax.ppermute(packed, "tp", [((t + 2 * step) % tp, t) for t in range(tp)]))
    held = jnp.stack(held)
    other = lax.ppermute(held, "tp", [(t ^ 1, t) for t in range(tp)])

    first_new, second_new, low = pl.pallas_call(
        moment_kernel,
        out_shape=(
            jax.ShapeDtypeStruct(first_moment.shape, f32),
            jax.ShapeDtypeStruct(second_moment.shape, f32),
            pltpu.HBM((fs, rows, 2 * cols + 128), bf16),
        ),
        in_specs=[VMEM] * 3,
        out_specs=(VMEM, VMEM, VMEM),
        compiler_params=SMALL,
        cost_estimate=cost(1 << 20, 2 << 20),
    )(pieces, first_moment, second_moment)
    low = lax.all_to_all(low, FS, 0, 0)

    span = width // depth
    per = fs // depth
    left, right, query_all, out_all, own_left, own_right = pl.pallas_call(
        functools.partial(prep_kernel, rank_cols),
        grid=(depth,),
        out_shape=(
            pltpu.HBM((width, ranks), bf16),
            pltpu.HBM((ranks, width), bf16),
            pltpu.HBM((width, cols), f32),
            pltpu.HBM((cols, width), f32),
            pltpu.HBM((own, ranks), bf16),
            pltpu.HBM((own, ranks), bf16),
        ),
        in_specs=[
            SMEM,
            pl.BlockSpec((per, 2 * own, cols), lambda i: (i, 0, 0)),
            pl.BlockSpec((tp // 2, per, kept, 128), lambda i: (0, i, 0, 0)),
            pl.BlockSpec((tp // 2, per, kept, 128), lambda i: (0, i, 0, 0)),
        ],
        out_specs=(
            pl.BlockSpec((span, ranks), lambda i: (i, 0)),
            pl.BlockSpec((ranks, span), lambda i: (0, i)),
            pl.BlockSpec((span, cols), lambda i: (i, 0)),
            pl.BlockSpec((cols, span), lambda i: (0, i)),
            pl.BlockSpec((own, ranks), lambda i: (0, 0)),
            pl.BlockSpec((own, ranks), lambda i: (0, 0)),
        ),
        scratch_shapes=[pltpu.VMEM((span, ranks), f32)],
        compiler_params=SMALL,
        cost_estimate=cost(1 << 30, 30 << 20),
    )(place, far(masters), far(held), far(other))

    squares, first, second = pl.pallas_call(
        functools.partial(sums_kernel, rank_cols),
        out_shape=(
            jax.ShapeDtypeStruct((tp, 8, 128), f32),
            jax.ShapeDtypeStruct((ranks, cols), bf16),
            jax.ShapeDtypeStruct((ranks, cols), bf16),
        ),
        in_specs=[SMEM, VMEM],
        out_specs=(VMEM, VMEM, VMEM),
        compiler_params=SMALL,
        cost_estimate=cost(1 << 16, 1 << 16),
    )(place, low)
    squares = lax.all_to_all(squares, "tp", 0, 0)

    query_copy, out_copy, query_new, out_new = pl.pallas_call(
        functools.partial(final_kernel, float(rows * fs * cols * tp)),
        grid=(depth,),
        out_shape=(
            jax.ShapeDtypeStruct((width, cols), bf16),
            jax.ShapeDtypeStruct((cols, width), bf16),
            jax.ShapeDtypeStruct((own, cols), f32),
            jax.ShapeDtypeStruct((own, cols), f32),
        ),
        in_specs=[
            VMEM,
            VMEM,
            VMEM,
            pl.BlockSpec((span, ranks), lambda i: (i, 0)),
            pl.BlockSpec((ranks, span), lambda i: (0, i)),
            pl.BlockSpec((span, cols), lambda i: (i, 0)),
            pl.BlockSpec((cols, span), lambda i: (0, i)),
            VMEM,
            VMEM,
            VMEM,
            VMEM,
        ],
        out_specs=(
            pl.BlockSpec((span, cols), lambda i: (i, 0)),
            pl.BlockSpec((cols, span), lambda i: (0, i)),
            pl.BlockSpec((own, cols), lambda i: (0, 0)),
            pl.BlockSpec((own, cols), lambda i: (0, 0)),
        ),
        compiler_params=SMALL,
        cost_estimate=cost(4 * width * ranks * cols, 20 << 20),
    )(
        squares,
        first,
        second,
        left,
        right,
        query_all,
        out_all,
        own_left,
        own_right,
        query_master,
        out_master.T,
    )
    return (query_new, out_new.T, query_copy, out_copy, first_new, second_new)


def solution(mesh):
    finer = Mesh(mesh.devices.reshape(12, 8, 8), ("z", "y", "tp"))
    both = P(FS, "tp")
    moment = P(None, FS, "tp")

    return jax.shard_map(
        body,
        mesh=finer,
        in_specs=(P(FS, None), both, both, P(FS, None), both, both, both, P("tp", FS), moment, moment),
        out_specs=(both, P("tp", FS), P(None, "tp"), P("tp", None), moment, moment),
        check_vma=False,
    )
```

```python
import functools

import jax
import jax.numpy as jnp
from jax import lax
from jax.experimental import pallas as pl
from jax.experimental.pallas import tpu as pltpu
from jax.sharding import Mesh
from jax.sharding import PartitionSpec as P


bf16 = jnp.bfloat16
f32 = jnp.float32
FS = ("z", "y")
VMEM = pl.BlockSpec(memory_space=pltpu.VMEM)
SMEM = pl.BlockSpec(memory_space=pltpu.SMEM)
REACH = 2.0**19
SMALL = pltpu.CompilerParams(vmem_limit_bytes=16 << 20)


def cost(flops, nbytes):
    return pl.CostEstimate(flops=flops, bytes_accessed=nbytes, transcendentals=0)


def coded(value):
    size = jnp.abs(value) * REACH
    size = size * size
    size = size * size
    size = size * size
    return jnp.where(value < 0.0, -size, size).astype(bf16)


def decoded(code):
    size = jnp.abs(code)
    fourth = lax.rsqrt(lax.rsqrt(size))
    eighth = fourth * lax.rsqrt(lax.rsqrt(lax.rsqrt(size))) * (1.0 / REACH)
    return jnp.where(code == 0.0, 0.0, jnp.where(code < 0.0, -eighth, eighth))


def turned(value):
    n = value.shape[1]
    row = lax.broadcasted_iota(jnp.int32, (n, n), 0)
    eye = (row == lax.broadcasted_iota(jnp.int32, (n, n), 1)).astype(f32).astype(bf16)
    return lax.dot_general(eye, value, (((1,), (1,)), ((), ())), preferred_element_type=f32)


def send_kernel(left, right, query_master, out_master, out, masters):
    own = query_master.shape[0]
    masters[:own] = coded(query_master[...])
    masters[own:] = coded(out_master[...])
    both = jnp.concatenate([left[...].astype(f32), right[...].astype(f32)], axis=1)
    used = both.shape[1]
    free = 128 - used
    kept = out.shape[1]
    rest = both[kept:]
    tail = jnp.concatenate([rest[:, j : j + free] for j in range(0, used, free)], axis=0)
    packed = jnp.concatenate([both[:kept], tail], axis=1).astype(bf16)
    out[...] = jnp.broadcast_to(packed[None], out.shape)


def unpacked(packed, used):
    free = 128 - used
    parts = used // free
    height = packed.shape[1] // parts
    wide = packed.astype(f32)
    tail = [wide[:, j * height : (j + 1) * height, used:] for j in range(parts)]
    tail = jnp.concatenate(tail + [jnp.zeros_like(tail[0])], axis=2)
    return jnp.concatenate([wide, tail], axis=1)


def proj_kernel(used, packed, saved_inputs, out_cotangent, out, left, right):
    step = pl.program_id(0)
    rows = saved_inputs.shape[1]

    @pl.when(step == 0)
    def _():
        left[...] = jnp.zeros_like(left)
        right[...] = jnp.zeros_like(right)

    factors = unpacked(packed[...], used).reshape(rows, 128).astype(bf16)
    left[...] += jnp.dot(saved_inputs[...], factors, preferred_element_type=f32)
    right[...] += jnp.dot(out_cotangent[...], factors, preferred_element_type=f32)

    @pl.when(step == pl.num_programs(0) - 1)
    def _():
        lane = lax.broadcasted_iota(jnp.int32, left.shape, 1)
        both = jnp.where(lane < used // 2, left[...], right[...])
        out[...] = both.T[:used].astype(bf16)


def grad_kernel(rank_cols, proj, query_cotangent, attn_outputs, out):
    cols = query_cotangent.shape[1]
    parts = []
    for k, other in enumerate((query_cotangent, attn_outputs)):
        starts = range(k * rank_cols, proj.shape[0], 2 * rank_cols)
        ranks = jnp.concatenate([proj[at : at + rank_cols] for at in starts], axis=0)
        parts.append(jnp.dot(ranks, other[...], preferred_element_type=f32).reshape(-1, 8, cols))
    first, second = parts
    both = jnp.concatenate([first[:, :4], second[:, :4], first[:, 4:], second[:, 4:]], axis=1)
    out[...] = both.astype(bf16)


def moment_kernel(pieces, first, second, first_new, second_new, low):
    rows = first.shape[1]
    grads = jnp.sum(pieces[...].astype(f32), axis=0)
    new_first = 0.9 * jnp.concatenate([first[0], first[1]], axis=0) + 0.1 * grads
    new_second = 0.99 * jnp.concatenate([second[0], second[1]], axis=0) + 0.01 * grads * grads
    direction = new_first / (jnp.sqrt(new_second) + 1e-08)
    first_new[0] = new_first[:rows]
    first_new[1] = new_first[rows:]
    second_new[0] = new_second[:rows]
    second_new[1] = new_second[rows:]
    squares = direction * direction
    lane = lax.broadcasted_iota(jnp.int32, (rows, 128), 1)
    sums = jnp.zeros((rows, 128), f32)
    for k in range(2):
        rest = jnp.sum(squares[k * rows : (k + 1) * rows], axis=(0, 1), keepdims=True)
        for part in range(3):
            rounded = rest.astype(bf16).astype(f32)
            sums = jnp.where(lane == 3 * k + part, rounded, sums)
            rest = rest - rounded
    sent = jnp.concatenate([direction[:rows], direction[rows:], sums], axis=1).astype(bf16)
    low[...] = jnp.broadcast_to(sent[None], low.shape)


def prep_kernel(rank_cols, place, masters, held, other, left, right, query_master, out_master, own_left, own_right, tile):
    own = masters.shape[1] // 2
    span = left.shape[0]
    cols = masters.shape[2]
    query_master[...] = decoded(masters[:, :own].reshape(span, cols).astype(f32))
    out_master[...] = decoded(turned(masters[:, own:].reshape(span, cols)))
    sides = [[], []]
    for half in (held, other):
        for s in range(half.shape[0]):
            block = unpacked(half[s], 2 * rank_cols).reshape(span, 128)
            for k in range(2):
                sides[k].append(block[:, k * rank_cols : (k + 1) * rank_cols])
    both = [jnp.concatenate(side, axis=1).astype(bf16) for side in sides]
    left[...] = both[0]
    right[...] = turned(both[1]).astype(bf16)

    @pl.when(pl.program_id(0) == place[0] // (span // own))
    def _():
        rows = pl.ds(pl.multiple_of(place[0] % (span // own) * own, own), own)
        for side, out in zip(both, (own_left, own_right)):
            tile[...] = side
            out[...] = tile[rows]


def sums_kernel(rank_cols, place, low, squares, first, second, second_turned):
    tp = squares.shape[0]
    cols = first.shape[1]
    per_block = rank_cols // low.shape[1]
    sums = jnp.sum(low[:, :, -128:].astype(f32), axis=0)[:1]
    squares[...] = jnp.broadcast_to(sums[None], squares.shape)
    for b in range(tp):
        chip, core = b % (tp // 2), b // (tp // 2)
        at = (place[1] + 2 * chip) % tp
        at = at + core * (1 - 2 * (at % 2))
        block = low[pl.ds(at * per_block, per_block)].astype(f32)
        for k, out in enumerate((first, second)):
            part = block[:, :, k * cols : (k + 1) * cols]
            part = jnp.concatenate([part[j] for j in range(per_block)], axis=0)
            out[b * rank_cols : (b + 1) * rank_cols] = part.astype(bf16)
    second_turned[...] = turned(second[...]).astype(bf16)


def final_kernel(
    entries,
    squares,
    first,
    second,
    second_turned,
    left,
    right,
    query_all,
    out_all,
    own_left,
    own_right,
    query_master,
    out_master,
    query_copy,
    out_copy,
    query_new,
    out_new,
):
    step = pl.program_id(0)
    sums = jnp.sum(squares[...], axis=0)[:1]
    lane = lax.broadcasted_iota(jnp.int32, sums.shape, 1)
    scales = []
    for k in range(2):
        total = jnp.sum(jnp.where(lane // 3 == k, sums, 0.0), axis=1, keepdims=True)
        scales.append(0.01 * lax.rsqrt(total / entries + 1e-06))
    moved = jnp.dot(left[...], first[...], preferred_element_type=f32)
    query_copy[...] = (query_all[...] - scales[0] * moved).astype(bf16)
    moved = jnp.dot(second_turned[...], right[...], preferred_element_type=f32)
    out_copy[...] = (out_all[...] - scales[1] * moved).astype(bf16)

    @pl.when(step == 0)
    def _():
        moved = jnp.dot(own_left[...], first[...], preferred_element_type=f32)
        query_new[...] = query_master[...] - scales[0] * moved
        moved = jnp.dot(own_right[...], second[...], preferred_element_type=f32)
        out_new[...] = out_master[...] - scales[1] * moved


def far(value):
    return pltpu.with_memory_space_constraint(value, pltpu.HBM)


def body(
    saved_inputs,
    query_cotangent,
    attn_outputs,
    out_cotangent,
    left_factor,
    right_factor,
    query_master,
    out_master,
    first_moment,
    second_moment,
):
    depth = lax.axis_size("z")
    fs = lax.axis_size(FS)
    tp = lax.axis_size("tp")
    own, rank_cols = left_factor.shape
    rows = first_moment.shape[1]
    cols = first_moment.shape[2]
    tokens = saved_inputs.shape[0]
    width = fs * own
    ranks = tp * rank_cols
    used = 2 * rank_cols
    kept = own * used // 128

    place = jnp.stack([lax.axis_index(FS), lax.axis_index("tp")]).astype(jnp.int32)
    packed, masters = pl.pallas_call(
        send_kernel,
        out_shape=(jax.ShapeDtypeStruct((fs, kept, 128), bf16), pltpu.HBM((2 * own, cols), bf16)),
        in_specs=[pl.BlockSpec()] * 4,
        out_specs=(VMEM, VMEM),
        compiler_params=SMALL,
        cost_estimate=cost(1 << 16, 1 << 20),
    )(far(left_factor), far(right_factor), far(query_master), far(out_master.T))
    masters = lax.all_gather(masters, FS)
    packed = lax.all_to_all(packed, FS, 0, 0)
    parts = 6
    proj = pl.pallas_call(
        functools.partial(proj_kernel, used),
        grid=(parts,),
        out_shape=jax.ShapeDtypeStruct((used, tokens), bf16),
        in_specs=[
            pl.BlockSpec((fs // parts, kept, 128), lambda i: (i, 0, 0)),
            pl.BlockSpec((tokens, width // parts), lambda i: (0, i)),
            pl.BlockSpec((tokens, width // parts), lambda i: (0, i)),
        ],
        out_specs=pl.BlockSpec((used, tokens), lambda i: (0, 0)),
        scratch_shapes=[pltpu.VMEM((tokens, 128), f32)] * 2,
        compiler_params=SMALL,
        cost_estimate=cost(4 * tokens * width * 128, 8 << 20),
    )(packed, far(saved_inputs), far(out_cotangent))
    proj = lax.all_gather(proj, "tp", axis=0, tiled=True)

    partial = pl.pallas_call(
        functools.partial(grad_kernel, rank_cols),
        out_shape=pltpu.HBM((fs // 2, 4 * rows, cols), bf16),
        in_specs=[VMEM] * 3,
        out_specs=VMEM,
        compiler_params=SMALL,
        cost_estimate=cost(4 * ranks * tokens * cols, 2 << 20),
    )(proj, query_cotangent, attn_outputs)
    pieces = lax.all_to_all(partial.reshape(fs, 2 * rows, cols), FS, 0, 0)

    held = [packed]
    for step in range(1, tp // 2):
        held.append(lax.ppermute(packed, "tp", [((t + 2 * step) % tp, t) for t in range(tp)]))
    held = jnp.stack(held)
    other = lax.ppermute(held, "tp", [(t ^ 1, t) for t in range(tp)])

    first_new, second_new, low = pl.pallas_call(
        moment_kernel,
        out_shape=(
            jax.ShapeDtypeStruct(first_moment.shape, f32),
            jax.ShapeDtypeStruct(second_moment.shape, f32),
            pltpu.HBM((fs, rows, 2 * cols + 128), bf16),
        ),
        in_specs=[VMEM] * 3,
        out_specs=(VMEM, VMEM, VMEM),
        compiler_params=SMALL,
        cost_estimate=cost(1 << 20, 2 << 20),
    )(pieces, first_moment, second_moment)
    low = lax.all_to_all(low, FS, 0, 0)

    span = width // depth
    per = fs // depth
    left, right, query_all, out_all, own_left, own_right = pl.pallas_call(
        functools.partial(prep_kernel, rank_cols),
        grid=(depth,),
        out_shape=(
            pltpu.HBM((width, ranks), bf16),
            pltpu.HBM((ranks, width), bf16),
            pltpu.HBM((width, cols), f32),
            pltpu.HBM((cols, width), f32),
            pltpu.HBM((own, ranks), bf16),
            pltpu.HBM((own, ranks), bf16),
        ),
        in_specs=[
            SMEM,
            pl.BlockSpec((per, 2 * own, cols), lambda i: (i, 0, 0)),
            pl.BlockSpec((tp // 2, per, kept, 128), lambda i: (0, i, 0, 0)),
            pl.BlockSpec((tp // 2, per, kept, 128), lambda i: (0, i, 0, 0)),
        ],
        out_specs=(
            pl.BlockSpec((span, ranks), lambda i: (i, 0)),
            pl.BlockSpec((ranks, span), lambda i: (0, i)),
            pl.BlockSpec((span, cols), lambda i: (i, 0)),
            pl.BlockSpec((cols, span), lambda i: (0, i)),
            pl.BlockSpec((own, ranks), lambda i: (0, 0)),
            pl.BlockSpec((own, ranks), lambda i: (0, 0)),
        ),
        scratch_shapes=[pltpu.VMEM((span, ranks), bf16)],
        compiler_params=SMALL,
        cost_estimate=cost(1 << 30, 30 << 20),
    )(place, far(masters), far(held), far(other))

    squares, first, second, second_turned = pl.pallas_call(
        functools.partial(sums_kernel, rank_cols),
        out_shape=(
            jax.ShapeDtypeStruct((tp, 8, 128), f32),
            jax.ShapeDtypeStruct((ranks, cols), bf16),
            jax.ShapeDtypeStruct((ranks, cols), bf16),
            jax.ShapeDtypeStruct((cols, ranks), bf16),
        ),
        in_specs=[SMEM, VMEM],
        out_specs=(VMEM, VMEM, VMEM, VMEM),
        compiler_params=SMALL,
        cost_estimate=cost(1 << 16, 1 << 16),
    )(place, low)
    squares = lax.all_to_all(squares, "tp", 0, 0)

    query_copy, out_copy, query_new, out_new = pl.pallas_call(
        functools.partial(final_kernel, float(rows * fs * cols * tp)),
        grid=(depth,),
        out_shape=(
            jax.ShapeDtypeStruct((width, cols), bf16),
            jax.ShapeDtypeStruct((cols, width), bf16),
            jax.ShapeDtypeStruct((own, cols), f32),
            jax.ShapeDtypeStruct((own, cols), f32),
        ),
        in_specs=[
            VMEM,
            VMEM,
            VMEM,
            VMEM,
            pl.BlockSpec((span, ranks), lambda i: (i, 0)),
            pl.BlockSpec((ranks, span), lambda i: (0, i)),
            pl.BlockSpec((span, cols), lambda i: (i, 0)),
            pl.BlockSpec((cols, span), lambda i: (0, i)),
            pl.BlockSpec((own, ranks), lambda i: (0, 0)),
            pl.BlockSpec((own, ranks), lambda i: (0, 0)),
            pl.BlockSpec((own, cols), lambda i: (0, 0)),
            pl.BlockSpec((own, cols), lambda i: (0, 0)),
        ],
        out_specs=(
            pl.BlockSpec((span, cols), lambda i: (i, 0)),
            pl.BlockSpec((cols, span), lambda i: (0, i)),
            pl.BlockSpec((own, cols), lambda i: (0, 0)),
            pl.BlockSpec((own, cols), lambda i: (0, 0)),
        ),
        compiler_params=SMALL,
        cost_estimate=cost(4 * width * ranks * cols, 20 << 20),
    )(
        squares,
        first,
        second,
        second_turned,
        far(left),
        far(right),
        far(query_all),
        far(out_all),
        far(own_left),
        far(own_right),
        far(query_master),
        far(out_master.T),
    )
    return (query_new, out_new.T, query_copy, out_copy, first_new, second_new)


def solution(mesh):
    finer = Mesh(mesh.devices.reshape(12, 8, 8), ("z", "y", "tp"))
    both = P(FS, "tp")
    moment = P(None, FS, "tp")

    return jax.shard_map(
        body,
        mesh=finer,
        in_specs=(P(FS, None), both, both, P(FS, None), both, both, both, P("tp", FS), moment, moment),
        out_specs=(both, P("tp", FS), P(None, "tp"), P("tp", None), moment, moment),
        check_vma=False,
    )
```

```python
import functools

import jax
import jax.numpy as jnp
from jax import lax
from jax.experimental import pallas as pl
from jax.experimental.pallas import tpu as pltpu
from jax.sharding import Mesh
from jax.sharding import PartitionSpec as P


bf16 = jnp.bfloat16
f32 = jnp.float32
FS = ("z", "y")
VMEM = pl.BlockSpec(memory_space=pltpu.VMEM)
ANY = pl.BlockSpec(memory_space=pl.ANY)
SMEM = pl.BlockSpec(memory_space=pltpu.SMEM)
REACH = 2.0**19
SMALL = pltpu.CompilerParams(vmem_limit_bytes=16 << 20)


def cost(flops, nbytes):
    return pl.CostEstimate(flops=flops, bytes_accessed=nbytes, transcendentals=0)


def coded(value):
    size = jnp.abs(value) * REACH
    size = size * size
    size = size * size
    size = size * size
    return jnp.where(value < 0.0, -size, size).astype(bf16)


def decoded(code):
    size = jnp.abs(code)
    fourth = lax.rsqrt(lax.rsqrt(size))
    eighth = fourth * lax.rsqrt(lax.rsqrt(lax.rsqrt(size))) * (1.0 / REACH)
    return jnp.where(code == 0.0, 0.0, jnp.where(code < 0.0, -eighth, eighth))


def turned(value):
    n = value.shape[1]
    row = lax.broadcasted_iota(jnp.int32, (n, n), 0)
    eye = (row == lax.broadcasted_iota(jnp.int32, (n, n), 1)).astype(f32).astype(bf16)
    return lax.dot_general(eye, value, (((1,), (1,)), ((), ())), preferred_element_type=f32)


def send_kernel(left, right, query_master, out_master, out, masters):
    own = query_master.shape[0]
    masters[:own] = coded(query_master[...])
    masters[own:] = coded(out_master[...])
    both = jnp.concatenate([left[...].astype(f32), right[...].astype(f32)], axis=1)
    used = both.shape[1]
    free = 128 - used
    kept = out.shape[1]
    rest = both[kept:]
    tail = jnp.concatenate([rest[:, j : j + free] for j in range(0, used, free)], axis=0)
    packed = jnp.concatenate([both[:kept], tail], axis=1).astype(bf16)
    out[...] = jnp.broadcast_to(packed[None], out.shape)


def unpacked(packed, used):
    free = 128 - used
    parts = used // free
    height = packed.shape[1] // parts
    wide = packed.astype(f32)
    tail = [wide[:, j * height : (j + 1) * height, used:] for j in range(parts)]
    tail = jnp.concatenate(tail + [jnp.zeros_like(tail[0])], axis=2)
    return jnp.concatenate([wide, tail], axis=1)


def proj_kernel(used, parts, packed, saved_inputs, out_cotangent, out, near_inputs, near_cotangent, arrived):
    width = saved_inputs.shape[1] // parts
    count = packed.shape[0] // parts
    pairs = ((saved_inputs, near_inputs), (out_cotangent, near_cotangent))
    spans = [pl.ds(i * width, width) for i in range(parts)]
    copies = [
        [pltpu.make_async_copy(x.at[:, at], y.at[:, at], arrived.at[i, k]) for k, (x, y) in enumerate(pairs)]
        for i, at in enumerate(spans)
    ]
    for pair in copies:
        for copy in pair:
            copy.start()
    sums = [0.0, 0.0]
    for i, at in enumerate(spans):
        factors = unpacked(packed[i * count : (i + 1) * count], used).reshape(width, 128).astype(bf16)
        for k, (_, near) in enumerate(pairs):
            copies[i][k].wait()
            sums[k] = sums[k] + jnp.dot(near[:, at], factors, preferred_element_type=f32)
    lane = lax.broadcasted_iota(jnp.int32, sums[0].shape, 1)
    out[...] = jnp.where(lane < used // 2, sums[0], sums[1]).T[:used].astype(bf16)


def grad_kernel(rank_cols, proj, query_cotangent, attn_outputs, out):
    cols = query_cotangent.shape[1]
    parts = []
    for k, other in enumerate((query_cotangent, attn_outputs)):
        starts = range(k * rank_cols, proj.shape[0], 2 * rank_cols)
        ranks = jnp.concatenate([proj[at : at + rank_cols] for at in starts], axis=0)
        parts.append(jnp.dot(ranks, other[...], preferred_element_type=f32).reshape(-1, 8, cols))
    first, second = parts
    both = jnp.concatenate([first[:, :4], second[:, :4], first[:, 4:], second[:, 4:]], axis=1)
    out[...] = both.astype(bf16)


def moment_kernel(pieces, first, second, first_new, second_new, low):
    rows = first.shape[1]
    grads = jnp.sum(pieces[...].astype(f32), axis=0)
    new_first = 0.9 * jnp.concatenate([first[0], first[1]], axis=0) + 0.1 * grads
    new_second = 0.99 * jnp.concatenate([second[0], second[1]], axis=0) + 0.01 * grads * grads
    direction = new_first / (jnp.sqrt(new_second) + 1e-08)
    first_new[0] = new_first[:rows]
    first_new[1] = new_first[rows:]
    second_new[0] = new_second[:rows]
    second_new[1] = new_second[rows:]
    squares = direction * direction
    lane = lax.broadcasted_iota(jnp.int32, (rows, 128), 1)
    sums = jnp.zeros((rows, 128), f32)
    for k in range(2):
        rest = jnp.sum(squares[k * rows : (k + 1) * rows], axis=(0, 1), keepdims=True)
        for part in range(3):
            rounded = rest.astype(bf16).astype(f32)
            sums = jnp.where(lane == 3 * k + part, rounded, sums)
            rest = rest - rounded
    sent = jnp.concatenate([direction[:rows], direction[rows:], sums], axis=1).astype(bf16)
    low[...] = jnp.broadcast_to(sent[None], low.shape)


def prep_kernel(rank_cols, place, held, other, left, right, own_left, own_right, tile):
    own = own_left.shape[0]
    span = left.shape[0]
    sides = [[], []]
    for half in (held, other):
        for s in range(half.shape[0]):
            block = unpacked(half[s], 2 * rank_cols).reshape(span, 128)
            for k in range(2):
                sides[k].append(block[:, k * rank_cols : (k + 1) * rank_cols])
    both = [jnp.concatenate(side, axis=1).astype(bf16) for side in sides]
    left[...] = both[0]
    right[...] = turned(both[1]).astype(bf16)

    @pl.when(pl.program_id(0) == place[0] // (span // own))
    def _():
        rows = pl.ds(pl.multiple_of(place[0] % (span // own) * own, own), own)
        for side, out in zip(both, (own_left, own_right)):
            tile[...] = side
            out[...] = tile[rows]


def sums_kernel(rank_cols, place, low, squares, first, second, second_turned):
    tp = squares.shape[0]
    cols = first.shape[1]
    per_block = rank_cols // low.shape[1]
    sums = jnp.sum(low[:, :, -128:].astype(f32), axis=0)[:1]
    squares[...] = jnp.broadcast_to(sums[None], squares.shape)
    for b in range(tp):
        chip, core = b % (tp // 2), b // (tp // 2)
        at = (place[1] + 2 * chip) % tp
        at = at + core * (1 - 2 * (at % 2))
        block = low[pl.ds(at * per_block, per_block)].astype(f32)
        for k, out in enumerate((first, second)):
            part = block[:, :, k * cols : (k + 1) * cols]
            part = jnp.concatenate([part[j] for j in range(per_block)], axis=0)
            out[b * rank_cols : (b + 1) * rank_cols] = part.astype(bf16)
    second_turned[...] = turned(second[...]).astype(bf16)


def final_kernel(
    entries,
    span,
    squares,
    first,
    second,
    second_turned,
    left,
    right,
    masters,
    own_left,
    own_right,
    query_master,
    out_master,
    query_copy,
    out_copy,
    query_new,
    out_new,
    near_left,
    near_right,
    near_masters,
    near_query,
    near_out,
    near_own,
    near_master,
    near_new,
    arrived,
    own_arrived,
    left_for,
    own_left_for,
):
    width = left.shape[0]
    cols = first.shape[1]
    own = query_master.shape[0]
    per = span // own
    parts = width // span
    spans = [pl.ds(i * span, span) for i in range(parts)]
    copies = []
    for i, at in enumerate(spans):
        held = pl.ds(i * per, per)
        ways = (
            (left.at[at], near_left.at[at]),
            (masters.at[held], near_masters.at[held]),
            (right.at[:, at], near_right.at[:, at]),
        )
        copies.append([pltpu.make_async_copy(x, y, arrived.at[i, k]) for k, (x, y) in enumerate(ways)])
    ways = (
        (own_left, near_own.at[0]),
        (own_right, near_own.at[1]),
        (query_master, near_master.at[0]),
        (out_master, near_master.at[1]),
    )
    own_copies = [pltpu.make_async_copy(x, y, own_arrived.at[k]) for k, (x, y) in enumerate(ways)]
    for copy in [c for part in copies for c in part] + own_copies:
        copy.start()

    sums = jnp.sum(squares[...], axis=0)[:1]
    lane = lax.broadcasted_iota(jnp.int32, sums.shape, 1)
    scales = []
    for k in range(2):
        total = jnp.sum(jnp.where(lane // 3 == k, sums, 0.0), axis=1, keepdims=True)
        scales.append(0.01 * lax.rsqrt(total / entries + 1e-06))

    sent = []
    for i, at in enumerate(spans):
        for copy in copies[i]:
            copy.wait()
        codes = near_masters[i * per : (i + 1) * per]
        moved = jnp.dot(near_left[at], first[...], preferred_element_type=f32)
        kept = decoded(codes[:, :own].reshape(span, cols).astype(f32))
        near_query[at] = (kept - scales[0] * moved).astype(bf16)
        sent.append(pltpu.make_async_copy(near_query.at[at], query_copy.at[at], left_for.at[i, 0]))
        sent[-1].start()
        moved = jnp.dot(second_turned[...], near_right[:, at], preferred_element_type=f32)
        kept = decoded(turned(codes[:, own:].reshape(span, cols)))
        near_out[:, at] = (kept - scales[1] * moved).astype(bf16)
        sent.append(pltpu.make_async_copy(near_out.at[:, at], out_copy.at[:, at], left_for.at[i, 1]))
        sent[-1].start()
    for copy in own_copies:
        copy.wait()
    for k, (step, new) in enumerate(((first, query_new), (second, out_new))):
        moved = jnp.dot(near_own[k], step[...], preferred_element_type=f32)
        near_new[k] = near_master[k] - scales[k] * moved
        sent.append(pltpu.make_async_copy(near_new.at[k], new, own_left_for.at[k]))
        sent[-1].start()
    for copy in sent:
        copy.wait()


def far(value):
    return pltpu.with_memory_space_constraint(value, pltpu.HBM)


def body(
    saved_inputs,
    query_cotangent,
    attn_outputs,
    out_cotangent,
    left_factor,
    right_factor,
    query_master,
    out_master,
    first_moment,
    second_moment,
):
    fs = lax.axis_size(FS)
    tp = lax.axis_size("tp")
    own, rank_cols = left_factor.shape
    rows = first_moment.shape[1]
    cols = first_moment.shape[2]
    tokens = saved_inputs.shape[0]
    width = fs * own
    ranks = tp * rank_cols
    used = 2 * rank_cols
    kept = own * used // 128

    place = jnp.stack([lax.axis_index(FS), lax.axis_index("tp")]).astype(jnp.int32)
    packed, masters = pl.pallas_call(
        send_kernel,
        out_shape=(
            jax.ShapeDtypeStruct((fs, kept, 128), bf16),
            pltpu.HBM((2 * own, cols), bf16),
        ),
        in_specs=[pl.BlockSpec()] * 4,
        out_specs=(VMEM, VMEM),
        compiler_params=SMALL,
        cost_estimate=cost(1 << 16, 1 << 20),
    )(far(left_factor), far(right_factor), far(query_master), far(out_master.T))
    masters = lax.all_gather(masters, FS)
    packed = lax.all_to_all(packed, FS, 0, 0)
    parts = 6
    proj = pl.pallas_call(
        functools.partial(proj_kernel, used, parts),
        out_shape=jax.ShapeDtypeStruct((used, tokens), bf16),
        in_specs=[VMEM, ANY, ANY],
        out_specs=VMEM,
        scratch_shapes=[pltpu.VMEM((tokens, width), bf16)] * 2 + [pltpu.SemaphoreType.DMA((parts, 2))],
        compiler_params=SMALL,
        cost_estimate=cost(4 * tokens * width * 128, 8 << 20),
    )(packed, far(saved_inputs), far(out_cotangent))
    proj = lax.all_gather(proj, "tp", axis=0, tiled=True)

    partial = pl.pallas_call(
        functools.partial(grad_kernel, rank_cols),
        out_shape=pltpu.HBM((fs // 2, 4 * rows, cols), bf16),
        in_specs=[VMEM] * 3,
        out_specs=VMEM,
        compiler_params=SMALL,
        cost_estimate=cost(4 * ranks * tokens * cols, 2 << 20),
    )(proj, query_cotangent, attn_outputs)
    pieces = lax.all_to_all(partial.reshape(fs, 2 * rows, cols), FS, 0, 0)

    held = [packed]
    for step in range(1, tp // 2):
        held.append(lax.ppermute(packed, "tp", [((t + 2 * step) % tp, t) for t in range(tp)]))
    held = jnp.stack(held)
    other = lax.ppermute(held, "tp", [(t ^ 1, t) for t in range(tp)])

    first_new, second_new, low = pl.pallas_call(
        moment_kernel,
        out_shape=(
            jax.ShapeDtypeStruct(first_moment.shape, f32),
            jax.ShapeDtypeStruct(second_moment.shape, f32),
            pltpu.HBM((fs, rows, 2 * cols + 128), bf16),
        ),
        in_specs=[VMEM] * 3,
        out_specs=(VMEM, VMEM, VMEM),
        compiler_params=SMALL,
        cost_estimate=cost(1 << 20, 2 << 20),
    )(pieces, first_moment, second_moment)
    low = lax.all_to_all(low, FS, 0, 0)

    span = width // 6
    per = span // own
    left, right, own_left, own_right = pl.pallas_call(
        functools.partial(prep_kernel, rank_cols),
        grid=(width // span,),
        out_shape=(
            pltpu.HBM((width, ranks), bf16),
            pltpu.HBM((ranks, width), bf16),
            pltpu.HBM((own, ranks), bf16),
            pltpu.HBM((own, ranks), bf16),
        ),
        in_specs=[
            SMEM,
            pl.BlockSpec((tp // 2, per, kept, 128), lambda i: (0, i, 0, 0)),
            pl.BlockSpec((tp // 2, per, kept, 128), lambda i: (0, i, 0, 0)),
        ],
        out_specs=(
            pl.BlockSpec((span, ranks), lambda i: (i, 0)),
            pl.BlockSpec((ranks, span), lambda i: (0, i)),
            pl.BlockSpec((own, ranks), lambda i: (0, 0)),
            pl.BlockSpec((own, ranks), lambda i: (0, 0)),
        ),
        scratch_shapes=[pltpu.VMEM((span, ranks), bf16)],
        compiler_params=SMALL,
        cost_estimate=cost(1 << 30, 30 << 20),
    )(place, far(held), far(other))

    squares, first, second, second_turned = pl.pallas_call(
        functools.partial(sums_kernel, rank_cols),
        out_shape=(
            jax.ShapeDtypeStruct((tp, 8, 128), f32),
            jax.ShapeDtypeStruct((ranks, cols), bf16),
            jax.ShapeDtypeStruct((ranks, cols), bf16),
            jax.ShapeDtypeStruct((cols, ranks), bf16),
        ),
        in_specs=[SMEM, VMEM],
        out_specs=(VMEM, VMEM, VMEM, VMEM),
        compiler_params=SMALL,
        cost_estimate=cost(1 << 16, 1 << 16),
    )(place, low)
    squares = lax.all_to_all(squares, "tp", 0, 0)

    parts = width // span
    query_copy, out_copy, query_new, out_new = pl.pallas_call(
        functools.partial(final_kernel, float(rows * fs * cols * tp), span),
        out_shape=(
            pltpu.HBM((width, cols), bf16),
            pltpu.HBM((cols, width), bf16),
            pltpu.HBM((own, cols), f32),
            pltpu.HBM((own, cols), f32),
        ),
        in_specs=[VMEM] * 4 + [ANY] * 7,
        out_specs=(ANY,) * 4,
        scratch_shapes=[
            pltpu.VMEM((width, ranks), bf16),
            pltpu.VMEM((ranks, width), bf16),
            pltpu.VMEM(masters.shape, bf16),
            pltpu.VMEM((width, cols), bf16),
            pltpu.VMEM((cols, width), bf16),
            pltpu.VMEM((2, own, ranks), bf16),
            pltpu.VMEM((2, own, cols), f32),
            pltpu.VMEM((2, own, cols), f32),
            pltpu.SemaphoreType.DMA((parts, 3)),
            pltpu.SemaphoreType.DMA((4,)),
            pltpu.SemaphoreType.DMA((parts, 2)),
            pltpu.SemaphoreType.DMA((2,)),
        ],
        compiler_params=pltpu.CompilerParams(vmem_limit_bytes=32 << 20),
        cost_estimate=cost(4 * width * ranks * cols, 20 << 20),
    )(
        squares,
        first,
        second,
        second_turned,
        far(left),
        far(right),
        far(masters),
        far(own_left),
        far(own_right),
        far(query_master),
        far(out_master.T),
    )
    return (query_new, out_new.T, query_copy, out_copy, first_new, second_new)


def solution(mesh):
    finer = Mesh(mesh.devices.reshape(12, 8, 8), ("z", "y", "tp"))
    both = P(FS, "tp")
    moment = P(None, FS, "tp")

    return jax.shard_map(
        body,
        mesh=finer,
        in_specs=(P(FS, None), both, both, P(FS, None), both, both, both, P("tp", FS), moment, moment),
        out_specs=(both, P("tp", FS), P(None, "tp"), P("tp", None), moment, moment),
        check_vma=False,
    )
```

```python
import functools

import jax
import jax.numpy as jnp
from jax import lax
from jax.experimental import pallas as pl
from jax.experimental.pallas import tpu as pltpu
from jax.sharding import Mesh
from jax.sharding import PartitionSpec as P


bf16 = jnp.bfloat16
f32 = jnp.float32
FS = ("z", "y")
VMEM = pl.BlockSpec(memory_space=pltpu.VMEM)
ANY = pl.BlockSpec(memory_space=pl.ANY)
SMEM = pl.BlockSpec(memory_space=pltpu.SMEM)
REACH = 2.0**19
SMALL = pltpu.CompilerParams(vmem_limit_bytes=16 << 20)


def cost(flops, nbytes):
    return pl.CostEstimate(flops=flops, bytes_accessed=nbytes, transcendentals=0)


def coded(value):
    size = jnp.abs(value) * REACH
    size = size * size
    size = size * size
    size = size * size
    return jnp.where(value < 0.0, -size, size).astype(bf16)


def decoded(code):
    size = jnp.abs(code)
    fourth = lax.rsqrt(lax.rsqrt(size))
    eighth = fourth * lax.rsqrt(lax.rsqrt(lax.rsqrt(size))) * (1.0 / REACH)
    return jnp.where(code == 0.0, 0.0, jnp.where(code < 0.0, -eighth, eighth))


def turned(value):
    n = value.shape[1]
    row = lax.broadcasted_iota(jnp.int32, (n, n), 0)
    eye = (row == lax.broadcasted_iota(jnp.int32, (n, n), 1)).astype(f32).astype(bf16)
    return lax.dot_general(eye, value, (((1,), (1,)), ((), ())), preferred_element_type=f32)


def send_kernel(left, right, query_master, out_master, out, masters):
    codes = jnp.concatenate([coded(query_master[...]), coded(out_master[...])], axis=0)
    masters[...] = jnp.broadcast_to(codes[None], masters.shape)
    both = jnp.concatenate([left[...].astype(f32), right[...].astype(f32)], axis=1)
    used = both.shape[1]
    free = 128 - used
    kept = out.shape[1]
    rest = both[kept:]
    tail = jnp.concatenate([rest[:, j : j + free] for j in range(0, used, free)], axis=0)
    packed = jnp.concatenate([both[:kept], tail], axis=1).astype(bf16)
    out[...] = jnp.broadcast_to(packed[None], out.shape)


def unpacked(packed, used):
    free = 128 - used
    parts = used // free
    height = packed.shape[1] // parts
    wide = packed.astype(f32)
    tail = [wide[:, j * height : (j + 1) * height, used:] for j in range(parts)]
    tail = jnp.concatenate(tail + [jnp.zeros_like(tail[0])], axis=2)
    return jnp.concatenate([wide, tail], axis=1)


def proj_kernel(used, parts, packed, saved_inputs, out_cotangent, out, near_inputs, near_cotangent, arrived):
    width = saved_inputs.shape[1] // parts
    count = packed.shape[0] // parts
    pairs = ((saved_inputs, near_inputs), (out_cotangent, near_cotangent))
    spans = [pl.ds(i * width, width) for i in range(parts)]
    copies = [
        [pltpu.make_async_copy(x.at[:, at], y.at[:, at], arrived.at[i, k]) for k, (x, y) in enumerate(pairs)]
        for i, at in enumerate(spans)
    ]
    for pair in copies:
        for copy in pair:
            copy.start()
    sums = [0.0, 0.0]
    for i, at in enumerate(spans):
        factors = unpacked(packed[i * count : (i + 1) * count], used).reshape(width, 128).astype(bf16)
        for k, (_, near) in enumerate(pairs):
            copies[i][k].wait()
            sums[k] = sums[k] + jnp.dot(near[:, at], factors, preferred_element_type=f32)
    lane = lax.broadcasted_iota(jnp.int32, sums[0].shape, 1)
    out[...] = jnp.where(lane < used // 2, sums[0], sums[1]).T[:used].astype(bf16)


def grad_kernel(rank_cols, proj, query_cotangent, attn_outputs, out):
    cols = query_cotangent.shape[1]
    parts = []
    for k, other in enumerate((query_cotangent, attn_outputs)):
        starts = range(k * rank_cols, proj.shape[0], 2 * rank_cols)
        ranks = jnp.concatenate([proj[at : at + rank_cols] for at in starts], axis=0)
        parts.append(jnp.dot(ranks, other[...], preferred_element_type=f32).reshape(-1, 8, cols))
    first, second = parts
    both = jnp.concatenate([first[:, :4], second[:, :4], first[:, 4:], second[:, 4:]], axis=1)
    out[...] = both.astype(bf16)


def moment_kernel(pieces, first, second, first_new, second_new, low):
    rows = first.shape[1]
    grads = jnp.sum(pieces[...].astype(f32), axis=0)
    new_first = 0.9 * jnp.concatenate([first[0], first[1]], axis=0) + 0.1 * grads
    new_second = 0.99 * jnp.concatenate([second[0], second[1]], axis=0) + 0.01 * grads * grads
    direction = new_first / (jnp.sqrt(new_second) + 1e-08)
    first_new[0] = new_first[:rows]
    first_new[1] = new_first[rows:]
    second_new[0] = new_second[:rows]
    second_new[1] = new_second[rows:]
    squares = direction * direction
    lane = lax.broadcasted_iota(jnp.int32, (rows, 128), 1)
    sums = jnp.zeros((rows, 128), f32)
    for k in range(2):
        rest = jnp.sum(squares[k * rows : (k + 1) * rows], axis=(0, 1), keepdims=True)
        for part in range(3):
            rounded = rest.astype(bf16).astype(f32)
            sums = jnp.where(lane == 3 * k + part, rounded, sums)
            rest = rest - rounded
    sent = jnp.concatenate([direction[:rows], direction[rows:], sums], axis=1).astype(bf16)
    low[...] = jnp.broadcast_to(sent[None], low.shape)


def prep_kernel(rank_cols, place, held, other, left, right, own_left, own_right, tile):
    own = own_left.shape[0]
    span = left.shape[0]
    sides = [[], []]
    for half in (held, other):
        for s in range(half.shape[0]):
            block = unpacked(half[s], 2 * rank_cols).reshape(span, 128)
            for k in range(2):
                sides[k].append(block[:, k * rank_cols : (k + 1) * rank_cols])
    both = [jnp.concatenate(side, axis=1).astype(bf16) for side in sides]
    left[...] = both[0]
    right[...] = turned(both[1]).astype(bf16)

    @pl.when(pl.program_id(0) == place[0] // (span // own))
    def _():
        rows = pl.ds(pl.multiple_of(place[0] % (span // own) * own, own), own)
        for side, out in zip(both, (own_left, own_right)):
            tile[...] = side
            out[...] = tile[rows]


def decode_kernel(span, masters, query_master, out_master, near, near_query, near_out, arrived, left_for):
    own = masters.shape[1] // 2
    cols = masters.shape[2]
    per = span // own
    parts = masters.shape[0] // per
    spans = [pl.ds(i * span, span) for i in range(parts)]
    copies = []
    for i in range(parts):
        held = pl.ds(i * per, per)
        copies.append(pltpu.make_async_copy(masters.at[held], near.at[held], arrived.at[i]))
        copies[-1].start()
    sent = []
    for i, at in enumerate(spans):
        copies[i].wait()
        codes = near[i * per : (i + 1) * per]
        near_query[at] = decoded(codes[:, :own].reshape(span, cols).astype(f32))
        near_out[:, at] = decoded(turned(codes[:, own:].reshape(span, cols)))
        sent.append(pltpu.make_async_copy(near_query.at[at], query_master.at[at], left_for.at[i, 0]))
        sent.append(pltpu.make_async_copy(near_out.at[:, at], out_master.at[:, at], left_for.at[i, 1]))
        sent[-2].start()
        sent[-1].start()
    for copy in sent:
        copy.wait()


def sums_kernel(rank_cols, place, low, squares, first, second, second_turned):
    tp = squares.shape[0]
    cols = first.shape[1]
    per_block = rank_cols // low.shape[1]
    sums = jnp.sum(low[:, :, -128:].astype(f32), axis=0)[:1]
    squares[...] = jnp.broadcast_to(sums[None], squares.shape)
    for b in range(tp):
        chip, core = b % (tp // 2), b // (tp // 2)
        at = (place[1] + 2 * chip) % tp
        at = at + core * (1 - 2 * (at % 2))
        block = low[pl.ds(at * per_block, per_block)].astype(f32)
        for k, out in enumerate((first, second)):
            part = block[:, :, k * cols : (k + 1) * cols]
            part = jnp.concatenate([part[j] for j in range(per_block)], axis=0)
            out[b * rank_cols : (b + 1) * rank_cols] = part.astype(bf16)
    second_turned[...] = turned(second[...]).astype(bf16)


def final_kernel(
    entries,
    span,
    squares,
    first,
    second,
    second_turned,
    left,
    right,
    query_all,
    out_all,
    own_left,
    own_right,
    query_master,
    out_master,
    query_copy,
    out_copy,
    query_new,
    out_new,
    near_left,
    near_right,
    near_query_all,
    near_out_all,
    near_query,
    near_out,
    near_own,
    near_master,
    near_new,
    arrived,
    own_arrived,
    left_for,
    own_left_for,
):
    width = left.shape[0]
    parts = width // span
    spans = [pl.ds(i * span, span) for i in range(parts)]
    copies = []
    for i, at in enumerate(spans):
        ways = (
            (left.at[at], near_left.at[at]),
            (query_all.at[at], near_query_all.at[at]),
            (right.at[:, at], near_right.at[:, at]),
            (out_all.at[:, at], near_out_all.at[:, at]),
        )
        copies.append([pltpu.make_async_copy(x, y, arrived.at[i, k]) for k, (x, y) in enumerate(ways)])
    ways = (
        (own_left, near_own.at[0]),
        (own_right, near_own.at[1]),
        (query_master, near_master.at[0]),
        (out_master, near_master.at[1]),
    )
    own_copies = [pltpu.make_async_copy(x, y, own_arrived.at[k]) for k, (x, y) in enumerate(ways)]
    for copy in [c for part in copies for c in part] + own_copies:
        copy.start()

    sums = jnp.sum(squares[...], axis=0)[:1]
    lane = lax.broadcasted_iota(jnp.int32, sums.shape, 1)
    scales = []
    for k in range(2):
        total = jnp.sum(jnp.where(lane // 3 == k, sums, 0.0), axis=1, keepdims=True)
        scales.append(0.01 * lax.rsqrt(total / entries + 1e-06))

    sent = []
    for i, at in enumerate(spans):
        for copy in copies[i]:
            copy.wait()
        moved = jnp.dot(near_left[at], first[...], preferred_element_type=f32)
        near_query[at] = (near_query_all[at] - scales[0] * moved).astype(bf16)
        sent.append(pltpu.make_async_copy(near_query.at[at], query_copy.at[at], left_for.at[i, 0]))
        sent[-1].start()
        moved = jnp.dot(second_turned[...], near_right[:, at], preferred_element_type=f32)
        near_out[:, at] = (near_out_all[:, at] - scales[1] * moved).astype(bf16)
        sent.append(pltpu.make_async_copy(near_out.at[:, at], out_copy.at[:, at], left_for.at[i, 1]))
        sent[-1].start()
    for copy in own_copies:
        copy.wait()
    for k, (step, new) in enumerate(((first, query_new), (second, out_new))):
        moved = jnp.dot(near_own[k], step[...], preferred_element_type=f32)
        near_new[k] = near_master[k] - scales[k] * moved
        sent.append(pltpu.make_async_copy(near_new.at[k], new, own_left_for.at[k]))
        sent[-1].start()
    for copy in sent:
        copy.wait()


def far(value):
    return pltpu.with_memory_space_constraint(value, pltpu.HBM)


def body(
    saved_inputs,
    query_cotangent,
    attn_outputs,
    out_cotangent,
    left_factor,
    right_factor,
    query_master,
    out_master,
    first_moment,
    second_moment,
):
    height = lax.axis_size("y")
    fs = lax.axis_size(FS)
    tp = lax.axis_size("tp")
    own, rank_cols = left_factor.shape
    rows = first_moment.shape[1]
    cols = first_moment.shape[2]
    tokens = saved_inputs.shape[0]
    width = fs * own
    ranks = tp * rank_cols
    used = 2 * rank_cols
    kept = own * used // 128

    place = jnp.stack([lax.axis_index(FS), lax.axis_index("tp")]).astype(jnp.int32)
    packed, masters = pl.pallas_call(
        send_kernel,
        out_shape=(
            jax.ShapeDtypeStruct((fs, kept, 128), bf16),
            pltpu.HBM((height, 2 * own, cols), bf16),
        ),
        in_specs=[pl.BlockSpec()] * 4,
        out_specs=(VMEM, VMEM),
        compiler_params=SMALL,
        cost_estimate=cost(1 << 16, 1 << 20),
    )(far(left_factor), far(right_factor), far(query_master), far(out_master.T))
    packed = lax.all_to_all(packed, FS, 0, 0)
    masters = lax.all_to_all(masters, "y", 0, 0)
    masters = lax.all_gather(masters, "z").reshape(fs, 2 * own, cols)
    parts = 6
    proj = pl.pallas_call(
        functools.partial(proj_kernel, used, parts),
        out_shape=jax.ShapeDtypeStruct((used, tokens), bf16),
        in_specs=[VMEM, ANY, ANY],
        out_specs=VMEM,
        scratch_shapes=[pltpu.VMEM((tokens, width), bf16)] * 2 + [pltpu.SemaphoreType.DMA((parts, 2))],
        compiler_params=SMALL,
        cost_estimate=cost(4 * tokens * width * 128, 8 << 20),
    )(packed, far(saved_inputs), far(out_cotangent))
    proj = lax.all_gather(proj, "tp", axis=0, tiled=True)

    partial = pl.pallas_call(
        functools.partial(grad_kernel, rank_cols),
        out_shape=pltpu.HBM((fs // 2, 4 * rows, cols), bf16),
        in_specs=[VMEM] * 3,
        out_specs=VMEM,
        compiler_params=SMALL,
        cost_estimate=cost(4 * ranks * tokens * cols, 2 << 20),
    )(proj, query_cotangent, attn_outputs)
    pieces = lax.all_to_all(partial.reshape(fs, 2 * rows, cols), FS, 0, 0)

    held = [packed]
    for step in range(1, tp // 2):
        held.append(lax.ppermute(packed, "tp", [((t + 2 * step) % tp, t) for t in range(tp)]))
    held = jnp.stack(held)
    other = lax.ppermute(held, "tp", [(t ^ 1, t) for t in range(tp)])

    first_new, second_new, low = pl.pallas_call(
        moment_kernel,
        out_shape=(
            jax.ShapeDtypeStruct(first_moment.shape, f32),
            jax.ShapeDtypeStruct(second_moment.shape, f32),
            pltpu.HBM((fs, rows, 2 * cols + 128), bf16),
        ),
        in_specs=[VMEM] * 3,
        out_specs=(VMEM, VMEM, VMEM),
        compiler_params=SMALL,
        cost_estimate=cost(1 << 20, 2 << 20),
    )(pieces, first_moment, second_moment)
    low = lax.all_to_all(low, FS, 0, 0)

    span = width // 6
    per = span // own
    left, right, own_left, own_right = pl.pallas_call(
        functools.partial(prep_kernel, rank_cols),
        grid=(width // span,),
        out_shape=(
            pltpu.HBM((width, ranks), bf16),
            pltpu.HBM((ranks, width), bf16),
            pltpu.HBM((own, ranks), bf16),
            pltpu.HBM((own, ranks), bf16),
        ),
        in_specs=[
            SMEM,
            pl.BlockSpec((tp // 2, per, kept, 128), lambda i: (0, i, 0, 0)),
            pl.BlockSpec((tp // 2, per, kept, 128), lambda i: (0, i, 0, 0)),
        ],
        out_specs=(
            pl.BlockSpec((span, ranks), lambda i: (i, 0)),
            pl.BlockSpec((ranks, span), lambda i: (0, i)),
            pl.BlockSpec((own, ranks), lambda i: (0, 0)),
            pl.BlockSpec((own, ranks), lambda i: (0, 0)),
        ),
        scratch_shapes=[pltpu.VMEM((span, ranks), bf16)],
        compiler_params=SMALL,
        cost_estimate=cost(1 << 30, 30 << 20),
    )(place, far(held), far(other))

    parts = width // span
    query_all, out_all = pl.pallas_call(
        functools.partial(decode_kernel, span),
        out_shape=(pltpu.HBM((width, cols), f32), pltpu.HBM((cols, width), f32)),
        in_specs=[ANY],
        out_specs=(ANY, ANY),
        scratch_shapes=[
            pltpu.VMEM(masters.shape, bf16),
            pltpu.VMEM((width, cols), f32),
            pltpu.VMEM((cols, width), f32),
            pltpu.SemaphoreType.DMA((parts,)),
            pltpu.SemaphoreType.DMA((parts, 2)),
        ],
        compiler_params=pltpu.CompilerParams(vmem_limit_bytes=24 << 20),
        cost_estimate=cost(1 << 30, 15 << 20),
    )(far(masters))

    squares, first, second, second_turned = pl.pallas_call(
        functools.partial(sums_kernel, rank_cols),
        out_shape=(
            jax.ShapeDtypeStruct((tp, 8, 128), f32),
            jax.ShapeDtypeStruct((ranks, cols), bf16),
            jax.ShapeDtypeStruct((ranks, cols), bf16),
            jax.ShapeDtypeStruct((cols, ranks), bf16),
        ),
        in_specs=[SMEM, VMEM],
        out_specs=(VMEM, VMEM, VMEM, VMEM),
        compiler_params=SMALL,
        cost_estimate=cost(1 << 16, 1 << 16),
    )(place, low)
    squares = lax.all_to_all(squares, "tp", 0, 0)

    parts = width // span
    query_copy, out_copy, query_new, out_new = pl.pallas_call(
        functools.partial(final_kernel, float(rows * fs * cols * tp), span),
        out_shape=(
            pltpu.HBM((width, cols), bf16),
            pltpu.HBM((cols, width), bf16),
            pltpu.HBM((own, cols), f32),
            pltpu.HBM((own, cols), f32),
        ),
        in_specs=[VMEM] * 4 + [ANY] * 8,
        out_specs=(ANY,) * 4,
        scratch_shapes=[
            pltpu.VMEM((width, ranks), bf16),
            pltpu.VMEM((ranks, width), bf16),
            pltpu.VMEM((width, cols), f32),
            pltpu.VMEM((cols, width), f32),
            pltpu.VMEM((width, cols), bf16),
            pltpu.VMEM((cols, width), bf16),
            pltpu.VMEM((2, own, ranks), bf16),
            pltpu.VMEM((2, own, cols), f32),
            pltpu.VMEM((2, own, cols), f32),
            pltpu.SemaphoreType.DMA((parts, 4)),
            pltpu.SemaphoreType.DMA((4,)),
            pltpu.SemaphoreType.DMA((parts, 2)),
            pltpu.SemaphoreType.DMA((2,)),
        ],
        compiler_params=pltpu.CompilerParams(vmem_limit_bytes=32 << 20),
        cost_estimate=cost(4 * width * ranks * cols, 20 << 20),
    )(
        squares,
        first,
        second,
        second_turned,
        far(left),
        far(right),
        far(query_all),
        far(out_all),
        far(own_left),
        far(own_right),
        far(query_master),
        far(out_master.T),
    )
    return (query_new, out_new.T, query_copy, out_copy, first_new, second_new)


def solution(mesh):
    finer = Mesh(mesh.devices.reshape(12, 8, 8), ("z", "y", "tp"))
    both = P(FS, "tp")
    moment = P(None, FS, "tp")

    return jax.shard_map(
        body,
        mesh=finer,
        in_specs=(P(FS, None), both, both, P(FS, None), both, both, both, P("tp", FS), moment, moment),
        out_specs=(both, P("tp", FS), P(None, "tp"), P("tp", None), moment, moment),
        check_vma=False,
    )
```

```python
import functools

import jax
import jax.numpy as jnp
from jax import lax
from jax.experimental import pallas as pl
from jax.experimental.pallas import tpu as pltpu
from jax.sharding import Mesh
from jax.sharding import PartitionSpec as P


bf16 = jnp.bfloat16
f32 = jnp.float32
FS = ("z", "y")
VMEM = pl.BlockSpec(memory_space=pltpu.VMEM)
ANY = pl.BlockSpec(memory_space=pl.ANY)
SMEM = pl.BlockSpec(memory_space=pltpu.SMEM)
REACH = 2.0**19
SMALL = pltpu.CompilerParams(vmem_limit_bytes=16 << 20)


def cost(flops, nbytes):
    return pl.CostEstimate(flops=flops, bytes_accessed=nbytes, transcendentals=0)


LONG = cost(1 << 35, 1 << 26)


def coded(value):
    size = jnp.abs(value) * REACH
    size = size * size
    size = size * size
    size = size * size
    return jnp.where(value < 0.0, -size, size).astype(bf16)


def decoded(code):
    size = jnp.abs(code)
    fourth = lax.rsqrt(lax.rsqrt(size))
    eighth = fourth * lax.rsqrt(lax.rsqrt(lax.rsqrt(size))) * (1.0 / REACH)
    return jnp.where(code == 0.0, 0.0, jnp.where(code < 0.0, -eighth, eighth))


def turned(value):
    n = value.shape[1]
    row = lax.broadcasted_iota(jnp.int32, (n, n), 0)
    eye = (row == lax.broadcasted_iota(jnp.int32, (n, n), 1)).astype(f32).astype(bf16)
    return lax.dot_general(eye, value, (((1,), (1,)), ((), ())), preferred_element_type=f32)


def send_kernel(left, right, query_master, out_master, out, masters):
    own = query_master.shape[0]
    masters[:own] = coded(query_master[...])
    masters[own:] = coded(out_master[...])
    both = jnp.concatenate([left[...].astype(f32), right[...].astype(f32)], axis=1)
    used = both.shape[1]
    free = 128 - used
    kept = out.shape[1]
    rest = both[kept:]
    tail = jnp.concatenate([rest[:, j : j + free] for j in range(0, used, free)], axis=0)
    packed = jnp.concatenate([both[:kept], tail], axis=1).astype(bf16)
    out[...] = jnp.broadcast_to(packed[None], out.shape)


def hold_kernel(masters, packed, out):
    pass


def unpacked(packed, used):
    free = 128 - used
    parts = used // free
    height = packed.shape[1] // parts
    wide = packed.astype(f32)
    tail = [wide[:, j * height : (j + 1) * height, used:] for j in range(parts)]
    tail = jnp.concatenate(tail + [jnp.zeros_like(tail[0])], axis=2)
    return jnp.concatenate([wide, tail], axis=1)


def proj_kernel(used, packed, saved_inputs, out_cotangent, out, factors):
    own = factors.shape[0] // packed.shape[0]
    step = 8
    for i in range(0, packed.shape[0], step):
        block = unpacked(packed[i : i + step], used).reshape(step * own, 128)
        factors[i * own : (i + step) * own] = block.astype(bf16)
    left = jnp.dot(saved_inputs[...], factors[...], preferred_element_type=f32)
    right = jnp.dot(out_cotangent[...], factors[...], preferred_element_type=f32)
    lane = lax.broadcasted_iota(jnp.int32, left.shape, 1)
    out[...] = jnp.where(lane < used // 2, left, right).T[:used].astype(bf16)


def grad_kernel(rank_cols, proj, query_cotangent, attn_outputs, out):
    cols = query_cotangent.shape[1]
    parts = []
    for k, other in enumerate((query_cotangent, attn_outputs)):
        starts = range(k * rank_cols, proj.shape[0], 2 * rank_cols)
        ranks = jnp.concatenate([proj[at : at + rank_cols] for at in starts], axis=0)
        parts.append(jnp.dot(ranks, other[...], preferred_element_type=f32).reshape(-1, 8, cols))
    first, second = parts
    both = jnp.concatenate([first[:, :4], second[:, :4], first[:, 4:], second[:, 4:]], axis=1)
    out[...] = both.astype(bf16)


def moment_kernel(pieces, first, second, first_new, second_new, low):
    rows = first.shape[1]
    grads = jnp.sum(pieces[...].astype(f32), axis=0)
    new_first = 0.9 * jnp.concatenate([first[0], first[1]], axis=0) + 0.1 * grads
    new_second = 0.99 * jnp.concatenate([second[0], second[1]], axis=0) + 0.01 * grads * grads
    direction = new_first / (jnp.sqrt(new_second) + 1e-08)
    first_new[0] = new_first[:rows]
    first_new[1] = new_first[rows:]
    second_new[0] = new_second[:rows]
    second_new[1] = new_second[rows:]
    squares = direction * direction
    lane = lax.broadcasted_iota(jnp.int32, (rows, 128), 1)
    sums = jnp.zeros((rows, 128), f32)
    for k in range(2):
        rest = jnp.sum(squares[k * rows : (k + 1) * rows], axis=(0, 1), keepdims=True)
        for part in range(3):
            rounded = rest.astype(bf16).astype(f32)
            sums = jnp.where(lane == 3 * k + part, rounded, sums)
            rest = rest - rounded
    sent = jnp.concatenate([direction[:rows], direction[rows:], sums], axis=1).astype(bf16)
    low[...] = jnp.broadcast_to(sent[None], low.shape)


def prep_kernel(rank_cols, place, held, other, left, right, own_left, own_right, tile):
    own = own_left.shape[0]
    span = left.shape[0]
    sides = [[], []]
    for half in (held, other):
        for s in range(half.shape[0]):
            block = unpacked(half[s], 2 * rank_cols).reshape(span, 128)
            for k in range(2):
                sides[k].append(block[:, k * rank_cols : (k + 1) * rank_cols])
    both = [jnp.concatenate(side, axis=1).astype(bf16) for side in sides]
    left[...] = both[0]
    right[...] = turned(both[1]).astype(bf16)

    @pl.when(pl.program_id(0) == place[0] // (span // own))
    def _():
        rows = pl.ds(pl.multiple_of(place[0] % (span // own) * own, own), own)
        for side, out in zip(both, (own_left, own_right)):
            tile[...] = side
            out[...] = tile[rows]


def sums_kernel(rank_cols, place, low, squares, first, second, second_turned):
    tp = squares.shape[0]
    cols = first.shape[1]
    per_block = rank_cols // low.shape[1]
    sums = jnp.sum(low[:, :, -128:].astype(f32), axis=0)[:1]
    squares[...] = jnp.broadcast_to(sums[None], squares.shape)
    for b in range(tp):
        chip, core = b % (tp // 2), b // (tp // 2)
        at = (place[1] + 2 * chip) % tp
        at = at + core * (1 - 2 * (at % 2))
        block = low[pl.ds(at * per_block, per_block)].astype(f32)
        for k, out in enumerate((first, second)):
            part = block[:, :, k * cols : (k + 1) * cols]
            part = jnp.concatenate([part[j] for j in range(per_block)], axis=0)
            out[b * rank_cols : (b + 1) * rank_cols] = part.astype(bf16)
    second_turned[...] = turned(second[...]).astype(bf16)


def final_kernel(
    entries,
    span,
    squares,
    first,
    second,
    second_turned,
    left,
    right,
    masters,
    own_left,
    own_right,
    query_master,
    out_master,
    query_copy,
    out_copy,
    query_new,
    out_new,
    near_query,
    near_out,
    near_own,
    near_master,
    near_new,
    own_arrived,
    left_for,
    own_left_for,
):
    width = left.shape[0]
    cols = first.shape[1]
    own = query_master.shape[0]
    per = span // own
    parts = width // span
    spans = [pl.ds(i * span, span) for i in range(parts)]
    ways = (
        (own_left, near_own.at[0]),
        (own_right, near_own.at[1]),
        (query_master, near_master.at[0]),
        (out_master, near_master.at[1]),
    )
    own_copies = [pltpu.make_async_copy(x, y, own_arrived.at[k]) for k, (x, y) in enumerate(ways)]
    for copy in own_copies:
        copy.start()

    sums = jnp.sum(squares[...], axis=0)[:1]
    lane = lax.broadcasted_iota(jnp.int32, sums.shape, 1)
    scales = []
    for k in range(2):
        total = jnp.sum(jnp.where(lane // 3 == k, sums, 0.0), axis=1, keepdims=True)
        scales.append(0.01 * lax.rsqrt(total / entries + 1e-06))

    sent = []
    for i, at in enumerate(spans):
        codes = masters[i * per : (i + 1) * per]
        moved = jnp.dot(left[at], first[...], preferred_element_type=f32)
        kept = decoded(codes[:, :own].reshape(span, cols).astype(f32))
        near_query[at] = (kept - scales[0] * moved).astype(bf16)
        sent.append(pltpu.make_async_copy(near_query.at[at], query_copy.at[at], left_for.at[i, 0]))
        sent[-1].start()
        moved = jnp.dot(second_turned[...], right[:, at], preferred_element_type=f32)
        kept = decoded(turned(codes[:, own:].reshape(span, cols)))
        near_out[:, at] = (kept - scales[1] * moved).astype(bf16)
        sent.append(pltpu.make_async_copy(near_out.at[:, at], out_copy.at[:, at], left_for.at[i, 1]))
        sent[-1].start()
    for copy in own_copies:
        copy.wait()
    for k, (step, new) in enumerate(((first, query_new), (second, out_new))):
        moved = jnp.dot(near_own[k], step[...], preferred_element_type=f32)
        near_new[k] = near_master[k] - scales[k] * moved
        sent.append(pltpu.make_async_copy(near_new.at[k], new, own_left_for.at[k]))
        sent[-1].start()
    for copy in sent:
        copy.wait()


def far(value):
    return pltpu.with_memory_space_constraint(value, pltpu.HBM)


def body(
    saved_inputs,
    query_cotangent,
    attn_outputs,
    out_cotangent,
    left_factor,
    right_factor,
    query_master,
    out_master,
    first_moment,
    second_moment,
):
    fs = lax.axis_size(FS)
    tp = lax.axis_size("tp")
    own, rank_cols = left_factor.shape
    rows = first_moment.shape[1]
    cols = first_moment.shape[2]
    tokens = saved_inputs.shape[0]
    width = fs * own
    ranks = tp * rank_cols
    used = 2 * rank_cols
    kept = own * used // 128

    place = jnp.stack([lax.axis_index(FS), lax.axis_index("tp")]).astype(jnp.int32)
    packed, masters = pl.pallas_call(
        send_kernel,
        out_shape=(jax.ShapeDtypeStruct((fs, kept, 128), bf16), pltpu.HBM((2 * own, cols), bf16)),
        in_specs=[pl.BlockSpec()] * 4,
        out_specs=(VMEM, VMEM),
        compiler_params=SMALL,
        cost_estimate=cost(1 << 16, 1 << 20),
    )(far(left_factor), far(right_factor), far(query_master), far(out_master.T))
    packed = pl.pallas_call(
        hold_kernel,
        out_shape=jax.ShapeDtypeStruct(packed.shape, bf16),
        in_specs=[ANY, ANY],
        out_specs=ANY,
        input_output_aliases={1: 0},
        compiler_params=SMALL,
        cost_estimate=LONG,
    )(far(masters), packed)
    masters = lax.all_gather(masters, FS)
    packed = lax.all_to_all(packed, FS, 0, 0)
    proj = pl.pallas_call(
        functools.partial(proj_kernel, used),
        out_shape=jax.ShapeDtypeStruct((used, tokens), bf16),
        in_specs=[VMEM] * 3,
        out_specs=VMEM,
        scratch_shapes=[pltpu.VMEM((width, 128), bf16)],
        compiler_params=SMALL,
        cost_estimate=cost(4 * tokens * width * 128, 8 << 20),
    )(packed, saved_inputs, out_cotangent)
    proj = lax.all_gather(proj, "tp", axis=0, tiled=True)

    partial = pl.pallas_call(
        functools.partial(grad_kernel, rank_cols),
        out_shape=pltpu.HBM((fs // 2, 4 * rows, cols), bf16),
        in_specs=[VMEM] * 3,
        out_specs=VMEM,
        compiler_params=SMALL,
        cost_estimate=cost(4 * ranks * tokens * cols, 2 << 20),
    )(proj, query_cotangent, attn_outputs)
    pieces = lax.all_to_all(partial.reshape(fs, 2 * rows, cols), FS, 0, 0)

    held = [packed]
    for step in range(1, tp // 2):
        held.append(lax.ppermute(packed, "tp", [((t + 2 * step) % tp, t) for t in range(tp)]))
    held = jnp.stack(held)
    other = lax.ppermute(held, "tp", [(t ^ 1, t) for t in range(tp)])

    first_new, second_new, low = pl.pallas_call(
        moment_kernel,
        out_shape=(
            jax.ShapeDtypeStruct(first_moment.shape, f32),
            jax.ShapeDtypeStruct(second_moment.shape, f32),
            pltpu.HBM((fs, rows, 2 * cols + 128), bf16),
        ),
        in_specs=[VMEM] * 3,
        out_specs=(VMEM, VMEM, VMEM),
        compiler_params=SMALL,
        cost_estimate=cost(1 << 20, 2 << 20),
    )(pieces, first_moment, second_moment)
    low = lax.all_to_all(low, FS, 0, 0)

    span = width // 6
    per = span // own
    left, right, own_left, own_right = pl.pallas_call(
        functools.partial(prep_kernel, rank_cols),
        grid=(width // span,),
        out_shape=(
            pltpu.HBM((width, ranks), bf16),
            pltpu.HBM((ranks, width), bf16),
            pltpu.HBM((own, ranks), bf16),
            pltpu.HBM((own, ranks), bf16),
        ),
        in_specs=[
            SMEM,
            pl.BlockSpec((tp // 2, per, kept, 128), lambda i: (0, i, 0, 0)),
            pl.BlockSpec((tp // 2, per, kept, 128), lambda i: (0, i, 0, 0)),
        ],
        out_specs=(
            pl.BlockSpec((span, ranks), lambda i: (i, 0)),
            pl.BlockSpec((ranks, span), lambda i: (0, i)),
            pl.BlockSpec((own, ranks), lambda i: (0, 0)),
            pl.BlockSpec((own, ranks), lambda i: (0, 0)),
        ),
        scratch_shapes=[pltpu.VMEM((span, ranks), bf16)],
        compiler_params=SMALL,
        cost_estimate=cost(1 << 30, 30 << 20),
    )(place, far(held), far(other))

    low, masters = lax.optimization_barrier((low, masters))
    squares, first, second, second_turned = pl.pallas_call(
        functools.partial(sums_kernel, rank_cols),
        out_shape=(
            jax.ShapeDtypeStruct((tp, 8, 128), f32),
            jax.ShapeDtypeStruct((ranks, cols), bf16),
            jax.ShapeDtypeStruct((ranks, cols), bf16),
            jax.ShapeDtypeStruct((cols, ranks), bf16),
        ),
        in_specs=[SMEM, VMEM],
        out_specs=(VMEM,) * 4,
        compiler_params=SMALL,
        cost_estimate=LONG,
    )(place, low)
    squares = lax.all_to_all(squares, "tp", 0, 0)

    parts = width // span
    query_copy, out_copy, query_new, out_new = pl.pallas_call(
        functools.partial(final_kernel, float(rows * fs * cols * tp), span),
        out_shape=(
            pltpu.HBM((width, cols), bf16),
            pltpu.HBM((cols, width), bf16),
            pltpu.HBM((own, cols), f32),
            pltpu.HBM((own, cols), f32),
        ),
        in_specs=[VMEM] * 7 + [ANY] * 4,
        out_specs=(ANY,) * 4,
        scratch_shapes=[
            pltpu.VMEM((width, cols), bf16),
            pltpu.VMEM((cols, width), bf16),
            pltpu.VMEM((2, own, ranks), bf16),
            pltpu.VMEM((2, own, cols), f32),
            pltpu.VMEM((2, own, cols), f32),
            pltpu.SemaphoreType.DMA((4,)),
            pltpu.SemaphoreType.DMA((parts, 2)),
            pltpu.SemaphoreType.DMA((2,)),
        ],
        compiler_params=pltpu.CompilerParams(vmem_limit_bytes=32 << 20),
        cost_estimate=cost(4 * width * ranks * cols, 20 << 20),
    )(
        squares,
        first,
        second,
        second_turned,
        left,
        right,
        masters,
        far(own_left),
        far(own_right),
        far(query_master),
        far(out_master.T),
    )
    return (query_new, out_new.T, query_copy, out_copy, first_new, second_new)


def solution(mesh):
    finer = Mesh(mesh.devices.reshape(12, 8, 8), ("z", "y", "tp"))
    both = P(FS, "tp")
    moment = P(None, FS, "tp")

    return jax.shard_map(
        body,
        mesh=finer,
        in_specs=(P(FS, None), both, both, P(FS, None), both, both, both, P("tp", FS), moment, moment),
        out_specs=(both, P("tp", FS), P(None, "tp"), P("tp", None), moment, moment),
        check_vma=False,
    )
```

```python
import functools

import jax
import jax.numpy as jnp
from jax import lax
from jax.experimental import pallas as pl
from jax.experimental.pallas import tpu as pltpu
from jax.sharding import Mesh
from jax.sharding import PartitionSpec as P


bf16 = jnp.bfloat16
f32 = jnp.float32
FS = ("z", "y")
VMEM = pl.BlockSpec(memory_space=pltpu.VMEM)
ANY = pl.BlockSpec(memory_space=pl.ANY)
SMEM = pl.BlockSpec(memory_space=pltpu.SMEM)
REACH = 2.0**34
SMALL = pltpu.CompilerParams(vmem_limit_bytes=16 << 20)


def cost(flops, nbytes):
    return pl.CostEstimate(flops=flops, bytes_accessed=nbytes, transcendentals=0)


LONG = cost(1 << 35, 1 << 26)


def coded(value):
    size = value * REACH
    size = size * size
    size = size * size
    return jnp.where(value < 0.0, -size, size).astype(bf16)


def decoded(code):
    wide = code.astype(f32)
    size = lax.rsqrt(lax.rsqrt(jnp.abs(wide))) * (1.0 / REACH)
    return jnp.where(wide < 0.0, -size, size)


def send_kernel(left, right, query_master, out_master, out, masters):
    own = query_master.shape[0]
    masters[:own] = coded(query_master[...])
    masters[own:] = coded(out_master[...])
    both = jnp.concatenate([left[...].astype(f32), right[...].astype(f32)], axis=1)
    used = both.shape[1]
    free = 128 - used
    kept = out.shape[1]
    rest = both[kept:]
    tail = jnp.concatenate([rest[:, j : j + free] for j in range(0, used, free)], axis=0)
    packed = jnp.concatenate([both[:kept], tail], axis=1).astype(bf16)
    out[...] = jnp.broadcast_to(packed[None], out.shape)


def hold_kernel(masters, packed, out):
    pass


def unpacked(packed, used):
    free = 128 - used
    parts = used // free
    height = packed.shape[1] // parts
    wide = packed.astype(f32)
    tail = [wide[:, j * height : (j + 1) * height, used:] for j in range(parts)]
    tail = jnp.concatenate(tail + [jnp.zeros_like(tail[0])], axis=2)
    return jnp.concatenate([wide, tail], axis=1)


def proj_kernel(used, packed, saved_inputs, out_cotangent, out, factors):
    own = factors.shape[0] // packed.shape[0]
    step = 8
    for i in range(0, packed.shape[0], step):
        block = unpacked(packed[i : i + step], used).reshape(step * own, 128)
        factors[i * own : (i + step) * own] = block.astype(bf16)
    left = jnp.dot(saved_inputs[...], factors[...], preferred_element_type=f32)
    right = jnp.dot(out_cotangent[...], factors[...], preferred_element_type=f32)
    lane = lax.broadcasted_iota(jnp.int32, left.shape, 1)
    out[...] = jnp.where(lane < used // 2, left, right).T[:used].astype(bf16)


def grad_kernel(rank_cols, proj, query_cotangent, attn_outputs, out):
    cols = query_cotangent.shape[1]
    parts = []
    for k, other in enumerate((query_cotangent, attn_outputs)):
        starts = range(k * rank_cols, proj.shape[0], 2 * rank_cols)
        ranks = jnp.concatenate([proj[at : at + rank_cols] for at in starts], axis=0)
        parts.append(jnp.dot(ranks, other[...], preferred_element_type=f32).reshape(-1, 8, cols))
    first, second = parts
    both = jnp.concatenate([first[:, :4], second[:, :4], first[:, 4:], second[:, 4:]], axis=1)
    out[...] = both.astype(bf16)


def moment_kernel(pieces, first, second, first_new, second_new, low):
    rows = first.shape[1]
    grads = jnp.sum(pieces[...].astype(f32), axis=0)
    new_first = 0.9 * jnp.concatenate([first[0], first[1]], axis=0) + 0.1 * grads
    new_second = 0.99 * jnp.concatenate([second[0], second[1]], axis=0) + 0.01 * grads * grads
    direction = new_first / (jnp.sqrt(new_second) + 1e-08)
    first_new[0] = new_first[:rows]
    first_new[1] = new_first[rows:]
    second_new[0] = new_second[:rows]
    second_new[1] = new_second[rows:]
    squares = direction * direction
    lane = lax.broadcasted_iota(jnp.int32, (rows, 128), 1)
    sums = jnp.zeros((rows, 128), f32)
    for k in range(2):
        rest = jnp.sum(squares[k * rows : (k + 1) * rows], axis=(0, 1), keepdims=True)
        for part in range(3):
            rounded = rest.astype(bf16).astype(f32)
            sums = jnp.where(lane == 3 * k + part, rounded, sums)
            rest = rest - rounded
    sent = jnp.concatenate([direction[:rows], direction[rows:], sums], axis=1).astype(bf16)
    low[...] = jnp.broadcast_to(sent[None], low.shape)


def prep_kernel(rank_cols, place, held, other, left, right, own_left, own_right, tile):
    own = own_left.shape[0]
    span = left.shape[0]
    sides = [[], []]
    for half in (held, other):
        for s in range(half.shape[0]):
            block = unpacked(half[s], 2 * rank_cols).reshape(span, 128)
            for k in range(2):
                sides[k].append(block[:, k * rank_cols : (k + 1) * rank_cols])
    both = [jnp.concatenate(side, axis=1).astype(bf16) for side in sides]
    left[...] = both[0]
    right[...] = both[1].T

    @pl.when(pl.program_id(0) == place[0] // (span // own))
    def _():
        rows = pl.ds(pl.multiple_of(place[0] % (span // own) * own, own), own)
        for side, out in zip(both, (own_left, own_right)):
            tile[...] = side
            out[...] = tile[rows]


def sums_kernel(low, squares):
    sums = jnp.sum(low[:, :, -128:].astype(f32), axis=0)[:1]
    squares[...] = jnp.broadcast_to(sums[None], squares.shape)


def final_kernel(
    entries,
    span,
    rank_cols,
    place,
    squares,
    low,
    left,
    right,
    masters,
    own_left,
    own_right,
    query_master,
    out_master,
    query_copy,
    out_copy,
    query_new,
    out_new,
    near_left,
    near_right,
    near_masters,
    near_query,
    near_out,
    near_own,
    near_master,
    near_new,
    first,
    second,
    arrived,
    own_arrived,
    left_for,
    own_left_for,
):
    width = left.shape[0]
    cols = first.shape[1]
    own = query_master.shape[0]
    per = span // own
    parts = width // span
    spans = [pl.ds(i * span, span) for i in range(parts)]
    copies = []
    for i, at in enumerate(spans):
        held = pl.ds(i * per, per)
        ways = (
            (left.at[at], near_left.at[at]),
            (masters.at[held], near_masters.at[held]),
            (right.at[:, at], near_right.at[:, at]),
        )
        copies.append([pltpu.make_async_copy(x, y, arrived.at[i, k]) for k, (x, y) in enumerate(ways)])
    ways = (
        (own_left, near_own.at[0]),
        (own_right, near_own.at[1]),
        (query_master, near_master.at[0]),
        (out_master, near_master.at[1]),
    )
    own_copies = [pltpu.make_async_copy(x, y, own_arrived.at[k]) for k, (x, y) in enumerate(ways)]
    for copy in [c for part in copies for c in part] + own_copies:
        copy.start()

    tp = squares.shape[0]
    per_block = rank_cols // low.shape[1]
    for b in range(tp):
        chip, core = b % (tp // 2), b // (tp // 2)
        at = (place[1] + 2 * chip) % tp
        at = at + core * (1 - 2 * (at % 2))
        block = low[pl.ds(at * per_block, per_block)].astype(f32)
        for k, step in enumerate((first, second)):
            part = block[:, :, k * cols : (k + 1) * cols]
            part = jnp.concatenate([part[j] for j in range(per_block)], axis=0)
            step[b * rank_cols : (b + 1) * rank_cols] = part.astype(bf16)
    second_turned = second[...].T

    sums = jnp.sum(squares[...], axis=0)
    lane = lax.broadcasted_iota(jnp.int32, sums.shape, 1)
    scales = []
    for k in range(2):
        total = jnp.sum(jnp.where(lane // 3 == k, sums, 0.0), axis=1, keepdims=True)
        scales.append(0.01 * lax.rsqrt(total / entries + 1e-06))

    sent = []
    for i, at in enumerate(spans):
        for copy in copies[i]:
            copy.wait()
        codes = near_masters[i * per : (i + 1) * per]
        moved = jnp.dot(near_left[at], first[...], preferred_element_type=f32)
        kept = decoded(codes[:, :own].reshape(span, cols))
        near_query[at] = (kept - scales[0] * moved).astype(bf16)
        sent.append(pltpu.make_async_copy(near_query.at[at], query_copy.at[at], left_for.at[i, 0]))
        sent[-1].start()
        moved = jnp.dot(second_turned, near_right[:, at], preferred_element_type=f32)
        kept = decoded(codes[:, own:].reshape(span, cols).T)
        near_out[:, at] = (kept - scales[1] * moved).astype(bf16)
        sent.append(pltpu.make_async_copy(near_out.at[:, at], out_copy.at[:, at], left_for.at[i, 1]))
        sent[-1].start()
    for copy in own_copies:
        copy.wait()
    for k, (step, new) in enumerate(((first, query_new), (second, out_new))):
        moved = jnp.dot(near_own[k], step[...], preferred_element_type=f32)
        near_new[k] = near_master[k] - scales[k] * moved
        sent.append(pltpu.make_async_copy(near_new.at[k], new, own_left_for.at[k]))
        sent[-1].start()
    for copy in sent:
        copy.wait()


def far(value):
    return pltpu.with_memory_space_constraint(value, pltpu.HBM)


def body(
    saved_inputs,
    query_cotangent,
    attn_outputs,
    out_cotangent,
    left_factor,
    right_factor,
    query_master,
    out_master,
    first_moment,
    second_moment,
):
    fs = lax.axis_size(FS)
    tp = lax.axis_size("tp")
    own, rank_cols = left_factor.shape
    rows = first_moment.shape[1]
    cols = first_moment.shape[2]
    tokens = saved_inputs.shape[0]
    width = fs * own
    ranks = tp * rank_cols
    used = 2 * rank_cols
    kept = own * used // 128

    place = jnp.stack([lax.axis_index(FS), lax.axis_index("tp")]).astype(jnp.int32)
    packed, masters = pl.pallas_call(
        send_kernel,
        out_shape=(jax.ShapeDtypeStruct((fs, kept, 128), bf16), pltpu.HBM((2 * own, cols), bf16)),
        in_specs=[pl.BlockSpec()] * 4,
        out_specs=(VMEM, VMEM),
        compiler_params=SMALL,
        cost_estimate=cost(1 << 16, 1 << 20),
    )(far(left_factor), far(right_factor), far(query_master), far(out_master.T))
    packed = pl.pallas_call(
        hold_kernel,
        out_shape=jax.ShapeDtypeStruct(packed.shape, bf16),
        in_specs=[ANY, ANY],
        out_specs=ANY,
        input_output_aliases={1: 0},
        compiler_params=SMALL,
        cost_estimate=LONG,
    )(far(masters), packed)
    masters = lax.all_gather(masters, FS)
    packed = lax.all_to_all(packed, FS, 0, 0)
    proj = pl.pallas_call(
        functools.partial(proj_kernel, used),
        out_shape=jax.ShapeDtypeStruct((used, tokens), bf16),
        in_specs=[VMEM] * 3,
        out_specs=VMEM,
        scratch_shapes=[pltpu.VMEM((width, 128), bf16)],
        compiler_params=SMALL,
        cost_estimate=cost(4 * tokens * width * 128, 8 << 20),
    )(packed, saved_inputs, out_cotangent)
    proj = lax.all_gather(proj, "tp", axis=0, tiled=True)

    partial = pl.pallas_call(
        functools.partial(grad_kernel, rank_cols),
        out_shape=pltpu.HBM((fs // 2, 4 * rows, cols), bf16),
        in_specs=[VMEM] * 3,
        out_specs=VMEM,
        compiler_params=SMALL,
        cost_estimate=cost(4 * ranks * tokens * cols, 2 << 20),
    )(proj, query_cotangent, attn_outputs)
    pieces = lax.all_to_all(partial.reshape(fs, 2 * rows, cols), FS, 0, 0)

    held = [packed]
    for step in range(1, tp // 2):
        held.append(lax.ppermute(packed, "tp", [((t + 2 * step) % tp, t) for t in range(tp)]))
    held = jnp.stack(held)
    other = lax.ppermute(held, "tp", [(t ^ 1, t) for t in range(tp)])

    first_new, second_new, low = pl.pallas_call(
        moment_kernel,
        out_shape=(
            jax.ShapeDtypeStruct(first_moment.shape, f32),
            jax.ShapeDtypeStruct(second_moment.shape, f32),
            pltpu.HBM((fs, rows, 2 * cols + 128), bf16),
        ),
        in_specs=[VMEM] * 3,
        out_specs=(VMEM, VMEM, VMEM),
        compiler_params=SMALL,
        cost_estimate=cost(1 << 20, 2 << 20),
    )(pieces, first_moment, second_moment)
    low = lax.all_to_all(low, FS, 0, 0)

    span = width // 6
    per = span // own
    left, right, own_left, own_right = pl.pallas_call(
        functools.partial(prep_kernel, rank_cols),
        grid=(width // span,),
        out_shape=(
            pltpu.HBM((width, ranks), bf16),
            pltpu.HBM((ranks, width), bf16),
            pltpu.HBM((own, ranks), bf16),
            pltpu.HBM((own, ranks), bf16),
        ),
        in_specs=[
            SMEM,
            pl.BlockSpec((tp // 2, per, kept, 128), lambda i: (0, i, 0, 0)),
            pl.BlockSpec((tp // 2, per, kept, 128), lambda i: (0, i, 0, 0)),
        ],
        out_specs=(
            pl.BlockSpec((span, ranks), lambda i: (i, 0)),
            pl.BlockSpec((ranks, span), lambda i: (0, i)),
            pl.BlockSpec((own, ranks), lambda i: (0, 0)),
            pl.BlockSpec((own, ranks), lambda i: (0, 0)),
        ),
        scratch_shapes=[pltpu.VMEM((span, ranks), bf16)],
        compiler_params=SMALL,
        cost_estimate=cost(1 << 30, 30 << 20),
    )(place, far(held), far(other))

    squares = pl.pallas_call(
        sums_kernel,
        out_shape=jax.ShapeDtypeStruct((tp, 1, 128), f32),
        in_specs=[VMEM],
        out_specs=VMEM,
        compiler_params=SMALL,
        cost_estimate=LONG,
    )(low)
    squares = lax.all_to_all(squares, "tp", 0, 0)

    parts = width // span
    query_copy, out_copy, query_new, out_new = pl.pallas_call(
        functools.partial(final_kernel, float(rows * fs * cols * tp), span, rank_cols),
        out_shape=(
            pltpu.HBM((width, cols), bf16),
            pltpu.HBM((cols, width), bf16),
            pltpu.HBM((own, cols), f32),
            pltpu.HBM((own, cols), f32),
        ),
        in_specs=[SMEM] + [VMEM] * 2 + [ANY] * 7,
        out_specs=(ANY,) * 4,
        scratch_shapes=[
            pltpu.VMEM((width, ranks), bf16),
            pltpu.VMEM((ranks, width), bf16),
            pltpu.VMEM(masters.shape, bf16),
            pltpu.VMEM((width, cols), bf16),
            pltpu.VMEM((cols, width), bf16),
            pltpu.VMEM((2, own, ranks), bf16),
            pltpu.VMEM((2, own, cols), f32),
            pltpu.VMEM((2, own, cols), f32),
            pltpu.VMEM((ranks, cols), bf16),
            pltpu.VMEM((ranks, cols), bf16),
            pltpu.SemaphoreType.DMA((parts, 3)),
            pltpu.SemaphoreType.DMA((4,)),
            pltpu.SemaphoreType.DMA((parts, 2)),
            pltpu.SemaphoreType.DMA((2,)),
        ],
        compiler_params=pltpu.CompilerParams(vmem_limit_bytes=32 << 20),
        cost_estimate=cost(4 * width * ranks * cols, 20 << 20),
    )(
        place,
        squares,
        low,
        far(left),
        far(right),
        far(masters),
        far(own_left),
        far(own_right),
        far(query_master),
        far(out_master.T),
    )
    return (query_new, out_new.T, query_copy, out_copy, first_new, second_new)


def solution(mesh):
    finer = Mesh(mesh.devices.reshape(12, 8, 8), ("z", "y", "tp"))
    both = P(FS, "tp")
    moment = P(None, FS, "tp")

    return jax.shard_map(
        body,
        mesh=finer,
        in_specs=(P(FS, None), both, both, P(FS, None), both, both, both, P("tp", FS), moment, moment),
        out_specs=(both, P("tp", FS), P(None, "tp"), P("tp", None), moment, moment),
        check_vma=False,
    )
```

```python
import functools

import jax
import jax.numpy as jnp
from jax import lax
from jax.experimental import pallas as pl
from jax.experimental.pallas import tpu as pltpu
from jax.sharding import Mesh
from jax.sharding import PartitionSpec as P


bf16 = jnp.bfloat16
f32 = jnp.float32
FS = ("z", "y")
VMEM = pl.BlockSpec(memory_space=pltpu.VMEM)
ANY = pl.BlockSpec(memory_space=pl.ANY)
SMEM = pl.BlockSpec(memory_space=pltpu.SMEM)
REACH = 2.0**34
SMALL = pltpu.CompilerParams(vmem_limit_bytes=16 << 20)


def cost(flops, nbytes):
    return pl.CostEstimate(flops=flops, bytes_accessed=nbytes, transcendentals=0)


LONG = cost(1 << 35, 1 << 26)


def coded(value):
    size = value * REACH
    size = size * size
    size = size * size
    return jnp.where(value < 0.0, -size, size).astype(bf16)


def decoded(code):
    wide = code.astype(f32)
    size = lax.rsqrt(lax.rsqrt(jnp.abs(wide))) * (1.0 / REACH)
    return jnp.where(wide < 0.0, -size, size)


def send_kernel(left, right, query_master, out_master, out, masters):
    own = query_master.shape[0]
    masters[:own] = coded(query_master[...])
    masters[own:] = coded(out_master[...])
    both = jnp.concatenate([left[...].astype(f32), right[...].astype(f32)], axis=1)
    used = both.shape[1]
    free = 128 - used
    kept = out.shape[1]
    rest = both[kept:]
    tail = jnp.concatenate([rest[:, j : j + free] for j in range(0, used, free)], axis=0)
    packed = jnp.concatenate([both[:kept], tail], axis=1).astype(bf16)
    out[...] = jnp.broadcast_to(packed[None], out.shape)


def hold_kernel(masters, packed, out):
    pass


def unpacked(packed, used):
    free = 128 - used
    parts = used // free
    height = packed.shape[1] // parts
    wide = packed.astype(f32)
    tail = [wide[:, j * height : (j + 1) * height, used:] for j in range(parts)]
    tail = jnp.concatenate(tail + [jnp.zeros_like(tail[0])], axis=2)
    return jnp.concatenate([wide, tail], axis=1)


def proj_kernel(used, packed, saved_inputs, out_cotangent, out, factors):
    own = factors.shape[0] // packed.shape[0]
    step = 8
    for i in range(0, packed.shape[0], step):
        block = unpacked(packed[i : i + step], used).reshape(step * own, 128)
        factors[i * own : (i + step) * own] = block.astype(bf16)
    left = jnp.dot(saved_inputs[...], factors[...], preferred_element_type=f32)
    right = jnp.dot(out_cotangent[...], factors[...], preferred_element_type=f32)
    lane = lax.broadcasted_iota(jnp.int32, left.shape, 1)
    out[...] = jnp.where(lane < used // 2, left, right).T[:used].astype(bf16)


def grad_kernel(rank_cols, proj, query_cotangent, attn_outputs, out):
    cols = query_cotangent.shape[1]
    parts = []
    for k, other in enumerate((query_cotangent, attn_outputs)):
        starts = range(k * rank_cols, proj.shape[0], 2 * rank_cols)
        ranks = jnp.concatenate([proj[at : at + rank_cols] for at in starts], axis=0)
        parts.append(jnp.dot(ranks, other[...], preferred_element_type=f32).reshape(-1, 8, cols))
    first, second = parts
    both = jnp.concatenate([first[:, :4], second[:, :4], first[:, 4:], second[:, 4:]], axis=1)
    out[...] = both.astype(bf16)


def moment_kernel(pieces, first, second, first_new, second_new, low):
    rows = first.shape[1]
    grads = jnp.sum(pieces[...].astype(f32), axis=0)
    new_first = 0.9 * jnp.concatenate([first[0], first[1]], axis=0) + 0.1 * grads
    new_second = 0.99 * jnp.concatenate([second[0], second[1]], axis=0) + 0.01 * grads * grads
    direction = new_first / (jnp.sqrt(new_second) + 1e-08)
    first_new[0] = new_first[:rows]
    first_new[1] = new_first[rows:]
    second_new[0] = new_second[:rows]
    second_new[1] = new_second[rows:]
    squares = direction * direction
    lane = lax.broadcasted_iota(jnp.int32, (rows, 128), 1)
    sums = jnp.zeros((rows, 128), f32)
    for k in range(2):
        rest = jnp.sum(squares[k * rows : (k + 1) * rows], axis=(0, 1), keepdims=True)
        for part in range(3):
            rounded = rest.astype(bf16).astype(f32)
            sums = jnp.where(lane == 3 * k + part, rounded, sums)
            rest = rest - rounded
    sent = jnp.concatenate([direction[:rows], direction[rows:], sums], axis=1).astype(bf16)
    low[...] = jnp.broadcast_to(sent[None], low.shape)


def prep_kernel(rank_cols, place, held, other, left, right, own_left, own_right, tile):
    own = own_left.shape[0]
    span = left.shape[0]
    sides = [[], []]
    for half in (held, other):
        for s in range(half.shape[0]):
            block = unpacked(half[s], 2 * rank_cols).reshape(span, 128)
            for k in range(2):
                sides[k].append(block[:, k * rank_cols : (k + 1) * rank_cols])
    both = [jnp.concatenate(side, axis=1).astype(bf16) for side in sides]
    left[...] = both[0]
    right[...] = both[1].T

    @pl.when(pl.program_id(0) == place[0] // (span // own))
    def _():
        rows = pl.ds(pl.multiple_of(place[0] % (span // own) * own, own), own)
        for side, out in zip(both, (own_left, own_right)):
            tile[...] = side
            out[...] = tile[rows]


def spread_kernel(low, out):
    out[...] = jnp.broadcast_to(low[...][None], out.shape)


def sums_kernel(low, squares):
    sums = jnp.sum(low[:, :, :, -128:].astype(f32), axis=(0, 1))[:1]
    squares[...] = jnp.broadcast_to(sums[None], squares.shape)


def final_kernel(
    entries,
    span,
    rank_cols,
    place,
    squares,
    low,
    left,
    right,
    masters,
    own_left,
    own_right,
    query_master,
    out_master,
    query_copy,
    out_copy,
    query_new,
    out_new,
    near_left,
    near_right,
    near_masters,
    near_query,
    near_out,
    near_own,
    near_master,
    near_new,
    first,
    second,
    arrived,
    own_arrived,
    left_for,
    own_left_for,
):
    width = left.shape[0]
    cols = first.shape[1]
    own = query_master.shape[0]
    per = span // own
    parts = width // span
    spans = [pl.ds(i * span, span) for i in range(parts)]
    copies = []
    for i, at in enumerate(spans):
        held = pl.ds(i * per, per)
        ways = (
            (left.at[at], near_left.at[at]),
            (masters.at[held], near_masters.at[held]),
            (right.at[:, at], near_right.at[:, at]),
        )
        copies.append([pltpu.make_async_copy(x, y, arrived.at[i, k]) for k, (x, y) in enumerate(ways)])
    ways = (
        (own_left, near_own.at[0]),
        (own_right, near_own.at[1]),
        (query_master, near_master.at[0]),
        (out_master, near_master.at[1]),
    )
    own_copies = [pltpu.make_async_copy(x, y, own_arrived.at[k]) for k, (x, y) in enumerate(ways)]
    for copy in [c for part in copies for c in part] + own_copies:
        copy.start()

    tp = squares.shape[0]
    height = low.shape[0]
    per_block = rank_cols // low.shape[2]
    for b in range(tp):
        chip, core = b % (tp // 2), b // (tp // 2)
        at = (place[1] + 2 * chip) % tp
        at = at + core * (1 - 2 * (at % 2))
        held = [at * per_block + j for j in range(per_block)]
        block = [low[j % height, j // height].astype(f32) for j in held]
        for k, step in enumerate((first, second)):
            part = jnp.concatenate([piece[:, k * cols : (k + 1) * cols] for piece in block], axis=0)
            step[b * rank_cols : (b + 1) * rank_cols] = part.astype(bf16)
    second_turned = second[...].T

    sums = jnp.sum(squares[...], axis=0)
    lane = lax.broadcasted_iota(jnp.int32, sums.shape, 1)
    scales = []
    for k in range(2):
        total = jnp.sum(jnp.where(lane // 3 == k, sums, 0.0), axis=1, keepdims=True)
        scales.append(0.01 * lax.rsqrt(total / entries + 1e-06))

    sent = []
    for i, at in enumerate(spans):
        for copy in copies[i]:
            copy.wait()
        codes = near_masters[i * per : (i + 1) * per]
        moved = jnp.dot(near_left[at], first[...], preferred_element_type=f32)
        kept = decoded(codes[:, :own].reshape(span, cols))
        near_query[at] = (kept - scales[0] * moved).astype(bf16)
        sent.append(pltpu.make_async_copy(near_query.at[at], query_copy.at[at], left_for.at[i, 0]))
        sent[-1].start()
        moved = jnp.dot(second_turned, near_right[:, at], preferred_element_type=f32)
        kept = decoded(codes[:, own:].reshape(span, cols).T)
        near_out[:, at] = (kept - scales[1] * moved).astype(bf16)
        sent.append(pltpu.make_async_copy(near_out.at[:, at], out_copy.at[:, at], left_for.at[i, 1]))
        sent[-1].start()
    for copy in own_copies:
        copy.wait()
    for k, (step, new) in enumerate(((first, query_new), (second, out_new))):
        moved = jnp.dot(near_own[k], step[...], preferred_element_type=f32)
        near_new[k] = near_master[k] - scales[k] * moved
        sent.append(pltpu.make_async_copy(near_new.at[k], new, own_left_for.at[k]))
        sent[-1].start()
    for copy in sent:
        copy.wait()


def far(value):
    return pltpu.with_memory_space_constraint(value, pltpu.HBM)


def body(
    saved_inputs,
    query_cotangent,
    attn_outputs,
    out_cotangent,
    left_factor,
    right_factor,
    query_master,
    out_master,
    first_moment,
    second_moment,
):
    depth = lax.axis_size("z")
    height = lax.axis_size("y")
    fs = depth * height
    tp = lax.axis_size("tp")
    own, rank_cols = left_factor.shape
    rows = first_moment.shape[1]
    cols = first_moment.shape[2]
    tokens = saved_inputs.shape[0]
    width = fs * own
    ranks = tp * rank_cols
    used = 2 * rank_cols
    kept = own * used // 128

    place = jnp.stack([lax.axis_index(FS), lax.axis_index("tp")]).astype(jnp.int32)
    packed, masters = pl.pallas_call(
        send_kernel,
        out_shape=(jax.ShapeDtypeStruct((fs, kept, 128), bf16), pltpu.HBM((2 * own, cols), bf16)),
        in_specs=[pl.BlockSpec()] * 4,
        out_specs=(VMEM, VMEM),
        compiler_params=SMALL,
        cost_estimate=cost(1 << 16, 1 << 20),
    )(far(left_factor), far(right_factor), far(query_master), far(out_master.T))
    packed = pl.pallas_call(
        hold_kernel,
        out_shape=jax.ShapeDtypeStruct(packed.shape, bf16),
        in_specs=[ANY, ANY],
        out_specs=ANY,
        input_output_aliases={1: 0},
        compiler_params=SMALL,
        cost_estimate=LONG,
    )(far(masters), packed)
    masters = lax.all_gather(masters, FS)
    packed = lax.all_to_all(packed, FS, 0, 0)
    proj = pl.pallas_call(
        functools.partial(proj_kernel, used),
        out_shape=jax.ShapeDtypeStruct((used, tokens), bf16),
        in_specs=[VMEM] * 3,
        out_specs=VMEM,
        scratch_shapes=[pltpu.VMEM((width, 128), bf16)],
        compiler_params=SMALL,
        cost_estimate=cost(4 * tokens * width * 128, 8 << 20),
    )(packed, saved_inputs, out_cotangent)
    proj = lax.all_gather(proj, "tp", axis=0, tiled=True)

    partial = pl.pallas_call(
        functools.partial(grad_kernel, rank_cols),
        out_shape=pltpu.HBM((fs // 2, 4 * rows, cols), bf16),
        in_specs=[VMEM] * 3,
        out_specs=VMEM,
        compiler_params=SMALL,
        cost_estimate=cost(4 * ranks * tokens * cols, 2 << 20),
    )(proj, query_cotangent, attn_outputs)
    pieces = lax.all_to_all(partial.reshape(fs, 2 * rows, cols), FS, 0, 0)

    held = [packed]
    for step in range(1, tp // 2):
        held.append(lax.ppermute(packed, "tp", [((t + 2 * step) % tp, t) for t in range(tp)]))
    held = jnp.stack(held)
    other = lax.ppermute(held, "tp", [(t ^ 1, t) for t in range(tp)])

    first_new, second_new, low = pl.pallas_call(
        moment_kernel,
        out_shape=(
            jax.ShapeDtypeStruct(first_moment.shape, f32),
            jax.ShapeDtypeStruct(second_moment.shape, f32),
            pltpu.HBM((depth, rows, 2 * cols + 128), bf16),
        ),
        in_specs=[VMEM] * 3,
        out_specs=(VMEM, VMEM, VMEM),
        compiler_params=SMALL,
        cost_estimate=cost(1 << 20, 2 << 20),
    )(pieces, first_moment, second_moment)
    low = lax.all_to_all(low, "z", 0, 0)
    low = pl.pallas_call(
        spread_kernel,
        out_shape=pltpu.HBM((height, *low.shape), bf16),
        in_specs=[VMEM],
        out_specs=VMEM,
        compiler_params=SMALL,
        cost_estimate=cost(1 << 16, 1 << 20),
    )(low)
    low = lax.all_to_all(low, "y", 0, 0)

    span = width // 6
    per = span // own
    left, right, own_left, own_right = pl.pallas_call(
        functools.partial(prep_kernel, rank_cols),
        grid=(width // span,),
        out_shape=(
            pltpu.HBM((width, ranks), bf16),
            pltpu.HBM((ranks, width), bf16),
            pltpu.HBM((own, ranks), bf16),
            pltpu.HBM((own, ranks), bf16),
        ),
        in_specs=[
            SMEM,
            pl.BlockSpec((tp // 2, per, kept, 128), lambda i: (0, i, 0, 0)),
            pl.BlockSpec((tp // 2, per, kept, 128), lambda i: (0, i, 0, 0)),
        ],
        out_specs=(
            pl.BlockSpec((span, ranks), lambda i: (i, 0)),
            pl.BlockSpec((ranks, span), lambda i: (0, i)),
            pl.BlockSpec((own, ranks), lambda i: (0, 0)),
            pl.BlockSpec((own, ranks), lambda i: (0, 0)),
        ),
        scratch_shapes=[pltpu.VMEM((span, ranks), bf16)],
        compiler_params=SMALL,
        cost_estimate=cost(1 << 30, 30 << 20),
    )(place, far(held), far(other))

    squares = pl.pallas_call(
        sums_kernel,
        out_shape=jax.ShapeDtypeStruct((tp, 1, 128), f32),
        in_specs=[VMEM],
        out_specs=VMEM,
        compiler_params=SMALL,
        cost_estimate=LONG,
    )(low)
    squares = lax.all_to_all(squares, "tp", 0, 0)

    parts = width // span
    query_copy, out_copy, query_new, out_new = pl.pallas_call(
        functools.partial(final_kernel, float(rows * fs * cols * tp), span, rank_cols),
        out_shape=(
            pltpu.HBM((width, cols), bf16),
            pltpu.HBM((cols, width), bf16),
            pltpu.HBM((own, cols), f32),
            pltpu.HBM((own, cols), f32),
        ),
        in_specs=[SMEM] + [VMEM] * 2 + [ANY] * 7,
        out_specs=(ANY,) * 4,
        scratch_shapes=[
            pltpu.VMEM((width, ranks), bf16),
            pltpu.VMEM((ranks, width), bf16),
            pltpu.VMEM(masters.shape, bf16),
            pltpu.VMEM((width, cols), bf16),
            pltpu.VMEM((cols, width), bf16),
            pltpu.VMEM((2, own, ranks), bf16),
            pltpu.VMEM((2, own, cols), f32),
            pltpu.VMEM((2, own, cols), f32),
            pltpu.VMEM((ranks, cols), bf16),
            pltpu.VMEM((ranks, cols), bf16),
            pltpu.SemaphoreType.DMA((parts, 3)),
            pltpu.SemaphoreType.DMA((4,)),
            pltpu.SemaphoreType.DMA((parts, 2)),
            pltpu.SemaphoreType.DMA((2,)),
        ],
        compiler_params=pltpu.CompilerParams(vmem_limit_bytes=32 << 20),
        cost_estimate=cost(4 * width * ranks * cols, 20 << 20),
    )(
        place,
        squares,
        low,
        far(left),
        far(right),
        far(masters),
        far(own_left),
        far(own_right),
        far(query_master),
        far(out_master.T),
    )
    return (query_new, out_new.T, query_copy, out_copy, first_new, second_new)


def solution(mesh):
    finer = Mesh(mesh.devices.reshape(12, 8, 8), ("z", "y", "tp"))
    both = P(FS, "tp")
    moment = P(None, FS, "tp")

    return jax.shard_map(
        body,
        mesh=finer,
        in_specs=(P(FS, None), both, both, P(FS, None), both, both, both, P("tp", FS), moment, moment),
        out_specs=(both, P("tp", FS), P(None, "tp"), P("tp", None), moment, moment),
        check_vma=False,
    )
```

```python
import functools

import jax
import jax.numpy as jnp
from jax import lax
from jax.experimental import pallas as pl
from jax.experimental.pallas import tpu as pltpu
from jax.sharding import Mesh
from jax.sharding import PartitionSpec as P


bf16 = jnp.bfloat16
f32 = jnp.float32
FS = ("z", "y")
VMEM = pl.BlockSpec(memory_space=pltpu.VMEM)
ANY = pl.BlockSpec(memory_space=pl.ANY)
SMEM = pl.BlockSpec(memory_space=pltpu.SMEM)
REACH = 2.0**34
SMALL = pltpu.CompilerParams(vmem_limit_bytes=16 << 20)


def cost(flops, nbytes):
    return pl.CostEstimate(flops=flops, bytes_accessed=nbytes, transcendentals=0)


LONG = cost(1 << 35, 1 << 26)


def coded(value):
    size = value * REACH
    size = size * size
    size = size * size
    return jnp.where(value < 0.0, -size, size).astype(bf16)


def decoded(code):
    wide = code.astype(f32)
    size = lax.rsqrt(lax.rsqrt(jnp.abs(wide))) * (1.0 / REACH)
    return jnp.where(wide < 0.0, -size, size)


def send_kernel(left, right, query_master, out_master, out, masters):
    own = query_master.shape[0]
    masters[:own] = coded(query_master[...])
    masters[own:] = coded(out_master[...])
    both = jnp.concatenate([left[...].astype(f32), right[...].astype(f32)], axis=1)
    used = both.shape[1]
    free = 128 - used
    kept = out.shape[1]
    rest = both[kept:]
    tail = jnp.concatenate([rest[:, j : j + free] for j in range(0, used, free)], axis=0)
    packed = jnp.concatenate([both[:kept], tail], axis=1).astype(bf16)
    out[...] = jnp.broadcast_to(packed[None], out.shape)


def hold_kernel(masters, packed, out):
    pass


def unpacked(packed, used):
    free = 128 - used
    parts = used // free
    height = packed.shape[1] // parts
    wide = packed.astype(f32)
    tail = [wide[:, j * height : (j + 1) * height, used:] for j in range(parts)]
    tail = jnp.concatenate(tail + [jnp.zeros_like(tail[0])], axis=2)
    return jnp.concatenate([wide, tail], axis=1)


def proj_kernel(used, packed, saved_inputs, out_cotangent, out, factors):
    own = factors.shape[0] // packed.shape[0]
    step = 8
    for i in range(0, packed.shape[0], step):
        block = unpacked(packed[i : i + step], used).reshape(step * own, 128)
        factors[i * own : (i + step) * own] = block.astype(bf16)
    left = jnp.dot(saved_inputs[...], factors[...], preferred_element_type=f32)
    right = jnp.dot(out_cotangent[...], factors[...], preferred_element_type=f32)
    lane = lax.broadcasted_iota(jnp.int32, left.shape, 1)
    out[...] = jnp.where(lane < used // 2, left, right).T[:used].astype(bf16)


def grad_kernel(rank_cols, proj, query_cotangent, attn_outputs, out):
    cols = query_cotangent.shape[1]
    parts = []
    for k, other in enumerate((query_cotangent, attn_outputs)):
        starts = range(k * rank_cols, proj.shape[0], 2 * rank_cols)
        ranks = jnp.concatenate([proj[at : at + rank_cols] for at in starts], axis=0)
        parts.append(jnp.dot(ranks, other[...], preferred_element_type=f32).reshape(-1, 8, cols))
    first, second = parts
    both = jnp.concatenate([first[:, :4], second[:, :4], first[:, 4:], second[:, 4:]], axis=1)
    out[...] = both.astype(bf16)


def moment_kernel(pieces, first, second, first_new, second_new, low):
    rows = first.shape[1]
    grads = jnp.sum(pieces[...].astype(f32), axis=0)
    new_first = 0.9 * jnp.concatenate([first[0], first[1]], axis=0) + 0.1 * grads
    new_second = 0.99 * jnp.concatenate([second[0], second[1]], axis=0) + 0.01 * grads * grads
    direction = new_first / (jnp.sqrt(new_second) + 1e-08)
    first_new[0] = new_first[:rows]
    first_new[1] = new_first[rows:]
    second_new[0] = new_second[:rows]
    second_new[1] = new_second[rows:]
    squares = direction * direction
    lane = lax.broadcasted_iota(jnp.int32, (rows, 128), 1)
    sums = jnp.zeros((rows, 128), f32)
    for k in range(2):
        rest = jnp.sum(squares[k * rows : (k + 1) * rows], axis=(0, 1), keepdims=True)
        for part in range(3):
            rounded = rest.astype(bf16).astype(f32)
            sums = jnp.where(lane == 3 * k + part, rounded, sums)
            rest = rest - rounded
    sent = jnp.concatenate([direction[:rows], direction[rows:], sums], axis=1).astype(bf16)
    low[...] = jnp.broadcast_to(sent[None], low.shape)


def prep_kernel(rank_cols, place, held, other, left, right, own_left, own_right, tile):
    own = own_left.shape[0]
    span = left.shape[0]
    sides = [[], []]
    for half in (held, other):
        for s in range(half.shape[0]):
            block = unpacked(half[s], 2 * rank_cols).reshape(span, 128)
            for k in range(2):
                sides[k].append(block[:, k * rank_cols : (k + 1) * rank_cols])
    both = [jnp.concatenate(side, axis=1).astype(bf16) for side in sides]
    left[...] = both[0]
    right[...] = both[1].T

    @pl.when(pl.program_id(0) == place[0] // (span // own))
    def _():
        rows = pl.ds(pl.multiple_of(place[0] % (span // own) * own, own), own)
        for side, out in zip(both, (own_left, own_right)):
            tile[...] = side
            out[...] = tile[rows]


def decode_kernel(span, masters, query_all, out_all, near, near_query, near_out, arrived, left_for):
    own = masters.shape[1] // 2
    cols = masters.shape[2]
    per = span // own
    parts = masters.shape[0] // per
    copies = []
    for i in range(parts):
        held = pl.ds(i * per, per)
        copies.append(pltpu.make_async_copy(masters.at[held], near.at[held], arrived.at[i]))
        copies[-1].start()
    sent = []
    for i in range(parts):
        at = pl.ds(i * span, span)
        copies[i].wait()
        codes = near[i * per : (i + 1) * per]
        near_query[at] = decoded(codes[:, :own].reshape(span, cols))
        sent.append(pltpu.make_async_copy(near_query.at[at], query_all.at[at], left_for.at[i, 0]))
        sent[-1].start()
        near_out[:, at] = decoded(codes[:, own:].reshape(span, cols).T)
        sent.append(pltpu.make_async_copy(near_out.at[:, at], out_all.at[:, at], left_for.at[i, 1]))
        sent[-1].start()
    for copy in sent:
        copy.wait()


def spread_kernel(low, out):
    out[...] = jnp.broadcast_to(low[...][None], out.shape)


def sums_kernel(low, squares):
    sums = jnp.sum(low[:, :, :, -128:].astype(f32), axis=(0, 1))[:1]
    squares[...] = jnp.broadcast_to(sums[None], squares.shape)


def final_kernel(
    entries,
    span,
    rank_cols,
    place,
    squares,
    low,
    left,
    right,
    query_all,
    out_all,
    own_left,
    own_right,
    query_master,
    out_master,
    query_copy,
    out_copy,
    query_new,
    out_new,
    near_query,
    near_out,
    near_own,
    near_master,
    near_new,
    first,
    second,
    own_arrived,
    left_for,
    own_left_for,
):
    width = left.shape[0]
    cols = first.shape[1]
    parts = width // span
    ways = (
        (own_left, near_own.at[0]),
        (own_right, near_own.at[1]),
        (query_master, near_master.at[0]),
        (out_master, near_master.at[1]),
    )
    own_copies = [pltpu.make_async_copy(x, y, own_arrived.at[k]) for k, (x, y) in enumerate(ways)]
    for copy in own_copies:
        copy.start()

    tp = squares.shape[0]
    height = low.shape[0]
    per_block = rank_cols // low.shape[2]
    for b in range(tp):
        chip, core = b % (tp // 2), b // (tp // 2)
        at = (place[1] + 2 * chip) % tp
        at = at + core * (1 - 2 * (at % 2))
        held = [at * per_block + j for j in range(per_block)]
        block = [low[j % height, j // height].astype(f32) for j in held]
        for k, step in enumerate((first, second)):
            part = jnp.concatenate([piece[:, k * cols : (k + 1) * cols] for piece in block], axis=0)
            step[b * rank_cols : (b + 1) * rank_cols] = part.astype(bf16)
    second_turned = second[...].T

    sums = jnp.sum(squares[...], axis=0)
    lane = lax.broadcasted_iota(jnp.int32, sums.shape, 1)
    scales = []
    for k in range(2):
        total = jnp.sum(jnp.where(lane // 3 == k, sums, 0.0), axis=1, keepdims=True)
        scales.append(0.01 * lax.rsqrt(total / entries + 1e-06))

    sent = []
    for i in range(parts):
        at = pl.ds(i * span, span)
        moved = jnp.dot(left[at], first[...], preferred_element_type=f32)
        near_query[at] = (query_all[at] - scales[0] * moved).astype(bf16)
        sent.append(pltpu.make_async_copy(near_query.at[at], query_copy.at[at], left_for.at[i, 0]))
        sent[-1].start()
        moved = jnp.dot(second_turned, right[:, at], preferred_element_type=f32)
        near_out[:, at] = (out_all[:, at] - scales[1] * moved).astype(bf16)
        sent.append(pltpu.make_async_copy(near_out.at[:, at], out_copy.at[:, at], left_for.at[i, 1]))
        sent[-1].start()
    for copy in own_copies:
        copy.wait()
    for k, (step, new) in enumerate(((first, query_new), (second, out_new))):
        moved = jnp.dot(near_own[k], step[...], preferred_element_type=f32)
        near_new[k] = near_master[k] - scales[k] * moved
        sent.append(pltpu.make_async_copy(near_new.at[k], new, own_left_for.at[k]))
        sent[-1].start()
    for copy in sent:
        copy.wait()


def far(value):
    return pltpu.with_memory_space_constraint(value, pltpu.HBM)


def body(
    saved_inputs,
    query_cotangent,
    attn_outputs,
    out_cotangent,
    left_factor,
    right_factor,
    query_master,
    out_master,
    first_moment,
    second_moment,
):
    depth = lax.axis_size("z")
    height = lax.axis_size("y")
    fs = depth * height
    tp = lax.axis_size("tp")
    own, rank_cols = left_factor.shape
    rows = first_moment.shape[1]
    cols = first_moment.shape[2]
    tokens = saved_inputs.shape[0]
    width = fs * own
    ranks = tp * rank_cols
    used = 2 * rank_cols
    kept = own * used // 128

    place = jnp.stack([lax.axis_index(FS), lax.axis_index("tp")]).astype(jnp.int32)
    packed, masters = pl.pallas_call(
        send_kernel,
        out_shape=(jax.ShapeDtypeStruct((fs, kept, 128), bf16), pltpu.HBM((2 * own, cols), bf16)),
        in_specs=[pl.BlockSpec()] * 4,
        out_specs=(VMEM, VMEM),
        compiler_params=SMALL,
        cost_estimate=cost(1 << 16, 1 << 20),
    )(far(left_factor), far(right_factor), far(query_master), far(out_master.T))
    packed = pl.pallas_call(
        hold_kernel,
        out_shape=jax.ShapeDtypeStruct(packed.shape, bf16),
        in_specs=[ANY, ANY],
        out_specs=ANY,
        input_output_aliases={1: 0},
        compiler_params=SMALL,
        cost_estimate=LONG,
    )(far(masters), packed)
    masters = lax.all_gather(masters, FS)
    packed = lax.all_to_all(packed, FS, 0, 0)
    proj = pl.pallas_call(
        functools.partial(proj_kernel, used),
        out_shape=jax.ShapeDtypeStruct((used, tokens), bf16),
        in_specs=[VMEM] * 3,
        out_specs=VMEM,
        scratch_shapes=[pltpu.VMEM((width, 128), bf16)],
        compiler_params=SMALL,
        cost_estimate=cost(4 * tokens * width * 128, 8 << 20),
    )(packed, saved_inputs, out_cotangent)
    proj = lax.all_gather(proj, "tp", axis=0, tiled=True)

    partial = pl.pallas_call(
        functools.partial(grad_kernel, rank_cols),
        out_shape=pltpu.HBM((fs // 2, 4 * rows, cols), bf16),
        in_specs=[VMEM] * 3,
        out_specs=VMEM,
        compiler_params=SMALL,
        cost_estimate=cost(4 * ranks * tokens * cols, 2 << 20),
    )(proj, query_cotangent, attn_outputs)
    pieces = lax.all_to_all(partial.reshape(fs, 2 * rows, cols), FS, 0, 0)

    held = [packed]
    for step in range(1, tp // 2):
        held.append(lax.ppermute(packed, "tp", [((t + 2 * step) % tp, t) for t in range(tp)]))
    held = jnp.stack(held)
    other = lax.ppermute(held, "tp", [(t ^ 1, t) for t in range(tp)])

    first_new, second_new, low = pl.pallas_call(
        moment_kernel,
        out_shape=(
            jax.ShapeDtypeStruct(first_moment.shape, f32),
            jax.ShapeDtypeStruct(second_moment.shape, f32),
            pltpu.HBM((depth, rows, 2 * cols + 128), bf16),
        ),
        in_specs=[VMEM] * 3,
        out_specs=(VMEM, VMEM, VMEM),
        compiler_params=SMALL,
        cost_estimate=cost(1 << 20, 2 << 20),
    )(pieces, first_moment, second_moment)
    low = lax.all_to_all(low, "z", 0, 0)
    low = pl.pallas_call(
        spread_kernel,
        out_shape=pltpu.HBM((height, *low.shape), bf16),
        in_specs=[VMEM],
        out_specs=VMEM,
        compiler_params=SMALL,
        cost_estimate=cost(1 << 16, 1 << 20),
    )(low)
    low = lax.all_to_all(low, "y", 0, 0)

    span = width // 6
    per = span // own
    left, right, own_left, own_right = pl.pallas_call(
        functools.partial(prep_kernel, rank_cols),
        grid=(width // span,),
        out_shape=(
            pltpu.HBM((width, ranks), bf16),
            pltpu.HBM((ranks, width), bf16),
            pltpu.HBM((own, ranks), bf16),
            pltpu.HBM((own, ranks), bf16),
        ),
        in_specs=[
            SMEM,
            pl.BlockSpec((tp // 2, per, kept, 128), lambda i: (0, i, 0, 0)),
            pl.BlockSpec((tp // 2, per, kept, 128), lambda i: (0, i, 0, 0)),
        ],
        out_specs=(
            pl.BlockSpec((span, ranks), lambda i: (i, 0)),
            pl.BlockSpec((ranks, span), lambda i: (0, i)),
            pl.BlockSpec((own, ranks), lambda i: (0, 0)),
            pl.BlockSpec((own, ranks), lambda i: (0, 0)),
        ),
        scratch_shapes=[pltpu.VMEM((span, ranks), bf16)],
        compiler_params=SMALL,
        cost_estimate=cost(1 << 30, 30 << 20),
    )(place, far(held), far(other))

    parts = width // span
    query_all, out_all = pl.pallas_call(
        functools.partial(decode_kernel, span),
        out_shape=(pltpu.HBM((width, cols), f32), pltpu.HBM((cols, width), f32)),
        in_specs=[ANY],
        out_specs=(ANY, ANY),
        scratch_shapes=[
            pltpu.VMEM(masters.shape, bf16),
            pltpu.VMEM((width, cols), f32),
            pltpu.VMEM((cols, width), f32),
            pltpu.SemaphoreType.DMA((parts,)),
            pltpu.SemaphoreType.DMA((parts, 2)),
        ],
        compiler_params=pltpu.CompilerParams(vmem_limit_bytes=24 << 20),
        cost_estimate=cost(1 << 30, 15 << 20),
    )(far(masters))

    squares = pl.pallas_call(
        sums_kernel,
        out_shape=jax.ShapeDtypeStruct((tp, 1, 128), f32),
        in_specs=[VMEM],
        out_specs=VMEM,
        compiler_params=SMALL,
        cost_estimate=LONG,
    )(low)
    squares = lax.all_to_all(squares, "tp", 0, 0)

    query_copy, out_copy, query_new, out_new = pl.pallas_call(
        functools.partial(final_kernel, float(rows * fs * cols * tp), span, rank_cols),
        out_shape=(
            pltpu.HBM((width, cols), bf16),
            pltpu.HBM((cols, width), bf16),
            pltpu.HBM((own, cols), f32),
            pltpu.HBM((own, cols), f32),
        ),
        in_specs=[SMEM] + [VMEM] * 6 + [ANY] * 4,
        out_specs=(ANY,) * 4,
        scratch_shapes=[
            pltpu.VMEM((width, cols), bf16),
            pltpu.VMEM((cols, width), bf16),
            pltpu.VMEM((2, own, ranks), bf16),
            pltpu.VMEM((2, own, cols), f32),
            pltpu.VMEM((2, own, cols), f32),
            pltpu.VMEM((ranks, cols), bf16),
            pltpu.VMEM((ranks, cols), bf16),
            pltpu.SemaphoreType.DMA((4,)),
            pltpu.SemaphoreType.DMA((parts, 2)),
            pltpu.SemaphoreType.DMA((2,)),
        ],
        compiler_params=SMALL,
        cost_estimate=cost(4 * width * ranks * cols, 20 << 20),
    )(
        place,
        squares,
        low,
        left,
        right,
        query_all,
        out_all,
        far(own_left),
        far(own_right),
        far(query_master),
        far(out_master.T),
    )
    return (query_new, out_new.T, query_copy, out_copy, first_new, second_new)


def solution(mesh):
    finer = Mesh(mesh.devices.reshape(12, 8, 8), ("z", "y", "tp"))
    both = P(FS, "tp")
    moment = P(None, FS, "tp")

    return jax.shard_map(
        body,
        mesh=finer,
        in_specs=(P(FS, None), both, both, P(FS, None), both, both, both, P("tp", FS), moment, moment),
        out_specs=(both, P("tp", FS), P(None, "tp"), P("tp", None), moment, moment),
        check_vma=False,
    )
```

```python
import functools

import jax
import jax.numpy as jnp
from jax import lax
from jax.experimental import pallas as pl
from jax.experimental.pallas import tpu as pltpu
from jax.sharding import Mesh
from jax.sharding import PartitionSpec as P


bf16 = jnp.bfloat16
f32 = jnp.float32
FS = ("z", "y")
VMEM = pl.BlockSpec(memory_space=pltpu.VMEM)
ANY = pl.BlockSpec(memory_space=pl.ANY)
SMEM = pl.BlockSpec(memory_space=pltpu.SMEM)
REACH = 2.0**34
SMALL = pltpu.CompilerParams(vmem_limit_bytes=16 << 20)


def cost(flops, nbytes):
    return pl.CostEstimate(flops=flops, bytes_accessed=nbytes, transcendentals=0)


LONG = cost(1 << 35, 1 << 26)


def coded(value):
    size = value * REACH
    size = size * size
    size = size * size
    return jnp.where(value < 0.0, -size, size).astype(bf16)


def decoded(code):
    wide = code.astype(f32)
    size = lax.rsqrt(lax.rsqrt(jnp.abs(wide))) * (1.0 / REACH)
    return jnp.where(wide < 0.0, -size, size)


def send_kernel(left, right, query_master, out_master, out, masters):
    own = query_master.shape[0]
    masters[:own] = coded(query_master[...])
    masters[own:] = coded(out_master[...])
    both = jnp.concatenate([left[...].astype(f32), right[...].astype(f32)], axis=1)
    used = both.shape[1]
    free = 128 - used
    kept = out.shape[1]
    rest = both[kept:]
    tail = jnp.concatenate([rest[:, j : j + free] for j in range(0, used, free)], axis=0)
    packed = jnp.concatenate([both[:kept], tail], axis=1).astype(bf16)
    out[...] = jnp.broadcast_to(packed[None], out.shape)


def hold_kernel(masters, packed, out):
    pass


def unpacked(packed, used):
    free = 128 - used
    parts = used // free
    height = packed.shape[1] // parts
    wide = packed.astype(f32)
    tail = [wide[:, j * height : (j + 1) * height, used:] for j in range(parts)]
    tail = jnp.concatenate(tail + [jnp.zeros_like(tail[0])], axis=2)
    return jnp.concatenate([wide, tail], axis=1)


def proj_kernel(used, packed, saved_inputs, out_cotangent, out, factors):
    own = factors.shape[0] // packed.shape[0]
    step = 8
    for i in range(0, packed.shape[0], step):
        block = unpacked(packed[i : i + step], used).reshape(step * own, 128)
        factors[i * own : (i + step) * own] = block.astype(bf16)
    left = jnp.dot(saved_inputs[...], factors[...], preferred_element_type=f32)
    right = jnp.dot(out_cotangent[...], factors[...], preferred_element_type=f32)
    lane = lax.broadcasted_iota(jnp.int32, left.shape, 1)
    out[...] = jnp.where(lane < used // 2, left, right).T[:used].astype(bf16)


def grad_kernel(rank_cols, proj, query_cotangent, attn_outputs, out):
    cols = query_cotangent.shape[1]
    parts = []
    for k, other in enumerate((query_cotangent, attn_outputs)):
        starts = range(k * rank_cols, proj.shape[0], 2 * rank_cols)
        ranks = jnp.concatenate([proj[at : at + rank_cols] for at in starts], axis=0)
        parts.append(jnp.dot(ranks, other[...], preferred_element_type=f32).reshape(-1, 8, cols))
    first, second = parts
    both = jnp.concatenate([first[:, :4], second[:, :4], first[:, 4:], second[:, 4:]], axis=1)
    out[...] = both.astype(bf16)


def moment_kernel(pieces, first, second, first_new, second_new, low):
    rows = first.shape[1]
    grads = jnp.sum(pieces[...].astype(f32), axis=0)
    new_first = 0.9 * jnp.concatenate([first[0], first[1]], axis=0) + 0.1 * grads
    new_second = 0.99 * jnp.concatenate([second[0], second[1]], axis=0) + 0.01 * grads * grads
    direction = new_first / (jnp.sqrt(new_second) + 1e-08)
    first_new[0] = new_first[:rows]
    first_new[1] = new_first[rows:]
    second_new[0] = new_second[:rows]
    second_new[1] = new_second[rows:]
    squares = direction * direction
    lane = lax.broadcasted_iota(jnp.int32, (rows, 128), 1)
    sums = jnp.zeros((rows, 128), f32)
    for k in range(2):
        rest = jnp.sum(squares[k * rows : (k + 1) * rows], axis=(0, 1), keepdims=True)
        for part in range(3):
            rounded = rest.astype(bf16).astype(f32)
            sums = jnp.where(lane == 3 * k + part, rounded, sums)
            rest = rest - rounded
    sent = jnp.concatenate([direction[:rows], direction[rows:], sums], axis=1).astype(bf16)
    low[...] = jnp.broadcast_to(sent[None], low.shape)


def prep_kernel(rank_cols, place, held, other, left, right, own_left, own_right, tile):
    own = own_left.shape[0]
    span = left.shape[0]
    sides = [[], []]
    for half in (held, other):
        for s in range(half.shape[0]):
            block = unpacked(half[s], 2 * rank_cols).reshape(span, 128)
            for k in range(2):
                sides[k].append(block[:, k * rank_cols : (k + 1) * rank_cols])
    both = [jnp.concatenate(side, axis=1).astype(bf16) for side in sides]
    left[...] = both[0]
    right[...] = both[1].T

    @pl.when(pl.program_id(0) == place[0] // (span // own))
    def _():
        rows = pl.ds(pl.multiple_of(place[0] % (span // own) * own, own), own)
        for side, out in zip(both, (own_left, own_right)):
            tile[...] = side
            out[...] = tile[rows]


def spread_kernel(low, out):
    out[...] = jnp.broadcast_to(low[...][None], out.shape)


def sums_kernel(low, squares):
    sums = jnp.sum(low[:, :, :, -128:].astype(f32), axis=(0, 1))[:1]
    squares[...] = jnp.broadcast_to(sums[None], squares.shape)


def final_kernel(
    entries,
    span,
    rank_cols,
    place,
    squares,
    low,
    left,
    right,
    masters,
    own_left,
    own_right,
    query_master,
    out_master,
    query_copy,
    out_copy,
    query_new,
    out_new,
    near_query,
    near_out,
    near_own,
    near_master,
    near_new,
    first,
    second,
    own_arrived,
    left_for,
    own_left_for,
):
    width = left.shape[0]
    cols = first.shape[1]
    own = query_master.shape[0]
    per = span // own
    parts = width // span
    ways = (
        (own_left, near_own.at[0]),
        (own_right, near_own.at[1]),
        (query_master, near_master.at[0]),
        (out_master, near_master.at[1]),
    )
    own_copies = [pltpu.make_async_copy(x, y, own_arrived.at[k]) for k, (x, y) in enumerate(ways)]
    for copy in own_copies:
        copy.start()

    tp = squares.shape[0]
    height = low.shape[0]
    per_block = rank_cols // low.shape[2]
    for b in range(tp):
        chip, core = b % (tp // 2), b // (tp // 2)
        at = (place[1] + 2 * chip) % tp
        at = at + core * (1 - 2 * (at % 2))
        held = [at * per_block + j for j in range(per_block)]
        block = [low[j % height, j // height].astype(f32) for j in held]
        for k, step in enumerate((first, second)):
            part = jnp.concatenate([piece[:, k * cols : (k + 1) * cols] for piece in block], axis=0)
            step[b * rank_cols : (b + 1) * rank_cols] = part.astype(bf16)
    second_turned = second[...].T

    sums = jnp.sum(squares[...], axis=0)
    lane = lax.broadcasted_iota(jnp.int32, sums.shape, 1)
    scales = []
    for k in range(2):
        total = jnp.sum(jnp.where(lane // 3 == k, sums, 0.0), axis=1, keepdims=True)
        scales.append(0.01 * lax.rsqrt(total / entries + 1e-06))

    sent = []
    for i in range(parts):
        at = pl.ds(i * span, span)
        codes = masters[i * per : (i + 1) * per]
        moved = jnp.dot(left[at], first[...], preferred_element_type=f32)
        kept = decoded(codes[:, :own].reshape(span, cols))
        near_query[at] = (kept - scales[0] * moved).astype(bf16)
        sent.append(pltpu.make_async_copy(near_query.at[at], query_copy.at[at], left_for.at[i, 0]))
        sent[-1].start()
        moved = jnp.dot(second_turned, right[:, at], preferred_element_type=f32)
        kept = decoded(codes[:, own:].reshape(span, cols).T)
        near_out[:, at] = (kept - scales[1] * moved).astype(bf16)
        sent.append(pltpu.make_async_copy(near_out.at[:, at], out_copy.at[:, at], left_for.at[i, 1]))
        sent[-1].start()
    for copy in own_copies:
        copy.wait()
    for k, (step, new) in enumerate(((first, query_new), (second, out_new))):
        moved = jnp.dot(near_own[k], step[...], preferred_element_type=f32)
        near_new[k] = near_master[k] - scales[k] * moved
        sent.append(pltpu.make_async_copy(near_new.at[k], new, own_left_for.at[k]))
        sent[-1].start()
    for copy in sent:
        copy.wait()


def far(value):
    return pltpu.with_memory_space_constraint(value, pltpu.HBM)


def body(
    saved_inputs,
    query_cotangent,
    attn_outputs,
    out_cotangent,
    left_factor,
    right_factor,
    query_master,
    out_master,
    first_moment,
    second_moment,
):
    depth = lax.axis_size("z")
    height = lax.axis_size("y")
    fs = depth * height
    tp = lax.axis_size("tp")
    own, rank_cols = left_factor.shape
    rows = first_moment.shape[1]
    cols = first_moment.shape[2]
    tokens = saved_inputs.shape[0]
    width = fs * own
    ranks = tp * rank_cols
    used = 2 * rank_cols
    kept = own * used // 128

    place = jnp.stack([lax.axis_index(FS), lax.axis_index("tp")]).astype(jnp.int32)
    packed, masters = pl.pallas_call(
        send_kernel,
        out_shape=(jax.ShapeDtypeStruct((fs, kept, 128), bf16), pltpu.HBM((2 * own, cols), bf16)),
        in_specs=[pl.BlockSpec()] * 4,
        out_specs=(VMEM, VMEM),
        compiler_params=SMALL,
        cost_estimate=cost(1 << 16, 1 << 20),
    )(far(left_factor), far(right_factor), far(query_master), far(out_master.T))
    packed = pl.pallas_call(
        hold_kernel,
        out_shape=jax.ShapeDtypeStruct(packed.shape, bf16),
        in_specs=[ANY, ANY],
        out_specs=ANY,
        input_output_aliases={1: 0},
        compiler_params=SMALL,
        cost_estimate=LONG,
    )(far(masters), packed)
    masters = lax.all_gather(masters, FS)
    packed = lax.all_to_all(packed, FS, 0, 0)
    proj = pl.pallas_call(
        functools.partial(proj_kernel, used),
        out_shape=jax.ShapeDtypeStruct((used, tokens), bf16),
        in_specs=[VMEM] * 3,
        out_specs=VMEM,
        scratch_shapes=[pltpu.VMEM((width, 128), bf16)],
        compiler_params=SMALL,
        cost_estimate=cost(4 * tokens * width * 128, 8 << 20),
    )(packed, saved_inputs, out_cotangent)
    proj = lax.all_gather(proj, "tp", axis=0, tiled=True)

    partial = pl.pallas_call(
        functools.partial(grad_kernel, rank_cols),
        out_shape=pltpu.HBM((fs // 2, 4 * rows, cols), bf16),
        in_specs=[VMEM] * 3,
        out_specs=VMEM,
        compiler_params=SMALL,
        cost_estimate=cost(4 * ranks * tokens * cols, 2 << 20),
    )(proj, query_cotangent, attn_outputs)
    pieces = lax.all_to_all(partial.reshape(fs, 2 * rows, cols), FS, 0, 0)

    held = [packed]
    for step in range(1, tp // 2):
        held.append(lax.ppermute(packed, "tp", [((t + 2 * step) % tp, t) for t in range(tp)]))
    held = jnp.stack(held)
    other = lax.ppermute(held, "tp", [(t ^ 1, t) for t in range(tp)])

    first_new, second_new, low = pl.pallas_call(
        moment_kernel,
        out_shape=(
            jax.ShapeDtypeStruct(first_moment.shape, f32),
            jax.ShapeDtypeStruct(second_moment.shape, f32),
            pltpu.HBM((depth, rows, 2 * cols + 128), bf16),
        ),
        in_specs=[VMEM] * 3,
        out_specs=(VMEM, VMEM, VMEM),
        compiler_params=SMALL,
        cost_estimate=cost(1 << 20, 2 << 20),
    )(pieces, first_moment, second_moment)
    low = lax.all_to_all(low, "z", 0, 0)
    low = pl.pallas_call(
        spread_kernel,
        out_shape=pltpu.HBM((height, *low.shape), bf16),
        in_specs=[VMEM],
        out_specs=VMEM,
        compiler_params=SMALL,
        cost_estimate=cost(1 << 16, 1 << 20),
    )(low)
    low = lax.all_to_all(low, "y", 0, 0)

    span = width // 6
    per = span // own
    left, right, own_left, own_right = pl.pallas_call(
        functools.partial(prep_kernel, rank_cols),
        grid=(width // span,),
        out_shape=(
            pltpu.HBM((width, ranks), bf16),
            pltpu.HBM((ranks, width), bf16),
            pltpu.HBM((own, ranks), bf16),
            pltpu.HBM((own, ranks), bf16),
        ),
        in_specs=[
            SMEM,
            pl.BlockSpec((tp // 2, per, kept, 128), lambda i: (0, i, 0, 0)),
            pl.BlockSpec((tp // 2, per, kept, 128), lambda i: (0, i, 0, 0)),
        ],
        out_specs=(
            pl.BlockSpec((span, ranks), lambda i: (i, 0)),
            pl.BlockSpec((ranks, span), lambda i: (0, i)),
            pl.BlockSpec((own, ranks), lambda i: (0, 0)),
            pl.BlockSpec((own, ranks), lambda i: (0, 0)),
        ),
        scratch_shapes=[pltpu.VMEM((span, ranks), bf16)],
        compiler_params=SMALL,
        cost_estimate=cost(1 << 30, 30 << 20),
    )(place, far(held), far(other))

    low, masters = lax.optimization_barrier((low, masters))
    parts = width // span
    squares = pl.pallas_call(
        sums_kernel,
        out_shape=jax.ShapeDtypeStruct((tp, 1, 128), f32),
        in_specs=[VMEM],
        out_specs=VMEM,
        compiler_params=SMALL,
        cost_estimate=LONG,
    )(low)
    squares = lax.all_to_all(squares, "tp", 0, 0)

    query_copy, out_copy, query_new, out_new = pl.pallas_call(
        functools.partial(final_kernel, float(rows * fs * cols * tp), span, rank_cols),
        out_shape=(
            pltpu.HBM((width, cols), bf16),
            pltpu.HBM((cols, width), bf16),
            pltpu.HBM((own, cols), f32),
            pltpu.HBM((own, cols), f32),
        ),
        in_specs=[SMEM] + [VMEM] * 5 + [ANY] * 4,
        out_specs=(ANY,) * 4,
        scratch_shapes=[
            pltpu.VMEM((width, cols), bf16),
            pltpu.VMEM((cols, width), bf16),
            pltpu.VMEM((2, own, ranks), bf16),
            pltpu.VMEM((2, own, cols), f32),
            pltpu.VMEM((2, own, cols), f32),
            pltpu.VMEM((ranks, cols), bf16),
            pltpu.VMEM((ranks, cols), bf16),
            pltpu.SemaphoreType.DMA((4,)),
            pltpu.SemaphoreType.DMA((parts, 2)),
            pltpu.SemaphoreType.DMA((2,)),
        ],
        compiler_params=SMALL,
        cost_estimate=cost(4 * width * ranks * cols, 20 << 20),
    )(
        place,
        squares,
        low,
        left,
        right,
        masters,
        far(own_left),
        far(own_right),
        far(query_master),
        far(out_master.T),
    )
    return (query_new, out_new.T, query_copy, out_copy, first_new, second_new)


def solution(mesh):
    finer = Mesh(mesh.devices.reshape(12, 8, 8), ("z", "y", "tp"))
    both = P(FS, "tp")
    moment = P(None, FS, "tp")

    return jax.shard_map(
        body,
        mesh=finer,
        in_specs=(P(FS, None), both, both, P(FS, None), both, both, both, P("tp", FS), moment, moment),
        out_specs=(both, P("tp", FS), P(None, "tp"), P("tp", None), moment, moment),
        check_vma=False,
    )
```

```python
import functools

import jax
import jax.numpy as jnp
from jax import lax
from jax.experimental import pallas as pl
from jax.experimental.pallas import tpu as pltpu
from jax.sharding import Mesh
from jax.sharding import PartitionSpec as P


bf16 = jnp.bfloat16
f32 = jnp.float32
FS = ("z", "y")
VMEM = pl.BlockSpec(memory_space=pltpu.VMEM)
ANY = pl.BlockSpec(memory_space=pl.ANY)
SMEM = pl.BlockSpec(memory_space=pltpu.SMEM)
REACH = 2.0**34
SMALL = pltpu.CompilerParams(vmem_limit_bytes=16 << 20)


def cost(flops, nbytes):
    return pl.CostEstimate(flops=flops, bytes_accessed=nbytes, transcendentals=0)


LONG = cost(1 << 35, 1 << 26)


def coded(value):
    size = value * REACH
    size = size * size
    size = size * size
    return jnp.where(value < 0.0, -size, size).astype(bf16)


def decoded(code):
    wide = code.astype(f32)
    size = lax.rsqrt(lax.rsqrt(jnp.abs(wide))) * (1.0 / REACH)
    return jnp.where(wide < 0.0, -size, size)


def send_kernel(left, right, query_master, out_master, out, masters):
    own = query_master.shape[0]
    masters[:own] = coded(query_master[...])
    masters[own:] = coded(out_master[...])
    both = jnp.concatenate([left[...].astype(f32), right[...].astype(f32)], axis=1)
    used = both.shape[1]
    free = 128 - used
    kept = out.shape[1]
    rest = both[kept:]
    tail = jnp.concatenate([rest[:, j : j + free] for j in range(0, used, free)], axis=0)
    packed = jnp.concatenate([both[:kept], tail], axis=1).astype(bf16)
    out[...] = jnp.broadcast_to(packed[None], out.shape)


def hold_kernel(masters, packed, out):
    pass


def unpacked(packed, used):
    free = 128 - used
    parts = used // free
    height = packed.shape[1] // parts
    wide = packed.astype(f32)
    tail = [wide[:, j * height : (j + 1) * height, used:] for j in range(parts)]
    tail = jnp.concatenate(tail + [jnp.zeros_like(tail[0])], axis=2)
    return jnp.concatenate([wide, tail], axis=1)


def proj_kernel(used, packed, saved_inputs, out_cotangent, out, factors):
    own = factors.shape[0] // packed.shape[0]
    step = 8
    for i in range(0, packed.shape[0], step):
        block = unpacked(packed[i : i + step], used).reshape(step * own, 128)
        factors[i * own : (i + step) * own] = block.astype(bf16)
    left = jnp.dot(saved_inputs[...], factors[...], preferred_element_type=f32)
    right = jnp.dot(out_cotangent[...], factors[...], preferred_element_type=f32)
    lane = lax.broadcasted_iota(jnp.int32, left.shape, 1)
    out[...] = jnp.where(lane < used // 2, left, right).T[:used].astype(bf16)


def grad_kernel(rank_cols, proj, query_cotangent, attn_outputs, out):
    cols = query_cotangent.shape[1]
    parts = []
    for k, other in enumerate((query_cotangent, attn_outputs)):
        starts = range(k * rank_cols, proj.shape[0], 2 * rank_cols)
        ranks = jnp.concatenate([proj[at : at + rank_cols] for at in starts], axis=0)
        parts.append(jnp.dot(ranks, other[...], preferred_element_type=f32).reshape(-1, 8, cols))
    first, second = parts
    both = jnp.concatenate([first[:, :4], second[:, :4], first[:, 4:], second[:, 4:]], axis=1)
    out[...] = both.astype(bf16)


def in_three(total):
    parts = []
    for _ in range(3):
        parts.append(total.astype(bf16).astype(f32))
        total = total - parts[-1]
    return parts


def moment_kernel(pieces, first, second, first_new, second_new, low):
    rows = first.shape[1]
    grads = jnp.sum(pieces[...].astype(f32), axis=0)
    new_first = 0.9 * jnp.concatenate([first[0], first[1]], axis=0) + 0.1 * grads
    new_second = 0.99 * jnp.concatenate([second[0], second[1]], axis=0) + 0.01 * grads * grads
    direction = new_first / (jnp.sqrt(new_second) + 1e-08)
    first_new[0] = new_first[:rows]
    first_new[1] = new_first[rows:]
    second_new[0] = new_second[:rows]
    second_new[1] = new_second[rows:]
    squares = direction * direction
    lane = lax.broadcasted_iota(jnp.int32, (rows, 128), 1)
    sums = jnp.zeros((rows, 128), f32)
    for k in range(2):
        total = jnp.sum(squares[k * rows : (k + 1) * rows], axis=(0, 1), keepdims=True)
        for part, value in enumerate(in_three(total)):
            sums = jnp.where(lane == 3 * k + part, value, sums)
    sent = jnp.concatenate([direction[:rows], direction[rows:], sums], axis=1).astype(bf16)
    low[...] = jnp.broadcast_to(sent[None], low.shape)


def prep_kernel(rank_cols, place, held, other, left, right, own_left, own_right, tile):
    own = own_left.shape[0]
    span = left.shape[0]
    chips = held.shape[0]
    blocks = [[unpacked(half[s], 2 * rank_cols).reshape(span, 128) for s in range(chips)] for half in (held, other)]
    here = place[1] % 2 == 0
    by_core = [
        [jnp.where(here, near, far) for near, far in zip(blocks[core], blocks[1 - core])] for core in range(2)
    ]
    for chip in range(chips):

        @pl.when(place[1] // 2 == chip)
        def _():
            for k in range(2):
                at = slice(k * rank_cols, (k + 1) * rank_cols)
                side = [by_core[core][(s - chip) % chips][:, at] for s in range(chips) for core in range(2)]
                side = jnp.concatenate(side, axis=1).astype(bf16)
                tile[k] = side
    left[...] = tile[0]
    right[...] = tile[1].T

    @pl.when(pl.program_id(0) == place[0] // (span // own))
    def _():
        rows = pl.ds(pl.multiple_of(place[0] % (span // own) * own, own), own)
        own_left[...] = tile[0, rows]
        own_right[...] = tile[1, rows]


def spread_kernel(low, out):
    depth, _, lanes = low.shape
    lanes = lanes - 128
    sums = jnp.sum(low[:, :, lanes:].astype(f32), axis=0)
    lane = lax.broadcasted_iota(jnp.int32, sums.shape, 1)
    squares = jnp.zeros(sums.shape, f32)
    for k in range(2):
        total = jnp.sum(jnp.where(lane // 3 == k, sums, 0.0)[:1], axis=1, keepdims=True)
        for part, value in enumerate(in_three(total)):
            squares = jnp.where(lane == 3 * k + part, value, squares)
    squares = jnp.concatenate([squares] * (lanes // 128), axis=1).astype(bf16)
    for y in range(out.shape[0]):
        out[y, :depth] = low[:, :, :lanes]
        out[y, depth] = squares


def sums_kernel(low, squares):
    depth = low.shape[1] - 1
    sums = jnp.sum(low[:, depth, :, :128].astype(f32), axis=0)[:1]
    squares[...] = jnp.broadcast_to(sums[None], squares.shape)


def final_kernel(
    entries,
    span,
    squares,
    low,
    left,
    right,
    masters,
    own_left,
    own_right,
    query_master,
    out_master,
    query_copy,
    out_copy,
    query_new,
    out_new,
    near_query,
    near_out,
    near_own,
    near_master,
    near_new,
    first,
    second,
    own_arrived,
    left_for,
    own_left_for,
):
    width = left.shape[0]
    cols = first.shape[1]
    own = query_master.shape[0]
    per = span // own
    parts = width // span
    ways = (
        (own_left, near_own.at[0]),
        (own_right, near_own.at[1]),
        (query_master, near_master.at[0]),
        (out_master, near_master.at[1]),
    )
    own_copies = [pltpu.make_async_copy(x, y, own_arrived.at[k]) for k, (x, y) in enumerate(ways)]
    for copy in own_copies:
        copy.start()

    height = low.shape[0]
    rows = low.shape[2]
    group = 16 // rows
    for g in range(0, first.shape[0] // rows, group):
        part = [low[f % height, f // height].astype(f32) for f in range(g, g + group)]
        part = jnp.concatenate(part, axis=0).astype(bf16)
        first[g * rows : (g + group) * rows] = part[:, :cols]
        second[g * rows : (g + group) * rows] = part[:, cols:]
    second_turned = second[...].T

    sums = jnp.sum(squares[...], axis=0)
    lane = lax.broadcasted_iota(jnp.int32, sums.shape, 1)
    scales = []
    for k in range(2):
        total = jnp.sum(jnp.where(lane // 3 == k, sums, 0.0), axis=1, keepdims=True)
        scales.append(0.01 * lax.rsqrt(total / entries + 1e-06))

    sent = []
    for i in range(parts):
        at = pl.ds(i * span, span)
        codes = masters[i * per : (i + 1) * per]
        moved = jnp.dot(left[at], first[...], preferred_element_type=f32)
        kept = decoded(codes[:, :own].reshape(span, cols))
        near_query[at] = (kept - scales[0] * moved).astype(bf16)
        sent.append(pltpu.make_async_copy(near_query.at[at], query_copy.at[at], left_for.at[i, 0]))
        sent[-1].start()
        moved = jnp.dot(second_turned, right[:, at], preferred_element_type=f32)
        kept = decoded(codes[:, own:].reshape(span, cols).T)
        near_out[:, at] = (kept - scales[1] * moved).astype(bf16)
        sent.append(pltpu.make_async_copy(near_out.at[:, at], out_copy.at[:, at], left_for.at[i, 1]))
        sent[-1].start()
    for copy in own_copies:
        copy.wait()
    for k, (step, new) in enumerate(((first, query_new), (second, out_new))):
        moved = jnp.dot(near_own[k], step[...], preferred_element_type=f32)
        near_new[k] = near_master[k] - scales[k] * moved
        sent.append(pltpu.make_async_copy(near_new.at[k], new, own_left_for.at[k]))
        sent[-1].start()
    for copy in sent:
        copy.wait()


def far(value):
    return pltpu.with_memory_space_constraint(value, pltpu.HBM)


def body(
    saved_inputs,
    query_cotangent,
    attn_outputs,
    out_cotangent,
    left_factor,
    right_factor,
    query_master,
    out_master,
    first_moment,
    second_moment,
):
    depth = lax.axis_size("z")
    height = lax.axis_size("y")
    fs = depth * height
    tp = lax.axis_size("tp")
    own, rank_cols = left_factor.shape
    rows = first_moment.shape[1]
    cols = first_moment.shape[2]
    tokens = saved_inputs.shape[0]
    width = fs * own
    ranks = tp * rank_cols
    used = 2 * rank_cols
    kept = own * used // 128

    place = jnp.stack([lax.axis_index(FS), lax.axis_index("tp")]).astype(jnp.int32)
    packed, masters = pl.pallas_call(
        send_kernel,
        out_shape=(
            jax.ShapeDtypeStruct((fs, kept, 128), bf16),
            pltpu.HBM((2 * own, cols), bf16),
        ),
        in_specs=[pl.BlockSpec()] * 4,
        out_specs=(VMEM, VMEM),
        compiler_params=SMALL,
        cost_estimate=cost(1 << 16, 1 << 20),
    )(far(left_factor), far(right_factor), far(query_master), far(out_master.T))
    packed = pl.pallas_call(
        hold_kernel,
        out_shape=jax.ShapeDtypeStruct(packed.shape, bf16),
        in_specs=[ANY, ANY],
        out_specs=ANY,
        input_output_aliases={1: 0},
        compiler_params=SMALL,
        cost_estimate=LONG,
    )(far(masters), packed)
    masters = lax.all_gather(masters, FS)
    packed = lax.all_to_all(packed, FS, 0, 0)
    proj = pl.pallas_call(
        functools.partial(proj_kernel, used),
        out_shape=jax.ShapeDtypeStruct((used, tokens), bf16),
        in_specs=[VMEM] * 3,
        out_specs=VMEM,
        scratch_shapes=[pltpu.VMEM((width, 128), bf16)],
        compiler_params=SMALL,
        cost_estimate=cost(4 * tokens * width * 128, 8 << 20),
    )(packed, saved_inputs, out_cotangent)
    proj = lax.all_gather(proj, "tp", axis=0, tiled=True)

    partial = pl.pallas_call(
        functools.partial(grad_kernel, rank_cols),
        out_shape=pltpu.HBM((fs // 2, 4 * rows, cols), bf16),
        in_specs=[VMEM] * 3,
        out_specs=VMEM,
        compiler_params=SMALL,
        cost_estimate=cost(4 * ranks * tokens * cols, 2 << 20),
    )(proj, query_cotangent, attn_outputs)
    pieces = lax.all_to_all(partial.reshape(fs, 2 * rows, cols), FS, 0, 0)

    held = [packed]
    for step in range(1, tp // 2):
        held.append(lax.ppermute(packed, "tp", [((t + 2 * step) % tp, t) for t in range(tp)]))
    held = jnp.stack(held)
    other = lax.ppermute(held, "tp", [(t ^ 1, t) for t in range(tp)])

    first_new, second_new, low = pl.pallas_call(
        moment_kernel,
        out_shape=(
            jax.ShapeDtypeStruct(first_moment.shape, f32),
            jax.ShapeDtypeStruct(second_moment.shape, f32),
            pltpu.HBM((depth, rows, 2 * cols + 128), bf16),
        ),
        in_specs=[VMEM] * 3,
        out_specs=(VMEM, VMEM, VMEM),
        compiler_params=SMALL,
        cost_estimate=cost(1 << 20, 2 << 20),
    )(pieces, first_moment, second_moment)
    low = lax.all_to_all(low, "z", 0, 0)
    low = pl.pallas_call(
        spread_kernel,
        out_shape=pltpu.HBM((height, depth + 1, rows, 2 * cols), bf16),
        in_specs=[VMEM],
        out_specs=VMEM,
        compiler_params=SMALL,
        cost_estimate=cost(1 << 16, 1 << 20),
    )(low)
    low = lax.all_to_all(low, "y", 0, 0)

    span = width // 4
    per = span // own
    left, right, own_left, own_right = pl.pallas_call(
        functools.partial(prep_kernel, rank_cols),
        grid=(width // span,),
        out_shape=(
            pltpu.HBM((width, ranks), bf16),
            pltpu.HBM((ranks, width), bf16),
            pltpu.HBM((own, ranks), bf16),
            pltpu.HBM((own, ranks), bf16),
        ),
        in_specs=[
            SMEM,
            pl.BlockSpec((tp // 2, per, kept, 128), lambda i: (0, i, 0, 0)),
            pl.BlockSpec((tp // 2, per, kept, 128), lambda i: (0, i, 0, 0)),
        ],
        out_specs=(
            pl.BlockSpec((span, ranks), lambda i: (i, 0)),
            pl.BlockSpec((ranks, span), lambda i: (0, i)),
            pl.BlockSpec((own, ranks), lambda i: (0, 0)),
            pl.BlockSpec((own, ranks), lambda i: (0, 0)),
        ),
        scratch_shapes=[pltpu.VMEM((2, span, ranks), bf16)],
        compiler_params=SMALL,
        cost_estimate=cost(1 << 30, 30 << 20),
    )(place, far(held), far(other))

    low, masters = lax.optimization_barrier((low, masters))
    parts = width // span
    squares = pl.pallas_call(
        sums_kernel,
        out_shape=jax.ShapeDtypeStruct((tp, 1, 128), f32),
        in_specs=[VMEM],
        out_specs=VMEM,
        compiler_params=SMALL,
        cost_estimate=LONG,
    )(low)
    squares = lax.all_to_all(squares, "tp", 0, 0)

    query_copy, out_copy, query_new, out_new = pl.pallas_call(
        functools.partial(final_kernel, float(rows * fs * cols * tp), span),
        out_shape=(
            pltpu.HBM((width, cols), bf16),
            pltpu.HBM((cols, width), bf16),
            pltpu.HBM((own, cols), f32),
            pltpu.HBM((own, cols), f32),
        ),
        in_specs=[VMEM] * 5 + [ANY] * 4,
        out_specs=(ANY,) * 4,
        scratch_shapes=[
            pltpu.VMEM((width, cols), bf16),
            pltpu.VMEM((cols, width), bf16),
            pltpu.VMEM((2, own, ranks), bf16),
            pltpu.VMEM((2, own, cols), f32),
            pltpu.VMEM((2, own, cols), f32),
            pltpu.VMEM((ranks, cols), bf16),
            pltpu.VMEM((ranks, cols), bf16),
            pltpu.SemaphoreType.DMA((4,)),
            pltpu.SemaphoreType.DMA((parts, 2)),
            pltpu.SemaphoreType.DMA((2,)),
        ],
        compiler_params=SMALL,
        cost_estimate=cost(4 * width * ranks * cols, 20 << 20),
    )(
        squares,
        low,
        left,
        right,
        masters,
        far(own_left),
        far(own_right),
        far(query_master),
        far(out_master.T),
    )
    return (query_new, out_new.T, query_copy, out_copy, first_new, second_new)


def solution(mesh):
    finer = Mesh(mesh.devices.reshape(12, 8, 8), ("z", "y", "tp"))
    both = P(FS, "tp")
    moment = P(None, FS, "tp")

    return jax.shard_map(
        body,
        mesh=finer,
        in_specs=(P(FS, None), both, both, P(FS, None), both, both, both, P("tp", FS), moment, moment),
        out_specs=(both, P("tp", FS), P(None, "tp"), P("tp", None), moment, moment),
        check_vma=False,
    )
```

```python
import functools

import jax
import jax.numpy as jnp
from jax import lax
from jax.experimental import pallas as pl
from jax.experimental.pallas import tpu as pltpu
from jax.sharding import Mesh
from jax.sharding import PartitionSpec as P


bf16 = jnp.bfloat16
f32 = jnp.float32
FS = ("z", "y")
VMEM = pl.BlockSpec(memory_space=pltpu.VMEM)
ANY = pl.BlockSpec(memory_space=pl.ANY)
SMEM = pl.BlockSpec(memory_space=pltpu.SMEM)
REACH = 2.0**34
SMALL = pltpu.CompilerParams(vmem_limit_bytes=16 << 20)


def cost(flops, nbytes):
    return pl.CostEstimate(flops=flops, bytes_accessed=nbytes, transcendentals=0)


LONG = cost(1 << 35, 1 << 26)


def coded(value):
    size = value * REACH
    size = size * size
    size = size * size
    return jnp.where(value < 0.0, -size, size).astype(bf16)


def decoded(code):
    wide = code.astype(f32)
    size = lax.rsqrt(lax.rsqrt(jnp.abs(wide))) * (1.0 / REACH)
    return jnp.where(wide < 0.0, -size, size)


def send_kernel(left, right, query_master, out_master, out, masters):
    own = query_master.shape[0]
    masters[:own] = coded(query_master[...])
    masters[own:] = coded(out_master[...])
    both = jnp.concatenate([left[...].astype(f32), right[...].astype(f32)], axis=1)
    used = both.shape[1]
    free = 128 - used
    kept = out.shape[1]
    rest = both[kept:]
    tail = jnp.concatenate([rest[:, j : j + free] for j in range(0, used, free)], axis=0)
    packed = jnp.concatenate([both[:kept], tail], axis=1).astype(bf16)
    out[...] = jnp.broadcast_to(packed[None], out.shape)


def hold_kernel(masters, packed, out):
    pass


def unpacked(packed, used):
    free = 128 - used
    parts = used // free
    height = packed.shape[1] // parts
    wide = packed.astype(f32)
    tail = [wide[:, j * height : (j + 1) * height, used:] for j in range(parts)]
    tail = jnp.concatenate(tail + [jnp.zeros_like(tail[0])], axis=2)
    return jnp.concatenate([wide, tail], axis=1)


def proj_kernel(used, packed, saved_inputs, out_cotangent, out, factors):
    own = factors.shape[0] // packed.shape[0]
    step = 8
    for i in range(0, packed.shape[0], step):
        block = unpacked(packed[i : i + step], used).reshape(step * own, 128)
        factors[i * own : (i + step) * own] = block.astype(bf16)
    left = jnp.dot(saved_inputs[...], factors[...], preferred_element_type=f32)
    right = jnp.dot(out_cotangent[...], factors[...], preferred_element_type=f32)
    lane = lax.broadcasted_iota(jnp.int32, left.shape, 1)
    out[...] = jnp.where(lane < used // 2, left, right).T[:used].astype(bf16)


def grad_kernel(rank_cols, proj, query_cotangent, attn_outputs, out):
    cols = query_cotangent.shape[1]
    parts = []
    for k, other in enumerate((query_cotangent, attn_outputs)):
        starts = range(k * rank_cols, proj.shape[0], 2 * rank_cols)
        ranks = jnp.concatenate([proj[at : at + rank_cols] for at in starts], axis=0)
        parts.append(jnp.dot(ranks, other[...], preferred_element_type=f32).reshape(-1, 8, cols))
    first, second = parts
    both = jnp.concatenate([first[:, :4], second[:, :4], first[:, 4:], second[:, 4:]], axis=1)
    height, depth = out.shape[:2]
    both = both.astype(bf16).reshape(depth, height // 2, 16, cols)
    for y in range(0, height, 2):
        out[y] = both[:, y // 2, :8]
        out[y + 1] = both[:, y // 2, 8:]


def fold_kernel(pieces, out):
    out[...] = jnp.sum(pieces[...].astype(f32), axis=0)


def in_three(total):
    parts = []
    for _ in range(3):
        parts.append(total.astype(bf16).astype(f32))
        total = total - parts[-1]
    return parts


def moment_kernel(pieces, first, second, first_new, second_new, low):
    rows = first.shape[1]
    grads = jnp.sum(pieces[...], axis=0)
    new_first = 0.9 * jnp.concatenate([first[0], first[1]], axis=0) + 0.1 * grads
    new_second = 0.99 * jnp.concatenate([second[0], second[1]], axis=0) + 0.01 * grads * grads
    direction = new_first / (jnp.sqrt(new_second) + 1e-08)
    first_new[0] = new_first[:rows]
    first_new[1] = new_first[rows:]
    second_new[0] = new_second[:rows]
    second_new[1] = new_second[rows:]
    squares = direction * direction
    lane = lax.broadcasted_iota(jnp.int32, (rows, 128), 1)
    sums = jnp.zeros((rows, 128), f32)
    for k in range(2):
        total = jnp.sum(squares[k * rows : (k + 1) * rows], axis=(0, 1), keepdims=True)
        for part, value in enumerate(in_three(total)):
            sums = jnp.where(lane == 3 * k + part, value, sums)
    sent = jnp.concatenate([direction[:rows], direction[rows:], sums], axis=1).astype(bf16)
    low[...] = jnp.broadcast_to(sent[None], low.shape)


def prep_kernel(rank_cols, place, held, other, left, right, own_left, own_right, tile):
    own = own_left.shape[0]
    span = left.shape[0]
    chips = held.shape[0]
    blocks = [[unpacked(half[s], 2 * rank_cols).reshape(span, 128) for s in range(chips)] for half in (held, other)]
    here = place[1] % 2 == 0
    by_core = [
        [jnp.where(here, near, far) for near, far in zip(blocks[core], blocks[1 - core])] for core in range(2)
    ]
    for chip in range(chips):

        @pl.when(place[1] // 2 == chip)
        def _():
            for k in range(2):
                at = slice(k * rank_cols, (k + 1) * rank_cols)
                side = [by_core[core][(s - chip) % chips][:, at] for s in range(chips) for core in range(2)]
                side = jnp.concatenate(side, axis=1).astype(bf16)
                tile[k] = side
    left[...] = tile[0]
    right[...] = tile[1].T

    @pl.when(pl.program_id(0) == place[0] // (span // own))
    def _():
        rows = pl.ds(pl.multiple_of(place[0] % (span // own) * own, own), own)
        own_left[...] = tile[0, rows]
        own_right[...] = tile[1, rows]


def spread_kernel(low, out):
    depth, _, lanes = low.shape
    lanes = lanes - 128
    sums = jnp.sum(low[:, :, lanes:].astype(f32), axis=0)
    lane = lax.broadcasted_iota(jnp.int32, sums.shape, 1)
    squares = jnp.zeros(sums.shape, f32)
    for k in range(2):
        total = jnp.sum(jnp.where(lane // 3 == k, sums, 0.0)[:1], axis=1, keepdims=True)
        for part, value in enumerate(in_three(total)):
            squares = jnp.where(lane == 3 * k + part, value, squares)
    squares = jnp.concatenate([squares] * (lanes // 128), axis=1).astype(bf16)
    for y in range(out.shape[0]):
        out[y, :depth] = low[:, :, :lanes]
        out[y, depth] = squares


def sums_kernel(low, squares):
    depth = low.shape[1] - 1
    sums = jnp.sum(low[:, depth, :, :128].astype(f32), axis=0)[:1]
    squares[...] = jnp.broadcast_to(sums[None], squares.shape)


def final_kernel(
    entries,
    span,
    squares,
    low,
    left,
    right,
    masters,
    own_left,
    own_right,
    query_master,
    out_master,
    query_copy,
    out_copy,
    query_new,
    out_new,
    near_query,
    near_out,
    near_own,
    near_master,
    near_new,
    first,
    second,
    own_arrived,
    left_for,
    own_left_for,
):
    width = left.shape[0]
    cols = first.shape[1]
    own = query_master.shape[0]
    per = span // own
    parts = width // span
    ways = (
        (own_left, near_own.at[0]),
        (own_right, near_own.at[1]),
        (query_master, near_master.at[0]),
        (out_master, near_master.at[1]),
    )
    own_copies = [pltpu.make_async_copy(x, y, own_arrived.at[k]) for k, (x, y) in enumerate(ways)]
    for copy in own_copies:
        copy.start()

    height = low.shape[0]
    rows = low.shape[2]
    group = 16 // rows
    for g in range(0, first.shape[0] // rows, group):
        part = [low[f % height, f // height].astype(f32) for f in range(g, g + group)]
        part = jnp.concatenate(part, axis=0).astype(bf16)
        first[g * rows : (g + group) * rows] = part[:, :cols]
        second[g * rows : (g + group) * rows] = part[:, cols:]
    second_turned = second[...].T

    sums = jnp.sum(squares[...], axis=0)
    lane = lax.broadcasted_iota(jnp.int32, sums.shape, 1)
    scales = []
    for k in range(2):
        total = jnp.sum(jnp.where(lane // 3 == k, sums, 0.0), axis=1, keepdims=True)
        scales.append(0.01 * lax.rsqrt(total / entries + 1e-06))

    sent = []
    for i in range(parts):
        at = pl.ds(i * span, span)
        codes = masters[i * per : (i + 1) * per]
        moved = jnp.dot(left[at], first[...], preferred_element_type=f32)
        kept = decoded(codes[:, :own].reshape(span, cols))
        near_query[at] = (kept - scales[0] * moved).astype(bf16)
        sent.append(pltpu.make_async_copy(near_query.at[at], query_copy.at[at], left_for.at[i, 0]))
        sent[-1].start()
        moved = jnp.dot(second_turned, right[:, at], preferred_element_type=f32)
        kept = decoded(codes[:, own:].reshape(span, cols).T)
        near_out[:, at] = (kept - scales[1] * moved).astype(bf16)
        sent.append(pltpu.make_async_copy(near_out.at[:, at], out_copy.at[:, at], left_for.at[i, 1]))
        sent[-1].start()
    for copy in own_copies:
        copy.wait()
    for k, (step, new) in enumerate(((first, query_new), (second, out_new))):
        moved = jnp.dot(near_own[k], step[...], preferred_element_type=f32)
        near_new[k] = near_master[k] - scales[k] * moved
        sent.append(pltpu.make_async_copy(near_new.at[k], new, own_left_for.at[k]))
        sent[-1].start()
    for copy in sent:
        copy.wait()


def far(value):
    return pltpu.with_memory_space_constraint(value, pltpu.HBM)


def body(
    saved_inputs,
    query_cotangent,
    attn_outputs,
    out_cotangent,
    left_factor,
    right_factor,
    query_master,
    out_master,
    first_moment,
    second_moment,
):
    depth = lax.axis_size("z")
    height = lax.axis_size("y")
    fs = depth * height
    tp = lax.axis_size("tp")
    own, rank_cols = left_factor.shape
    rows = first_moment.shape[1]
    cols = first_moment.shape[2]
    tokens = saved_inputs.shape[0]
    width = fs * own
    ranks = tp * rank_cols
    used = 2 * rank_cols
    kept = own * used // 128

    place = jnp.stack([lax.axis_index(FS), lax.axis_index("tp")]).astype(jnp.int32)
    packed, masters = pl.pallas_call(
        send_kernel,
        out_shape=(
            jax.ShapeDtypeStruct((fs, kept, 128), bf16),
            pltpu.HBM((2 * own, cols), bf16),
        ),
        in_specs=[pl.BlockSpec()] * 4,
        out_specs=(VMEM, VMEM),
        compiler_params=SMALL,
        cost_estimate=cost(1 << 16, 1 << 20),
    )(far(left_factor), far(right_factor), far(query_master), far(out_master.T))
    packed = pl.pallas_call(
        hold_kernel,
        out_shape=jax.ShapeDtypeStruct(packed.shape, bf16),
        in_specs=[ANY, ANY],
        out_specs=ANY,
        input_output_aliases={1: 0},
        compiler_params=SMALL,
        cost_estimate=LONG,
    )(far(masters), packed)
    masters = lax.all_gather(masters, FS)
    packed = lax.all_to_all(packed, FS, 0, 0)
    proj = pl.pallas_call(
        functools.partial(proj_kernel, used),
        out_shape=jax.ShapeDtypeStruct((used, tokens), bf16),
        in_specs=[VMEM] * 3,
        out_specs=VMEM,
        scratch_shapes=[pltpu.VMEM((width, 128), bf16)],
        compiler_params=SMALL,
        cost_estimate=cost(4 * tokens * width * 128, 8 << 20),
    )(packed, saved_inputs, out_cotangent)
    proj = lax.all_gather(proj, "tp", axis=0, tiled=True)

    partial = pl.pallas_call(
        functools.partial(grad_kernel, rank_cols),
        out_shape=pltpu.HBM((height, depth, 2 * rows, cols), bf16),
        in_specs=[VMEM] * 3,
        out_specs=VMEM,
        compiler_params=SMALL,
        cost_estimate=cost(4 * ranks * tokens * cols, 2 << 20),
    )(proj, query_cotangent, attn_outputs)
    pieces = lax.all_to_all(partial, "y", 0, 0)
    pieces = pl.pallas_call(
        fold_kernel,
        out_shape=jax.ShapeDtypeStruct((depth, 2 * rows, cols), f32),
        in_specs=[VMEM],
        out_specs=VMEM,
        compiler_params=SMALL,
        cost_estimate=cost(1 << 20, 1 << 20),
    )(pieces)
    pieces = lax.all_to_all(pieces, "z", 0, 0)

    held = [packed]
    for step in range(1, tp // 2):
        held.append(lax.ppermute(packed, "tp", [((t + 2 * step) % tp, t) for t in range(tp)]))
    held = jnp.stack(held)
    other = lax.ppermute(held, "tp", [(t ^ 1, t) for t in range(tp)])

    first_new, second_new, low = pl.pallas_call(
        moment_kernel,
        out_shape=(
            jax.ShapeDtypeStruct(first_moment.shape, f32),
            jax.ShapeDtypeStruct(second_moment.shape, f32),
            pltpu.HBM((depth, rows, 2 * cols + 128), bf16),
        ),
        in_specs=[VMEM] * 3,
        out_specs=(VMEM, VMEM, VMEM),
        compiler_params=SMALL,
        cost_estimate=cost(1 << 20, 2 << 20),
    )(pieces, first_moment, second_moment)
    low = lax.all_to_all(low, "z", 0, 0)
    low = pl.pallas_call(
        spread_kernel,
        out_shape=pltpu.HBM((height, depth + 1, rows, 2 * cols), bf16),
        in_specs=[VMEM],
        out_specs=VMEM,
        compiler_params=SMALL,
        cost_estimate=cost(1 << 16, 1 << 20),
    )(low)
    low = lax.all_to_all(low, "y", 0, 0)

    span = width // 4
    per = span // own
    left, right, own_left, own_right = pl.pallas_call(
        functools.partial(prep_kernel, rank_cols),
        grid=(width // span,),
        out_shape=(
            pltpu.HBM((width, ranks), bf16),
            pltpu.HBM((ranks, width), bf16),
            pltpu.HBM((own, ranks), bf16),
            pltpu.HBM((own, ranks), bf16),
        ),
        in_specs=[
            SMEM,
            pl.BlockSpec((tp // 2, per, kept, 128), lambda i: (0, i, 0, 0)),
            pl.BlockSpec((tp // 2, per, kept, 128), lambda i: (0, i, 0, 0)),
        ],
        out_specs=(
            pl.BlockSpec((span, ranks), lambda i: (i, 0)),
            pl.BlockSpec((ranks, span), lambda i: (0, i)),
            pl.BlockSpec((own, ranks), lambda i: (0, 0)),
            pl.BlockSpec((own, ranks), lambda i: (0, 0)),
        ),
        scratch_shapes=[pltpu.VMEM((2, span, ranks), bf16)],
        compiler_params=SMALL,
        cost_estimate=cost(1 << 30, 30 << 20),
    )(place, far(held), far(other))

    low, masters = lax.optimization_barrier((low, masters))
    parts = width // span
    squares = pl.pallas_call(
        sums_kernel,
        out_shape=jax.ShapeDtypeStruct((tp, 1, 128), f32),
        in_specs=[VMEM],
        out_specs=VMEM,
        compiler_params=SMALL,
        cost_estimate=LONG,
    )(low)
    squares = lax.all_to_all(squares, "tp", 0, 0)

    query_copy, out_copy, query_new, out_new = pl.pallas_call(
        functools.partial(final_kernel, float(rows * fs * cols * tp), span),
        out_shape=(
            pltpu.HBM((width, cols), bf16),
            pltpu.HBM((cols, width), bf16),
            pltpu.HBM((own, cols), f32),
            pltpu.HBM((own, cols), f32),
        ),
        in_specs=[VMEM] * 5 + [ANY] * 4,
        out_specs=(ANY,) * 4,
        scratch_shapes=[
            pltpu.VMEM((width, cols), bf16),
            pltpu.VMEM((cols, width), bf16),
            pltpu.VMEM((2, own, ranks), bf16),
            pltpu.VMEM((2, own, cols), f32),
            pltpu.VMEM((2, own, cols), f32),
            pltpu.VMEM((ranks, cols), bf16),
            pltpu.VMEM((ranks, cols), bf16),
            pltpu.SemaphoreType.DMA((4,)),
            pltpu.SemaphoreType.DMA((parts, 2)),
            pltpu.SemaphoreType.DMA((2,)),
        ],
        compiler_params=SMALL,
        cost_estimate=cost(4 * width * ranks * cols, 20 << 20),
    )(
        squares,
        low,
        left,
        right,
        masters,
        far(own_left),
        far(own_right),
        far(query_master),
        far(out_master.T),
    )
    return (query_new, out_new.T, query_copy, out_copy, first_new, second_new)


def solution(mesh):
    finer = Mesh(mesh.devices.reshape(12, 8, 8), ("z", "y", "tp"))
    both = P(FS, "tp")
    moment = P(None, FS, "tp")

    return jax.shard_map(
        body,
        mesh=finer,
        in_specs=(P(FS, None), both, both, P(FS, None), both, both, both, P("tp", FS), moment, moment),
        out_specs=(both, P("tp", FS), P(None, "tp"), P("tp", None), moment, moment),
        check_vma=False,
    )
```

```python
import functools

import jax
import jax.numpy as jnp
from jax import lax
from jax.experimental import pallas as pl
from jax.experimental.pallas import tpu as pltpu
from jax.sharding import Mesh
from jax.sharding import PartitionSpec as P


bf16 = jnp.bfloat16
f32 = jnp.float32
FS = ("z", "y")
VMEM = pl.BlockSpec(memory_space=pltpu.VMEM)
ANY = pl.BlockSpec(memory_space=pl.ANY)
SMEM = pl.BlockSpec(memory_space=pltpu.SMEM)
REACH = 2.0**34
SMALL = pltpu.CompilerParams(vmem_limit_bytes=16 << 20)


def cost(flops, nbytes):
    return pl.CostEstimate(flops=flops, bytes_accessed=nbytes, transcendentals=0)


LONG = cost(1 << 35, 1 << 26)


def coded(value):
    size = value * REACH
    size = size * size
    size = size * size
    return jnp.where(value < 0.0, -size, size).astype(bf16)


def decoded(code):
    wide = code.astype(f32)
    size = lax.rsqrt(lax.rsqrt(jnp.abs(wide))) * (1.0 / REACH)
    return jnp.where(wide < 0.0, -size, size)


def send_kernel(left, right, query_master, out_master, out, masters):
    own = query_master.shape[0]
    masters[:own] = coded(query_master[...])
    masters[own:] = coded(out_master[...])
    both = jnp.concatenate([left[...].astype(f32), right[...].astype(f32)], axis=1)
    used = both.shape[1]
    free = 128 - used
    kept = out.shape[1]
    rest = both[kept:]
    tail = jnp.concatenate([rest[:, j : j + free] for j in range(0, used, free)], axis=0)
    packed = jnp.concatenate([both[:kept], tail], axis=1).astype(bf16)
    out[...] = jnp.broadcast_to(packed[None], out.shape)


def copies_kernel(packed, out):
    out[...] = jnp.broadcast_to(packed[...][None], out.shape)


def by_place(packed):
    height, depth = packed.shape[:2]
    return jnp.concatenate([packed[y, z][None] for z in range(depth) for y in range(height)], axis=0)


def hold_kernel(masters, packed, out):
    pass


def unpacked(packed, used):
    free = 128 - used
    parts = used // free
    height = packed.shape[1] // parts
    wide = packed.astype(f32)
    tail = [wide[:, j * height : (j + 1) * height, used:] for j in range(parts)]
    tail = jnp.concatenate(tail + [jnp.zeros_like(tail[0])], axis=2)
    return jnp.concatenate([wide, tail], axis=1)


def proj_kernel(used, packed, saved_inputs, out_cotangent, out, factors):
    depth = packed.shape[1]
    span = factors.shape[0] // depth
    for z in range(depth):
        block = unpacked(by_place(packed[:, z : z + 1]), used).reshape(span, 128)
        factors[z * span : (z + 1) * span] = block.astype(bf16)
    left = jnp.dot(saved_inputs[...], factors[...], preferred_element_type=f32)
    right = jnp.dot(out_cotangent[...], factors[...], preferred_element_type=f32)
    lane = lax.broadcasted_iota(jnp.int32, left.shape, 1)
    out[...] = jnp.where(lane < used // 2, left, right).T[:used].astype(bf16)


def grad_kernel(rank_cols, proj, query_cotangent, attn_outputs, out):
    cols = query_cotangent.shape[1]
    parts = []
    for k, other in enumerate((query_cotangent, attn_outputs)):
        starts = range(k * rank_cols, proj.shape[0], 2 * rank_cols)
        ranks = jnp.concatenate([proj[at : at + rank_cols] for at in starts], axis=0)
        parts.append(jnp.dot(ranks, other[...], preferred_element_type=f32).reshape(-1, 8, cols))
    first, second = parts
    both = jnp.concatenate([first[:, :4], second[:, :4], first[:, 4:], second[:, 4:]], axis=1)
    out[...] = both.astype(bf16)


def in_three(total):
    parts = []
    for _ in range(3):
        parts.append(total.astype(bf16).astype(f32))
        total = total - parts[-1]
    return parts


def moment_kernel(pieces, first, second, first_new, second_new, low):
    rows = first.shape[1]
    grads = jnp.sum(pieces[...].astype(f32), axis=0)
    new_first = 0.9 * jnp.concatenate([first[0], first[1]], axis=0) + 0.1 * grads
    new_second = 0.99 * jnp.concatenate([second[0], second[1]], axis=0) + 0.01 * grads * grads
    direction = new_first / (jnp.sqrt(new_second) + 1e-08)
    first_new[0] = new_first[:rows]
    first_new[1] = new_first[rows:]
    second_new[0] = new_second[:rows]
    second_new[1] = new_second[rows:]
    squares = direction * direction
    lane = lax.broadcasted_iota(jnp.int32, (rows, 128), 1)
    sums = jnp.zeros((rows, 128), f32)
    for k in range(2):
        total = jnp.sum(squares[k * rows : (k + 1) * rows], axis=(0, 1), keepdims=True)
        for part, value in enumerate(in_three(total)):
            sums = jnp.where(lane == 3 * k + part, value, sums)
    sent = jnp.concatenate([direction[:rows], direction[rows:], sums], axis=1).astype(bf16)
    low[...] = jnp.broadcast_to(sent[None], low.shape)


def prep_kernel(rank_cols, place, held, other, left, right, own_left, own_right, tile):
    own = own_left.shape[0]
    span = left.shape[0]
    chips = held.shape[0]
    blocks = [[unpacked(by_place(half[s]), 2 * rank_cols).reshape(span, 128) for s in range(chips)] for half in (held, other)]
    here = place[1] % 2 == 0
    by_core = [
        [jnp.where(here, near, far) for near, far in zip(blocks[core], blocks[1 - core])] for core in range(2)
    ]
    for chip in range(chips):

        @pl.when(place[1] // 2 == chip)
        def _():
            for k in range(2):
                at = slice(k * rank_cols, (k + 1) * rank_cols)
                side = [by_core[core][(s - chip) % chips][:, at] for s in range(chips) for core in range(2)]
                side = jnp.concatenate(side, axis=1).astype(bf16)
                tile[k] = side
    left[...] = tile[0]
    right[...] = tile[1].T

    @pl.when(pl.program_id(0) == place[0] // (span // own))
    def _():
        rows = pl.ds(pl.multiple_of(place[0] % (span // own) * own, own), own)
        own_left[...] = tile[0, rows]
        own_right[...] = tile[1, rows]


def spread_kernel(low, out):
    depth, _, lanes = low.shape
    lanes = lanes - 128
    sums = jnp.sum(low[:, :, lanes:].astype(f32), axis=0)
    lane = lax.broadcasted_iota(jnp.int32, sums.shape, 1)
    squares = jnp.zeros(sums.shape, f32)
    for k in range(2):
        total = jnp.sum(jnp.where(lane // 3 == k, sums, 0.0)[:1], axis=1, keepdims=True)
        for part, value in enumerate(in_three(total)):
            squares = jnp.where(lane == 3 * k + part, value, squares)
    squares = jnp.concatenate([squares] * (lanes // 128), axis=1).astype(bf16)
    for y in range(out.shape[0]):
        out[y, :depth] = low[:, :, :lanes]
        out[y, depth] = squares


def sums_kernel(low, squares):
    depth = low.shape[1] - 1
    sums = jnp.sum(low[:, depth, :, :128].astype(f32), axis=0)[:1]
    squares[...] = jnp.broadcast_to(sums[None], squares.shape)


def final_kernel(
    entries,
    span,
    squares,
    low,
    left,
    right,
    masters,
    own_left,
    own_right,
    query_master,
    out_master,
    query_copy,
    out_copy,
    query_new,
    out_new,
    near_query,
    near_out,
    near_own,
    near_master,
    near_new,
    first,
    second,
    own_arrived,
    left_for,
    own_left_for,
):
    width = left.shape[0]
    cols = first.shape[1]
    own = query_master.shape[0]
    per = span // own
    parts = width // span
    ways = (
        (own_left, near_own.at[0]),
        (own_right, near_own.at[1]),
        (query_master, near_master.at[0]),
        (out_master, near_master.at[1]),
    )
    own_copies = [pltpu.make_async_copy(x, y, own_arrived.at[k]) for k, (x, y) in enumerate(ways)]
    for copy in own_copies:
        copy.start()

    height = low.shape[0]
    rows = low.shape[2]
    group = 16 // rows
    for g in range(0, first.shape[0] // rows, group):
        part = [low[f % height, f // height].astype(f32) for f in range(g, g + group)]
        part = jnp.concatenate(part, axis=0).astype(bf16)
        first[g * rows : (g + group) * rows] = part[:, :cols]
        second[g * rows : (g + group) * rows] = part[:, cols:]
    second_turned = second[...].T

    sums = jnp.sum(squares[...], axis=0)
    lane = lax.broadcasted_iota(jnp.int32, sums.shape, 1)
    scales = []
    for k in range(2):
        total = jnp.sum(jnp.where(lane // 3 == k, sums, 0.0), axis=1, keepdims=True)
        scales.append(0.01 * lax.rsqrt(total / entries + 1e-06))

    sent = []
    for i in range(parts):
        at = pl.ds(i * span, span)
        codes = masters[i * per : (i + 1) * per]
        moved = jnp.dot(left[at], first[...], preferred_element_type=f32)
        kept = decoded(codes[:, :own].reshape(span, cols))
        near_query[at] = (kept - scales[0] * moved).astype(bf16)
        sent.append(pltpu.make_async_copy(near_query.at[at], query_copy.at[at], left_for.at[i, 0]))
        sent[-1].start()
        moved = jnp.dot(second_turned, right[:, at], preferred_element_type=f32)
        kept = decoded(codes[:, own:].reshape(span, cols).T)
        near_out[:, at] = (kept - scales[1] * moved).astype(bf16)
        sent.append(pltpu.make_async_copy(near_out.at[:, at], out_copy.at[:, at], left_for.at[i, 1]))
        sent[-1].start()
    for copy in own_copies:
        copy.wait()
    for k, (step, new) in enumerate(((first, query_new), (second, out_new))):
        moved = jnp.dot(near_own[k], step[...], preferred_element_type=f32)
        near_new[k] = near_master[k] - scales[k] * moved
        sent.append(pltpu.make_async_copy(near_new.at[k], new, own_left_for.at[k]))
        sent[-1].start()
    for copy in sent:
        copy.wait()


def far(value):
    return pltpu.with_memory_space_constraint(value, pltpu.HBM)


def body(
    saved_inputs,
    query_cotangent,
    attn_outputs,
    out_cotangent,
    left_factor,
    right_factor,
    query_master,
    out_master,
    first_moment,
    second_moment,
):
    depth = lax.axis_size("z")
    height = lax.axis_size("y")
    fs = depth * height
    tp = lax.axis_size("tp")
    own, rank_cols = left_factor.shape
    rows = first_moment.shape[1]
    cols = first_moment.shape[2]
    tokens = saved_inputs.shape[0]
    width = fs * own
    ranks = tp * rank_cols
    used = 2 * rank_cols
    kept = own * used // 128

    place = jnp.stack([lax.axis_index(FS), lax.axis_index("tp")]).astype(jnp.int32)
    packed, masters = pl.pallas_call(
        send_kernel,
        out_shape=(
            jax.ShapeDtypeStruct((depth, kept, 128), bf16),
            pltpu.HBM((2 * own, cols), bf16),
        ),
        in_specs=[pl.BlockSpec()] * 4,
        out_specs=(VMEM, VMEM),
        compiler_params=SMALL,
        cost_estimate=cost(1 << 16, 1 << 20),
    )(far(left_factor), far(right_factor), far(query_master), far(out_master.T))
    packed = pl.pallas_call(
        hold_kernel,
        out_shape=jax.ShapeDtypeStruct(packed.shape, bf16),
        in_specs=[ANY, ANY],
        out_specs=ANY,
        input_output_aliases={1: 0},
        compiler_params=SMALL,
        cost_estimate=LONG,
    )(far(masters), packed)
    masters = lax.all_gather(masters, FS)
    packed = lax.all_to_all(packed, "z", 0, 0)
    packed = pl.pallas_call(
        copies_kernel,
        out_shape=jax.ShapeDtypeStruct((height, depth, kept, 128), bf16),
        in_specs=[VMEM],
        out_specs=VMEM,
        compiler_params=SMALL,
        cost_estimate=cost(1 << 16, 1 << 20),
    )(packed)
    packed = lax.all_to_all(packed, "y", 0, 0)
    proj = pl.pallas_call(
        functools.partial(proj_kernel, used),
        out_shape=jax.ShapeDtypeStruct((used, tokens), bf16),
        in_specs=[VMEM] * 3,
        out_specs=VMEM,
        scratch_shapes=[pltpu.VMEM((width, 128), bf16)],
        compiler_params=SMALL,
        cost_estimate=cost(4 * tokens * width * 128, 8 << 20),
    )(packed, saved_inputs, out_cotangent)
    proj = lax.all_gather(proj, "tp", axis=0, tiled=True)

    partial = pl.pallas_call(
        functools.partial(grad_kernel, rank_cols),
        out_shape=pltpu.HBM((fs // 2, 4 * rows, cols), bf16),
        in_specs=[VMEM] * 3,
        out_specs=VMEM,
        compiler_params=SMALL,
        cost_estimate=cost(4 * ranks * tokens * cols, 2 << 20),
    )(proj, query_cotangent, attn_outputs)
    pieces = lax.all_to_all(partial.reshape(fs, 2 * rows, cols), FS, 0, 0)

    held = [packed]
    for step in range(1, tp // 2):
        held.append(lax.ppermute(packed, "tp", [((t + 2 * step) % tp, t) for t in range(tp)]))
    held = jnp.stack(held)
    other = lax.ppermute(held, "tp", [(t ^ 1, t) for t in range(tp)])

    first_new, second_new, low = pl.pallas_call(
        moment_kernel,
        out_shape=(
            jax.ShapeDtypeStruct(first_moment.shape, f32),
            jax.ShapeDtypeStruct(second_moment.shape, f32),
            pltpu.HBM((depth, rows, 2 * cols + 128), bf16),
        ),
        in_specs=[VMEM] * 3,
        out_specs=(VMEM, VMEM, VMEM),
        compiler_params=SMALL,
        cost_estimate=cost(1 << 20, 2 << 20),
    )(pieces, first_moment, second_moment)
    low = lax.all_to_all(low, "z", 0, 0)
    low = pl.pallas_call(
        spread_kernel,
        out_shape=pltpu.HBM((height, depth + 1, rows, 2 * cols), bf16),
        in_specs=[VMEM],
        out_specs=VMEM,
        compiler_params=SMALL,
        cost_estimate=cost(1 << 16, 1 << 20),
    )(low)
    low = lax.all_to_all(low, "y", 0, 0)

    span = width // 4
    per = span // own
    left, right, own_left, own_right = pl.pallas_call(
        functools.partial(prep_kernel, rank_cols),
        grid=(width // span,),
        out_shape=(
            pltpu.HBM((width, ranks), bf16),
            pltpu.HBM((ranks, width), bf16),
            pltpu.HBM((own, ranks), bf16),
            pltpu.HBM((own, ranks), bf16),
        ),
        in_specs=[
            SMEM,
            pl.BlockSpec((tp // 2, height, per // height, kept, 128), lambda i: (0, 0, i, 0, 0)),
            pl.BlockSpec((tp // 2, height, per // height, kept, 128), lambda i: (0, 0, i, 0, 0)),
        ],
        out_specs=(
            pl.BlockSpec((span, ranks), lambda i: (i, 0)),
            pl.BlockSpec((ranks, span), lambda i: (0, i)),
            pl.BlockSpec((own, ranks), lambda i: (0, 0)),
            pl.BlockSpec((own, ranks), lambda i: (0, 0)),
        ),
        scratch_shapes=[pltpu.VMEM((2, span, ranks), bf16)],
        compiler_params=SMALL,
        cost_estimate=cost(1 << 30, 30 << 20),
    )(place, far(held), far(other))

    low, masters = lax.optimization_barrier((low, masters))
    parts = width // span
    squares = pl.pallas_call(
        sums_kernel,
        out_shape=jax.ShapeDtypeStruct((tp, 1, 128), f32),
        in_specs=[VMEM],
        out_specs=VMEM,
        compiler_params=SMALL,
        cost_estimate=LONG,
    )(low)
    squares = lax.all_to_all(squares, "tp", 0, 0)

    query_copy, out_copy, query_new, out_new = pl.pallas_call(
        functools.partial(final_kernel, float(rows * fs * cols * tp), span),
        out_shape=(
            pltpu.HBM((width, cols), bf16),
            pltpu.HBM((cols, width), bf16),
            pltpu.HBM((own, cols), f32),
            pltpu.HBM((own, cols), f32),
        ),
        in_specs=[VMEM] * 5 + [ANY] * 4,
        out_specs=(ANY,) * 4,
        scratch_shapes=[
            pltpu.VMEM((width, cols), bf16),
            pltpu.VMEM((cols, width), bf16),
            pltpu.VMEM((2, own, ranks), bf16),
            pltpu.VMEM((2, own, cols), f32),
            pltpu.VMEM((2, own, cols), f32),
            pltpu.VMEM((ranks, cols), bf16),
            pltpu.VMEM((ranks, cols), bf16),
            pltpu.SemaphoreType.DMA((4,)),
            pltpu.SemaphoreType.DMA((parts, 2)),
            pltpu.SemaphoreType.DMA((2,)),
        ],
        compiler_params=SMALL,
        cost_estimate=cost(4 * width * ranks * cols, 20 << 20),
    )(
        squares,
        low,
        left,
        right,
        masters,
        far(own_left),
        far(own_right),
        far(query_master),
        far(out_master.T),
    )
    return (query_new, out_new.T, query_copy, out_copy, first_new, second_new)


def solution(mesh):
    finer = Mesh(mesh.devices.reshape(12, 8, 8), ("z", "y", "tp"))
    both = P(FS, "tp")
    moment = P(None, FS, "tp")

    return jax.shard_map(
        body,
        mesh=finer,
        in_specs=(P(FS, None), both, both, P(FS, None), both, both, both, P("tp", FS), moment, moment),
        out_specs=(both, P("tp", FS), P(None, "tp"), P("tp", None), moment, moment),
        check_vma=False,
    )
```

```python
import functools

import jax
import jax.numpy as jnp
from jax import lax
from jax.experimental import pallas as pl
from jax.experimental.pallas import tpu as pltpu
from jax.sharding import Mesh
from jax.sharding import PartitionSpec as P


bf16 = jnp.bfloat16
f32 = jnp.float32
FS = ("z", "y")
VMEM = pl.BlockSpec(memory_space=pltpu.VMEM)
ANY = pl.BlockSpec(memory_space=pl.ANY)
SMEM = pl.BlockSpec(memory_space=pltpu.SMEM)
REACH = 2.0**34
SMALL = pltpu.CompilerParams(vmem_limit_bytes=16 << 20)


def cost(flops, nbytes):
    return pl.CostEstimate(flops=flops, bytes_accessed=nbytes, transcendentals=0)


LONG = cost(1 << 35, 1 << 26)


def coded(value):
    size = value * REACH
    size = size * size
    size = size * size
    return jnp.where(value < 0.0, -size, size).astype(bf16)


def decoded(code):
    wide = code.astype(f32)
    size = lax.rsqrt(lax.rsqrt(jnp.abs(wide))) * (1.0 / REACH)
    return jnp.where(wide < 0.0, -size, size)


def send_kernel(left, right, query_master, out_master, out, masters):
    own = query_master.shape[0]
    masters[:own] = coded(query_master[...])
    masters[own:] = coded(out_master[...])
    both = jnp.concatenate([left[...].astype(f32), right[...].astype(f32)], axis=1)
    used = both.shape[1]
    free = 128 - used
    kept = out.shape[1]
    rest = both[kept:]
    tail = jnp.concatenate([rest[:, j : j + free] for j in range(0, used, free)], axis=0)
    packed = jnp.concatenate([both[:kept], tail], axis=1).astype(bf16)
    out[...] = jnp.broadcast_to(packed[None], out.shape)


def copies_kernel(packed, out):
    out[...] = jnp.broadcast_to(packed[...][None], out.shape)


def by_place(packed):
    height, depth = packed.shape[:2]
    return jnp.concatenate([packed[y, z][None] for z in range(depth) for y in range(height)], axis=0)


def hold_kernel(masters, packed, out):
    pass


def unpacked(packed, used):
    free = 128 - used
    parts = used // free
    height = packed.shape[1] // parts
    wide = packed.astype(f32)
    tail = [wide[:, j * height : (j + 1) * height, used:] for j in range(parts)]
    tail = jnp.concatenate(tail + [jnp.zeros_like(tail[0])], axis=2)
    return jnp.concatenate([wide, tail], axis=1)


def proj_kernel(used, packed, saved_inputs, out_cotangent, out, factors):
    depth = packed.shape[1]
    span = factors.shape[0] // depth
    for z in range(depth):
        block = unpacked(by_place(packed[:, z : z + 1]), used).reshape(span, 128)
        factors[z * span : (z + 1) * span] = block.astype(bf16)
    left = jnp.dot(saved_inputs[...], factors[...], preferred_element_type=f32)
    right = jnp.dot(out_cotangent[...], factors[...], preferred_element_type=f32)
    lane = lax.broadcasted_iota(jnp.int32, left.shape, 1)
    out[...] = jnp.where(lane < used // 2, left, right).T[:used].astype(bf16)


def grad_kernel(rank_cols, proj, query_cotangent, attn_outputs, out):
    cols = query_cotangent.shape[1]
    parts = []
    for k, other in enumerate((query_cotangent, attn_outputs)):
        starts = range(k * rank_cols, proj.shape[0], 2 * rank_cols)
        ranks = jnp.concatenate([proj[at : at + rank_cols] for at in starts], axis=0)
        parts.append(jnp.dot(ranks, other[...], preferred_element_type=f32).reshape(-1, 8, cols))
    first, second = parts
    both = jnp.concatenate([first[:, :4], second[:, :4], first[:, 4:], second[:, 4:]], axis=1)
    out[...] = both.astype(bf16)


def in_three(total):
    parts = []
    for _ in range(3):
        parts.append(total.astype(bf16).astype(f32))
        total = total - parts[-1]
    return parts


def moment_kernel(pieces, first, second, first_new, second_new, low):
    rows = first.shape[1]
    grads = jnp.sum(pieces[...].astype(f32), axis=0)
    new_first = 0.9 * jnp.concatenate([first[0], first[1]], axis=0) + 0.1 * grads
    new_second = 0.99 * jnp.concatenate([second[0], second[1]], axis=0) + 0.01 * grads * grads
    direction = new_first / (jnp.sqrt(new_second) + 1e-08)
    first_new[0] = new_first[:rows]
    first_new[1] = new_first[rows:]
    second_new[0] = new_second[:rows]
    second_new[1] = new_second[rows:]
    squares = direction * direction
    lane = lax.broadcasted_iota(jnp.int32, (rows, 128), 1)
    sums = jnp.zeros((rows, 128), f32)
    for k in range(2):
        total = jnp.sum(squares[k * rows : (k + 1) * rows], axis=(0, 1), keepdims=True)
        for part, value in enumerate(in_three(total)):
            sums = jnp.where(lane == 3 * k + part, value, sums)
    sent = jnp.concatenate([direction[:rows], direction[rows:], sums], axis=1).astype(bf16)
    low[...] = jnp.broadcast_to(sent[None], low.shape)


def prep_kernel(rank_cols, place, mine, pair, held, other, left, right, own_left, own_right, tile):
    own = own_left.shape[0]
    span = left.shape[0]
    chips = 1 + held.shape[0]
    here = place[1] % 2 == 0
    same = [mine[...]] + [held[s] for s in range(chips - 1)]
    cross = [pair[...]] + [other[s] for s in range(chips - 1)]
    by_core = [
        [
            unpacked(by_place(jnp.where(here, near, far)), 2 * rank_cols).reshape(span, 128)
            for near, far in zip(*both)
        ]
        for both in ((same, cross), (cross, same))
    ]
    for chip in range(chips):

        @pl.when(place[1] // 2 == chip)
        def _():
            for k in range(2):
                at = slice(k * rank_cols, (k + 1) * rank_cols)
                side = [by_core[core][(s - chip) % chips][:, at] for s in range(chips) for core in range(2)]
                side = jnp.concatenate(side, axis=1).astype(bf16)
                tile[k] = side
    left[...] = tile[0]
    right[...] = tile[1].T

    @pl.when(pl.program_id(0) == place[0] // (span // own))
    def _():
        rows = pl.ds(pl.multiple_of(place[0] % (span // own) * own, own), own)
        own_left[...] = tile[0, rows]
        own_right[...] = tile[1, rows]


def spread_kernel(low, out):
    depth, _, lanes = low.shape
    lanes = lanes - 128
    sums = jnp.sum(low[:, :, lanes:].astype(f32), axis=0)
    lane = lax.broadcasted_iota(jnp.int32, sums.shape, 1)
    squares = jnp.zeros(sums.shape, f32)
    for k in range(2):
        total = jnp.sum(jnp.where(lane // 3 == k, sums, 0.0)[:1], axis=1, keepdims=True)
        for part, value in enumerate(in_three(total)):
            squares = jnp.where(lane == 3 * k + part, value, squares)
    squares = jnp.concatenate([squares] * (lanes // 128), axis=1).astype(bf16)
    for y in range(out.shape[0]):
        out[y, :depth] = low[:, :, :lanes]
        out[y, depth] = squares


def sums_kernel(low, squares):
    depth = low.shape[1] - 1
    sums = jnp.sum(low[:, depth, :, :128].astype(f32), axis=0)[:1]
    squares[...] = jnp.broadcast_to(sums[None], squares.shape)


def final_kernel(
    entries,
    span,
    squares,
    low,
    left,
    right,
    masters,
    own_left,
    own_right,
    query_master,
    out_master,
    query_copy,
    out_copy,
    query_new,
    out_new,
    near_query,
    near_out,
    near_own,
    near_master,
    near_new,
    first,
    second,
    own_arrived,
    left_for,
    own_left_for,
):
    width = left.shape[0]
    cols = first.shape[1]
    own = query_master.shape[0]
    per = span // own
    parts = width // span
    ways = (
        (own_left, near_own.at[0]),
        (own_right, near_own.at[1]),
        (query_master, near_master.at[0]),
        (out_master, near_master.at[1]),
    )
    own_copies = [pltpu.make_async_copy(x, y, own_arrived.at[k]) for k, (x, y) in enumerate(ways)]
    for copy in own_copies:
        copy.start()

    height = low.shape[0]
    rows = low.shape[2]
    group = 16 // rows
    for g in range(0, first.shape[0] // rows, group):
        part = [low[f % height, f // height].astype(f32) for f in range(g, g + group)]
        part = jnp.concatenate(part, axis=0).astype(bf16)
        first[g * rows : (g + group) * rows] = part[:, :cols]
        second[g * rows : (g + group) * rows] = part[:, cols:]
    second_turned = second[...].T

    sums = jnp.sum(squares[...], axis=0)
    lane = lax.broadcasted_iota(jnp.int32, sums.shape, 1)
    scales = []
    for k in range(2):
        total = jnp.sum(jnp.where(lane // 3 == k, sums, 0.0), axis=1, keepdims=True)
        scales.append(0.01 * lax.rsqrt(total / entries + 1e-06))

    sent = []
    for i in range(parts):
        at = pl.ds(i * span, span)
        codes = masters[i * per : (i + 1) * per]
        moved = jnp.dot(left[at], first[...], preferred_element_type=f32)
        kept = decoded(codes[:, :own].reshape(span, cols))
        near_query[at] = (kept - scales[0] * moved).astype(bf16)
        sent.append(pltpu.make_async_copy(near_query.at[at], query_copy.at[at], left_for.at[i, 0]))
        sent[-1].start()
        moved = jnp.dot(second_turned, right[:, at], preferred_element_type=f32)
        kept = decoded(codes[:, own:].reshape(span, cols).T)
        near_out[:, at] = (kept - scales[1] * moved).astype(bf16)
        sent.append(pltpu.make_async_copy(near_out.at[:, at], out_copy.at[:, at], left_for.at[i, 1]))
        sent[-1].start()
    for copy in own_copies:
        copy.wait()
    for k, (step, new) in enumerate(((first, query_new), (second, out_new))):
        moved = jnp.dot(near_own[k], step[...], preferred_element_type=f32)
        near_new[k] = near_master[k] - scales[k] * moved
        sent.append(pltpu.make_async_copy(near_new.at[k], new, own_left_for.at[k]))
        sent[-1].start()
    for copy in sent:
        copy.wait()


def far(value):
    return pltpu.with_memory_space_constraint(value, pltpu.HBM)


def body(
    saved_inputs,
    query_cotangent,
    attn_outputs,
    out_cotangent,
    left_factor,
    right_factor,
    query_master,
    out_master,
    first_moment,
    second_moment,
):
    depth = lax.axis_size("z")
    height = lax.axis_size("y")
    fs = depth * height
    tp = lax.axis_size("tp")
    own, rank_cols = left_factor.shape
    rows = first_moment.shape[1]
    cols = first_moment.shape[2]
    tokens = saved_inputs.shape[0]
    width = fs * own
    ranks = tp * rank_cols
    used = 2 * rank_cols
    kept = own * used // 128

    place = jnp.stack([lax.axis_index(FS), lax.axis_index("tp")]).astype(jnp.int32)
    packed, masters = pl.pallas_call(
        send_kernel,
        out_shape=(
            jax.ShapeDtypeStruct((depth, kept, 128), bf16),
            pltpu.HBM((2 * own, cols), bf16),
        ),
        in_specs=[pl.BlockSpec()] * 4,
        out_specs=(VMEM, VMEM),
        compiler_params=SMALL,
        cost_estimate=cost(1 << 16, 1 << 20),
    )(far(left_factor), far(right_factor), far(query_master), far(out_master.T))
    packed = pl.pallas_call(
        hold_kernel,
        out_shape=jax.ShapeDtypeStruct(packed.shape, bf16),
        in_specs=[ANY, ANY],
        out_specs=ANY,
        input_output_aliases={1: 0},
        compiler_params=SMALL,
        cost_estimate=LONG,
    )(far(masters), packed)
    masters = lax.all_gather(masters, FS)
    packed = lax.all_to_all(packed, "z", 0, 0)
    packed = pl.pallas_call(
        copies_kernel,
        out_shape=jax.ShapeDtypeStruct((height, depth, kept, 128), bf16),
        in_specs=[VMEM],
        out_specs=VMEM,
        compiler_params=SMALL,
        cost_estimate=cost(1 << 16, 1 << 20),
    )(packed)
    packed = lax.all_to_all(packed, "y", 0, 0)
    proj = pl.pallas_call(
        functools.partial(proj_kernel, used),
        out_shape=jax.ShapeDtypeStruct((used, tokens), bf16),
        in_specs=[VMEM] * 3,
        out_specs=VMEM,
        scratch_shapes=[pltpu.VMEM((width, 128), bf16)],
        compiler_params=SMALL,
        cost_estimate=cost(4 * tokens * width * 128, 8 << 20),
    )(packed, saved_inputs, out_cotangent)
    proj = lax.all_gather(proj, "tp", axis=0, tiled=True)

    partial = pl.pallas_call(
        functools.partial(grad_kernel, rank_cols),
        out_shape=pltpu.HBM((fs // 2, 4 * rows, cols), bf16),
        in_specs=[VMEM] * 3,
        out_specs=VMEM,
        compiler_params=SMALL,
        cost_estimate=cost(4 * ranks * tokens * cols, 2 << 20),
    )(proj, query_cotangent, attn_outputs)
    pieces = lax.all_to_all(partial.reshape(fs, 2 * rows, cols), FS, 0, 0)

    swap = [(t ^ 1, t) for t in range(tp)]
    pair = lax.ppermute(packed, "tp", swap)
    held = []
    for step in range(1, tp // 2):
        held.append(lax.ppermute(packed, "tp", [((t + 2 * step) % tp, t) for t in range(tp)]))
    held = jnp.stack(held)
    other = lax.ppermute(held, "tp", swap)

    first_new, second_new, low = pl.pallas_call(
        moment_kernel,
        out_shape=(
            jax.ShapeDtypeStruct(first_moment.shape, f32),
            jax.ShapeDtypeStruct(second_moment.shape, f32),
            jax.ShapeDtypeStruct((depth, rows, 2 * cols + 128), bf16),
        ),
        in_specs=[VMEM] * 3,
        out_specs=(VMEM, VMEM, VMEM),
        compiler_params=SMALL,
        cost_estimate=cost(1 << 20, 2 << 20),
    )(pieces, first_moment, second_moment)
    low = lax.all_to_all(low, "z", 0, 0)
    low = pl.pallas_call(
        spread_kernel,
        out_shape=pltpu.HBM((height, depth + 1, rows, 2 * cols), bf16),
        in_specs=[VMEM],
        out_specs=VMEM,
        compiler_params=SMALL,
        cost_estimate=cost(1 << 16, 1 << 20),
    )(low)
    low = lax.all_to_all(low, "y", 0, 0)

    span = width // 4
    per = span // own
    left, right, own_left, own_right = pl.pallas_call(
        functools.partial(prep_kernel, rank_cols),
        grid=(width // span,),
        out_shape=(
            pltpu.HBM((width, ranks), bf16),
            pltpu.HBM((ranks, width), bf16),
            pltpu.HBM((own, ranks), bf16),
            pltpu.HBM((own, ranks), bf16),
        ),
        in_specs=[
            SMEM,
            pl.BlockSpec((height, per // height, kept, 128), lambda i: (0, i, 0, 0)),
            pl.BlockSpec((height, per // height, kept, 128), lambda i: (0, i, 0, 0)),
            pl.BlockSpec((tp // 2 - 1, height, per // height, kept, 128), lambda i: (0, 0, i, 0, 0)),
            pl.BlockSpec((tp // 2 - 1, height, per // height, kept, 128), lambda i: (0, 0, i, 0, 0)),
        ],
        out_specs=(
            pl.BlockSpec((span, ranks), lambda i: (i, 0)),
            pl.BlockSpec((ranks, span), lambda i: (0, i)),
            pl.BlockSpec((own, ranks), lambda i: (0, 0)),
            pl.BlockSpec((own, ranks), lambda i: (0, 0)),
        ),
        scratch_shapes=[pltpu.VMEM((2, span, ranks), bf16)],
        compiler_params=SMALL,
        cost_estimate=cost(1 << 30, 30 << 20),
    )(place, far(packed), far(pair), far(held), far(other))

    low, masters = lax.optimization_barrier((low, masters))
    parts = width // span
    squares = pl.pallas_call(
        sums_kernel,
        out_shape=jax.ShapeDtypeStruct((tp, 1, 128), f32),
        in_specs=[VMEM],
        out_specs=VMEM,
        compiler_params=SMALL,
        cost_estimate=LONG,
    )(low)
    squares = lax.all_to_all(squares, "tp", 0, 0)

    query_copy, out_copy, query_new, out_new = pl.pallas_call(
        functools.partial(final_kernel, float(rows * fs * cols * tp), span),
        out_shape=(
            pltpu.HBM((width, cols), bf16),
            pltpu.HBM((cols, width), bf16),
            pltpu.HBM((own, cols), f32),
            pltpu.HBM((own, cols), f32),
        ),
        in_specs=[VMEM] * 5 + [ANY] * 4,
        out_specs=(ANY,) * 4,
        scratch_shapes=[
            pltpu.VMEM((width, cols), bf16),
            pltpu.VMEM((cols, width), bf16),
            pltpu.VMEM((2, own, ranks), bf16),
            pltpu.VMEM((2, own, cols), f32),
            pltpu.VMEM((2, own, cols), f32),
            pltpu.VMEM((ranks, cols), bf16),
            pltpu.VMEM((ranks, cols), bf16),
            pltpu.SemaphoreType.DMA((4,)),
            pltpu.SemaphoreType.DMA((parts, 2)),
            pltpu.SemaphoreType.DMA((2,)),
        ],
        compiler_params=SMALL,
        cost_estimate=cost(4 * width * ranks * cols, 20 << 20),
    )(
        squares,
        low,
        left,
        right,
        masters,
        far(own_left),
        far(own_right),
        far(query_master),
        far(out_master.T),
    )
    return (query_new, out_new.T, query_copy, out_copy, first_new, second_new)


def solution(mesh):
    finer = Mesh(mesh.devices.reshape(12, 8, 8), ("z", "y", "tp"))
    both = P(FS, "tp")
    moment = P(None, FS, "tp")

    return jax.shard_map(
        body,
        mesh=finer,
        in_specs=(P(FS, None), both, both, P(FS, None), both, both, both, P("tp", FS), moment, moment),
        out_specs=(both, P("tp", FS), P(None, "tp"), P("tp", None), moment, moment),
        check_vma=False,
    )
```

```python
import functools

import jax
import jax.numpy as jnp
from jax import lax
from jax.experimental import pallas as pl
from jax.experimental.pallas import tpu as pltpu
from jax.sharding import Mesh
from jax.sharding import PartitionSpec as P


bf16 = jnp.bfloat16
f32 = jnp.float32
FS = ("z", "y")
VMEM = pl.BlockSpec(memory_space=pltpu.VMEM)
ANY = pl.BlockSpec(memory_space=pl.ANY)
SMEM = pl.BlockSpec(memory_space=pltpu.SMEM)
REACH = 2.0**34
SMALL = pltpu.CompilerParams(vmem_limit_bytes=16 << 20)


def cost(flops, nbytes):
    return pl.CostEstimate(flops=flops, bytes_accessed=nbytes, transcendentals=0)


LONG = cost(1 << 35, 1 << 26)


def coded(value, reach=REACH):
    size = value * reach
    size = size * size
    size = size * size
    return jnp.where(value < 0.0, -size, size).astype(bf16)


def decoded(code, reach=REACH):
    wide = code.astype(f32)
    size = lax.rsqrt(lax.rsqrt(jnp.abs(wide))) * (1.0 / reach)
    return jnp.where(wide < 0.0, -size, size)


def send_kernel(left, right, query_master, out_master, out, masters):
    own = query_master.shape[0]
    masters[:own] = coded(query_master[...])
    masters[own:] = coded(out_master[...])
    both = jnp.concatenate([left[...].astype(f32), right[...].astype(f32)], axis=1)
    used = both.shape[1]
    free = 128 - used
    kept = out.shape[1]
    rest = both[kept:]
    tail = jnp.concatenate([rest[:, j : j + free] for j in range(0, used, free)], axis=0)
    packed = jnp.concatenate([both[:kept], tail], axis=1).astype(bf16)
    out[...] = jnp.broadcast_to(packed[None], out.shape)


def copies_kernel(packed, out):
    out[...] = jnp.broadcast_to(packed[...][None], out.shape)


def by_place(packed):
    height, depth = packed.shape[:2]
    return jnp.concatenate([packed[y, z][None] for z in range(depth) for y in range(height)], axis=0)


def hold_kernel(masters, packed, out):
    pass


def unpacked(packed, used):
    free = 128 - used
    parts = used // free
    height = packed.shape[1] // parts
    wide = packed.astype(f32)
    tail = [wide[:, j * height : (j + 1) * height, used:] for j in range(parts)]
    tail = jnp.concatenate(tail + [jnp.zeros_like(tail[0])], axis=2)
    return jnp.concatenate([wide, tail], axis=1)


def proj_kernel(used, packed, saved_inputs, out_cotangent, out, factors):
    depth = packed.shape[1]
    span = factors.shape[0] // depth
    for z in range(depth):
        block = unpacked(by_place(packed[:, z : z + 1]), used).reshape(span, 128)
        factors[z * span : (z + 1) * span] = block.astype(bf16)
    left = jnp.dot(saved_inputs[...], factors[...], preferred_element_type=f32)
    right = jnp.dot(out_cotangent[...], factors[...], preferred_element_type=f32)
    lane = lax.broadcasted_iota(jnp.int32, left.shape, 1)
    out[...] = jnp.where(lane < used // 2, left, right).T[:used].astype(bf16)


def grad_kernel(rank_cols, proj, query_cotangent, attn_outputs, out):
    cols = query_cotangent.shape[1]
    parts = []
    for k, other in enumerate((query_cotangent, attn_outputs)):
        starts = range(k * rank_cols, proj.shape[0], 2 * rank_cols)
        ranks = jnp.concatenate([proj[at : at + rank_cols] for at in starts], axis=0)
        parts.append(jnp.dot(ranks, other[...], preferred_element_type=f32).reshape(-1, 8, cols))
    first, second = parts
    both = jnp.concatenate([first[:, :4], second[:, :4], first[:, 4:], second[:, 4:]], axis=1)
    height, depth = out.shape[:2]
    both = both.astype(bf16).reshape(depth, height // 2, 16, cols)
    for y in range(0, height, 2):
        out[y] = both[:, y // 2, :8]
        out[y + 1] = both[:, y // 2, 8:]


def fold_kernel(pieces, out):
    out[...] = coded(jnp.sum(pieces[...].astype(f32), axis=0), 1.0)


def in_three(total):
    parts = []
    for _ in range(3):
        parts.append(total.astype(bf16).astype(f32))
        total = total - parts[-1]
    return parts


def moment_kernel(pieces, first, second, first_new, second_new, low):
    rows = first.shape[1]
    grads = jnp.sum(decoded(pieces[...], 1.0), axis=0)
    new_first = 0.9 * jnp.concatenate([first[0], first[1]], axis=0) + 0.1 * grads
    new_second = 0.99 * jnp.concatenate([second[0], second[1]], axis=0) + 0.01 * grads * grads
    direction = new_first / (jnp.sqrt(new_second) + 1e-08)
    first_new[0] = new_first[:rows]
    first_new[1] = new_first[rows:]
    second_new[0] = new_second[:rows]
    second_new[1] = new_second[rows:]
    squares = direction * direction
    lane = lax.broadcasted_iota(jnp.int32, (rows, 128), 1)
    sums = jnp.zeros((rows, 128), f32)
    for k in range(2):
        total = jnp.sum(squares[k * rows : (k + 1) * rows], axis=(0, 1), keepdims=True)
        for part, value in enumerate(in_three(total)):
            sums = jnp.where(lane == 3 * k + part, value, sums)
    sent = jnp.concatenate([direction[:rows], direction[rows:], sums], axis=1).astype(bf16)
    low[...] = jnp.broadcast_to(sent[None], low.shape)


def prep_kernel(rank_cols, place, held, other, left, right, own_left, own_right, tile):
    own = own_left.shape[0]
    span = left.shape[0]
    chips = held.shape[0]
    blocks = [[unpacked(by_place(half[s]), 2 * rank_cols).reshape(span, 128) for s in range(chips)] for half in (held, other)]
    here = place[1] % 2 == 0
    by_core = [
        [jnp.where(here, near, far) for near, far in zip(blocks[core], blocks[1 - core])] for core in range(2)
    ]
    for chip in range(chips):

        @pl.when(place[1] // 2 == chip)
        def _():
            for k in range(2):
                at = slice(k * rank_cols, (k + 1) * rank_cols)
                side = [by_core[core][(s - chip) % chips][:, at] for s in range(chips) for core in range(2)]
                side = jnp.concatenate(side, axis=1).astype(bf16)
                tile[k] = side
    left[...] = tile[0]
    right[...] = tile[1].T

    @pl.when(pl.program_id(0) == place[0] // (span // own))
    def _():
        rows = pl.ds(pl.multiple_of(place[0] % (span // own) * own, own), own)
        own_left[...] = tile[0, rows]
        own_right[...] = tile[1, rows]


def spread_kernel(low, out):
    depth, _, lanes = low.shape
    lanes = lanes - 128
    sums = jnp.sum(low[:, :, lanes:].astype(f32), axis=0)
    lane = lax.broadcasted_iota(jnp.int32, sums.shape, 1)
    squares = jnp.zeros(sums.shape, f32)
    for k in range(2):
        total = jnp.sum(jnp.where(lane // 3 == k, sums, 0.0)[:1], axis=1, keepdims=True)
        for part, value in enumerate(in_three(total)):
            squares = jnp.where(lane == 3 * k + part, value, squares)
    squares = jnp.concatenate([squares] * (lanes // 128), axis=1).astype(bf16)
    for y in range(out.shape[0]):
        out[y, :depth] = low[:, :, :lanes]
        out[y, depth] = squares


def sums_kernel(low, squares):
    depth = low.shape[1] - 1
    sums = jnp.sum(low[:, depth, :, :128].astype(f32), axis=0)[:1]
    squares[...] = jnp.broadcast_to(sums[None], squares.shape)


def final_kernel(
    entries,
    span,
    squares,
    low,
    left,
    right,
    masters,
    own_left,
    own_right,
    query_master,
    out_master,
    query_copy,
    out_copy,
    query_new,
    out_new,
    near_query,
    near_out,
    near_own,
    near_master,
    near_new,
    first,
    second,
    own_arrived,
    left_for,
    own_left_for,
):
    width = left.shape[0]
    cols = first.shape[1]
    own = query_master.shape[0]
    per = span // own
    parts = width // span
    ways = (
        (own_left, near_own.at[0]),
        (own_right, near_own.at[1]),
        (query_master, near_master.at[0]),
        (out_master, near_master.at[1]),
    )
    own_copies = [pltpu.make_async_copy(x, y, own_arrived.at[k]) for k, (x, y) in enumerate(ways)]
    for copy in own_copies:
        copy.start()

    height = low.shape[0]
    rows = low.shape[2]
    group = 16 // rows
    for g in range(0, first.shape[0] // rows, group):
        part = [low[f % height, f // height].astype(f32) for f in range(g, g + group)]
        part = jnp.concatenate(part, axis=0).astype(bf16)
        first[g * rows : (g + group) * rows] = part[:, :cols]
        second[g * rows : (g + group) * rows] = part[:, cols:]
    second_turned = second[...].T

    sums = jnp.sum(squares[...], axis=0)
    lane = lax.broadcasted_iota(jnp.int32, sums.shape, 1)
    scales = []
    for k in range(2):
        total = jnp.sum(jnp.where(lane // 3 == k, sums, 0.0), axis=1, keepdims=True)
        scales.append(0.01 * lax.rsqrt(total / entries + 1e-06))

    sent = []
    for i in range(parts):
        at = pl.ds(i * span, span)
        codes = masters[i * per : (i + 1) * per]
        moved = jnp.dot(left[at], first[...], preferred_element_type=f32)
        kept = decoded(codes[:, :own].reshape(span, cols))
        near_query[at] = (kept - scales[0] * moved).astype(bf16)
        sent.append(pltpu.make_async_copy(near_query.at[at], query_copy.at[at], left_for.at[i, 0]))
        sent[-1].start()
        moved = jnp.dot(second_turned, right[:, at], preferred_element_type=f32)
        kept = decoded(codes[:, own:].reshape(span, cols).T)
        near_out[:, at] = (kept - scales[1] * moved).astype(bf16)
        sent.append(pltpu.make_async_copy(near_out.at[:, at], out_copy.at[:, at], left_for.at[i, 1]))
        sent[-1].start()
    for copy in own_copies:
        copy.wait()
    for k, (step, new) in enumerate(((first, query_new), (second, out_new))):
        moved = jnp.dot(near_own[k], step[...], preferred_element_type=f32)
        near_new[k] = near_master[k] - scales[k] * moved
        sent.append(pltpu.make_async_copy(near_new.at[k], new, own_left_for.at[k]))
        sent[-1].start()
    for copy in sent:
        copy.wait()


def far(value):
    return pltpu.with_memory_space_constraint(value, pltpu.HBM)


def body(
    saved_inputs,
    query_cotangent,
    attn_outputs,
    out_cotangent,
    left_factor,
    right_factor,
    query_master,
    out_master,
    first_moment,
    second_moment,
):
    depth = lax.axis_size("z")
    height = lax.axis_size("y")
    fs = depth * height
    tp = lax.axis_size("tp")
    own, rank_cols = left_factor.shape
    rows = first_moment.shape[1]
    cols = first_moment.shape[2]
    tokens = saved_inputs.shape[0]
    width = fs * own
    ranks = tp * rank_cols
    used = 2 * rank_cols
    kept = own * used // 128

    place = jnp.stack([lax.axis_index(FS), lax.axis_index("tp")]).astype(jnp.int32)
    packed, masters = pl.pallas_call(
        send_kernel,
        out_shape=(
            jax.ShapeDtypeStruct((depth, kept, 128), bf16),
            pltpu.HBM((2 * own, cols), bf16),
        ),
        in_specs=[pl.BlockSpec()] * 4,
        out_specs=(VMEM, VMEM),
        compiler_params=SMALL,
        cost_estimate=cost(1 << 16, 1 << 20),
    )(far(left_factor), far(right_factor), far(query_master), far(out_master.T))
    packed = pl.pallas_call(
        hold_kernel,
        out_shape=jax.ShapeDtypeStruct(packed.shape, bf16),
        in_specs=[ANY, ANY],
        out_specs=ANY,
        input_output_aliases={1: 0},
        compiler_params=SMALL,
        cost_estimate=LONG,
    )(far(masters), packed)
    masters = lax.all_gather(masters, FS)
    packed = lax.all_to_all(packed, "z", 0, 0)
    packed = pl.pallas_call(
        copies_kernel,
        out_shape=jax.ShapeDtypeStruct((height, depth, kept, 128), bf16),
        in_specs=[VMEM],
        out_specs=VMEM,
        compiler_params=SMALL,
        cost_estimate=cost(1 << 16, 1 << 20),
    )(packed)
    packed = lax.all_to_all(packed, "y", 0, 0)
    proj = pl.pallas_call(
        functools.partial(proj_kernel, used),
        out_shape=jax.ShapeDtypeStruct((used, tokens), bf16),
        in_specs=[VMEM] * 3,
        out_specs=VMEM,
        scratch_shapes=[pltpu.VMEM((width, 128), bf16)],
        compiler_params=SMALL,
        cost_estimate=cost(4 * tokens * width * 128, 8 << 20),
    )(packed, saved_inputs, out_cotangent)
    proj = lax.all_gather(proj, "tp", axis=0, tiled=True)

    partial = pl.pallas_call(
        functools.partial(grad_kernel, rank_cols),
        out_shape=pltpu.HBM((height, depth, 2 * rows, cols), bf16),
        in_specs=[VMEM] * 3,
        out_specs=VMEM,
        compiler_params=SMALL,
        cost_estimate=cost(4 * ranks * tokens * cols, 2 << 20),
    )(proj, query_cotangent, attn_outputs)
    pieces = lax.all_to_all(partial, "y", 0, 0)
    pieces = pl.pallas_call(
        fold_kernel,
        out_shape=jax.ShapeDtypeStruct((depth, 2 * rows, cols), bf16),
        in_specs=[VMEM],
        out_specs=VMEM,
        compiler_params=SMALL,
        cost_estimate=cost(1 << 20, 1 << 20),
    )(pieces)
    pieces = lax.all_to_all(pieces, "z", 0, 0)

    held = [packed]
    for step in range(1, tp // 2):
        held.append(lax.ppermute(packed, "tp", [((t + 2 * step) % tp, t) for t in range(tp)]))
    held = jnp.stack(held)
    other = lax.ppermute(held, "tp", [(t ^ 1, t) for t in range(tp)])

    first_new, second_new, low = pl.pallas_call(
        moment_kernel,
        out_shape=(
            jax.ShapeDtypeStruct(first_moment.shape, f32),
            jax.ShapeDtypeStruct(second_moment.shape, f32),
            pltpu.HBM((depth, rows, 2 * cols + 128), bf16),
        ),
        in_specs=[VMEM] * 3,
        out_specs=(VMEM, VMEM, VMEM),
        compiler_params=SMALL,
        cost_estimate=cost(1 << 20, 2 << 20),
    )(pieces, first_moment, second_moment)
    low = lax.all_to_all(low, "z", 0, 0)
    low = pl.pallas_call(
        spread_kernel,
        out_shape=pltpu.HBM((height, depth + 1, rows, 2 * cols), bf16),
        in_specs=[VMEM],
        out_specs=VMEM,
        compiler_params=SMALL,
        cost_estimate=cost(1 << 16, 1 << 20),
    )(low)
    low = lax.all_to_all(low, "y", 0, 0)

    span = width // 4
    per = span // own
    left, right, own_left, own_right = pl.pallas_call(
        functools.partial(prep_kernel, rank_cols),
        grid=(width // span,),
        out_shape=(
            pltpu.HBM((width, ranks), bf16),
            pltpu.HBM((ranks, width), bf16),
            pltpu.HBM((own, ranks), bf16),
            pltpu.HBM((own, ranks), bf16),
        ),
        in_specs=[
            SMEM,
            pl.BlockSpec((tp // 2, height, per // height, kept, 128), lambda i: (0, 0, i, 0, 0)),
            pl.BlockSpec((tp // 2, height, per // height, kept, 128), lambda i: (0, 0, i, 0, 0)),
        ],
        out_specs=(
            pl.BlockSpec((span, ranks), lambda i: (i, 0)),
            pl.BlockSpec((ranks, span), lambda i: (0, i)),
            pl.BlockSpec((own, ranks), lambda i: (0, 0)),
            pl.BlockSpec((own, ranks), lambda i: (0, 0)),
        ),
        scratch_shapes=[pltpu.VMEM((2, span, ranks), bf16)],
        compiler_params=SMALL,
        cost_estimate=cost(1 << 30, 30 << 20),
    )(place, far(held), far(other))

    low, masters = lax.optimization_barrier((low, masters))
    parts = width // span
    squares = pl.pallas_call(
        sums_kernel,
        out_shape=jax.ShapeDtypeStruct((tp, 1, 128), f32),
        in_specs=[VMEM],
        out_specs=VMEM,
        compiler_params=SMALL,
        cost_estimate=LONG,
    )(low)
    squares = lax.all_to_all(squares, "tp", 0, 0)

    query_copy, out_copy, query_new, out_new = pl.pallas_call(
        functools.partial(final_kernel, float(rows * fs * cols * tp), span),
        out_shape=(
            pltpu.HBM((width, cols), bf16),
            pltpu.HBM((cols, width), bf16),
            pltpu.HBM((own, cols), f32),
            pltpu.HBM((own, cols), f32),
        ),
        in_specs=[VMEM] * 5 + [ANY] * 4,
        out_specs=(ANY,) * 4,
        scratch_shapes=[
            pltpu.VMEM((width, cols), bf16),
            pltpu.VMEM((cols, width), bf16),
            pltpu.VMEM((2, own, ranks), bf16),
            pltpu.VMEM((2, own, cols), f32),
            pltpu.VMEM((2, own, cols), f32),
            pltpu.VMEM((ranks, cols), bf16),
            pltpu.VMEM((ranks, cols), bf16),
            pltpu.SemaphoreType.DMA((4,)),
            pltpu.SemaphoreType.DMA((parts, 2)),
            pltpu.SemaphoreType.DMA((2,)),
        ],
        compiler_params=SMALL,
        cost_estimate=cost(4 * width * ranks * cols, 20 << 20),
    )(
        squares,
        low,
        left,
        right,
        masters,
        far(own_left),
        far(own_right),
        far(query_master),
        far(out_master.T),
    )
    return (query_new, out_new.T, query_copy, out_copy, first_new, second_new)


def solution(mesh):
    finer = Mesh(mesh.devices.reshape(12, 8, 8), ("z", "y", "tp"))
    both = P(FS, "tp")
    moment = P(None, FS, "tp")

    return jax.shard_map(
        body,
        mesh=finer,
        in_specs=(P(FS, None), both, both, P(FS, None), both, both, both, P("tp", FS), moment, moment),
        out_specs=(both, P("tp", FS), P(None, "tp"), P("tp", None), moment, moment),
        check_vma=False,
    )
```

```python
import functools

import jax
import jax.numpy as jnp
from jax import lax
from jax.experimental import pallas as pl
from jax.experimental.pallas import tpu as pltpu
from jax.sharding import Mesh
from jax.sharding import PartitionSpec as P


bf16 = jnp.bfloat16
f32 = jnp.float32
FS = ("z", "y")
VMEM = pl.BlockSpec(memory_space=pltpu.VMEM)
ANY = pl.BlockSpec(memory_space=pl.ANY)
SMEM = pl.BlockSpec(memory_space=pltpu.SMEM)
REACH = 2.0**34
GRAD_REACH = 2.0**10
SMALL = pltpu.CompilerParams(vmem_limit_bytes=16 << 20)


def cost(flops, nbytes):
    return pl.CostEstimate(flops=flops, bytes_accessed=nbytes, transcendentals=0)


LONG = cost(1 << 35, 1 << 26)


def coded(value, reach):
    size = value * reach
    size = size * size
    size = size * size
    return jnp.where(value < 0.0, -size, size).astype(bf16)


def decoded(code, reach):
    wide = code.astype(f32)
    size = lax.rsqrt(lax.rsqrt(jnp.abs(wide))) * (1.0 / reach)
    return jnp.where(wide < 0.0, -size, size)


def send_kernel(left, right, query_master, out_master, out, masters):
    own = query_master.shape[0]
    masters[:own] = coded(query_master[...], REACH)
    masters[own:] = coded(out_master[...], REACH)
    both = jnp.concatenate([left[...].astype(f32), right[...].astype(f32)], axis=1)
    used = both.shape[1]
    free = 128 - used
    kept = out.shape[1]
    rest = both[kept:]
    tail = jnp.concatenate([rest[:, j : j + free] for j in range(0, used, free)], axis=0)
    packed = jnp.concatenate([both[:kept], tail], axis=1).astype(bf16)
    out[...] = jnp.broadcast_to(packed[None], out.shape)


def copies_kernel(packed, out):
    out[...] = jnp.broadcast_to(packed[...][None], out.shape)


def by_place(packed):
    height, depth = packed.shape[:2]
    return jnp.concatenate([packed[y, z][None] for z in range(depth) for y in range(height)], axis=0)


def hold_kernel(masters, packed, out):
    pass


def unpacked(packed, used):
    free = 128 - used
    parts = used // free
    height = packed.shape[1] // parts
    wide = packed.astype(f32)
    tail = [wide[:, j * height : (j + 1) * height, used:] for j in range(parts)]
    tail = jnp.concatenate(tail + [jnp.zeros_like(tail[0])], axis=2)
    return jnp.concatenate([wide, tail], axis=1)


def proj_kernel(used, packed, saved_inputs, out_cotangent, out, factors):
    depth = packed.shape[1]
    span = factors.shape[0] // depth
    for z in range(depth):
        block = unpacked(by_place(packed[:, z : z + 1]), used).reshape(span, 128)
        factors[z * span : (z + 1) * span] = block.astype(bf16)
    left = jnp.dot(saved_inputs[...], factors[...], preferred_element_type=f32)
    right = jnp.dot(out_cotangent[...], factors[...], preferred_element_type=f32)
    lane = lax.broadcasted_iota(jnp.int32, left.shape, 1)
    out[...] = jnp.where(lane < used // 2, left, right).T[:used].astype(bf16)


def grad_kernel(rank_cols, proj, query_cotangent, attn_outputs, out):
    cols = query_cotangent.shape[1]
    parts = []
    for k, other in enumerate((query_cotangent, attn_outputs)):
        starts = range(k * rank_cols, proj.shape[0], 2 * rank_cols)
        ranks = jnp.concatenate([proj[at : at + rank_cols] for at in starts], axis=0)
        parts.append(jnp.dot(ranks, other[...], preferred_element_type=f32).reshape(-1, 8, cols))
    first, second = parts
    both = jnp.concatenate([first[:, :4], second[:, :4], first[:, 4:], second[:, 4:]], axis=1)
    out[...] = coded(both, GRAD_REACH)


def in_three(total):
    parts = []
    for _ in range(3):
        parts.append(total.astype(bf16).astype(f32))
        total = total - parts[-1]
    return parts


def moment_kernel(pieces, first, second, first_new, second_new, low):
    rows = first.shape[1]
    grads = jnp.sum(decoded(pieces[...], GRAD_REACH), axis=0)
    new_first = 0.9 * jnp.concatenate([first[0], first[1]], axis=0) + 0.1 * grads
    new_second = 0.99 * jnp.concatenate([second[0], second[1]], axis=0) + 0.01 * grads * grads
    direction = new_first / (jnp.sqrt(new_second) + 1e-08)
    first_new[0] = new_first[:rows]
    first_new[1] = new_first[rows:]
    second_new[0] = new_second[:rows]
    second_new[1] = new_second[rows:]
    squares = direction * direction
    lane = lax.broadcasted_iota(jnp.int32, (rows, 128), 1)
    sums = jnp.zeros((rows, 128), f32)
    for k in range(2):
        total = jnp.sum(squares[k * rows : (k + 1) * rows], axis=(0, 1), keepdims=True)
        for part, value in enumerate(in_three(total)):
            sums = jnp.where(lane == 3 * k + part, value, sums)
    sent = jnp.concatenate([direction[:rows], direction[rows:], sums], axis=1).astype(bf16)
    low[...] = jnp.broadcast_to(sent[None], low.shape)


def prep_kernel(rank_cols, place, held, other, left, right, own_left, own_right, tile):
    own = own_left.shape[0]
    span = left.shape[0]
    chips = held.shape[0]
    blocks = [[unpacked(by_place(half[s]), 2 * rank_cols).reshape(span, 128) for s in range(chips)] for half in (held, other)]
    here = place[1] % 2 == 0
    by_core = [
        [jnp.where(here, near, far) for near, far in zip(blocks[core], blocks[1 - core])] for core in range(2)
    ]
    for chip in range(chips):

        @pl.when(place[1] // 2 == chip)
        def _():
            for k in range(2):
                at = slice(k * rank_cols, (k + 1) * rank_cols)
                side = [by_core[core][(s - chip) % chips][:, at] for s in range(chips) for core in range(2)]
                side = jnp.concatenate(side, axis=1).astype(bf16)
                tile[k] = side
    left[...] = tile[0]
    right[...] = tile[1].T

    @pl.when(pl.program_id(0) == place[0] // (span // own))
    def _():
        rows = pl.ds(pl.multiple_of(place[0] % (span // own) * own, own), own)
        own_left[...] = tile[0, rows]
        own_right[...] = tile[1, rows]


def spread_kernel(low, out):
    depth, _, lanes = low.shape
    lanes = lanes - 128
    sums = jnp.sum(low[:, :, lanes:].astype(f32), axis=0)
    lane = lax.broadcasted_iota(jnp.int32, sums.shape, 1)
    squares = jnp.zeros(sums.shape, f32)
    for k in range(2):
        total = jnp.sum(jnp.where(lane // 3 == k, sums, 0.0)[:1], axis=1, keepdims=True)
        for part, value in enumerate(in_three(total)):
            squares = jnp.where(lane == 3 * k + part, value, squares)
    squares = jnp.concatenate([squares] * (lanes // 128), axis=1).astype(bf16)
    for y in range(out.shape[0]):
        out[y, :depth] = low[:, :, :lanes]
        out[y, depth] = squares


def sums_kernel(low, squares):
    depth = low.shape[1] - 1
    sums = jnp.sum(low[:, depth, :, :128].astype(f32), axis=0)[:1]
    squares[...] = jnp.broadcast_to(sums[None], squares.shape)


def final_kernel(
    entries,
    span,
    squares,
    low,
    left,
    right,
    masters,
    own_left,
    own_right,
    query_master,
    out_master,
    query_copy,
    out_copy,
    query_new,
    out_new,
    near_query,
    near_out,
    near_own,
    near_master,
    near_new,
    first,
    second,
    own_arrived,
    left_for,
    own_left_for,
):
    width = left.shape[0]
    cols = first.shape[1]
    own = query_master.shape[0]
    per = span // own
    parts = width // span
    ways = (
        (own_left, near_own.at[0]),
        (own_right, near_own.at[1]),
        (query_master, near_master.at[0]),
        (out_master, near_master.at[1]),
    )
    own_copies = [pltpu.make_async_copy(x, y, own_arrived.at[k]) for k, (x, y) in enumerate(ways)]
    for copy in own_copies:
        copy.start()

    height = low.shape[0]
    rows = low.shape[2]
    group = 16 // rows
    for g in range(0, first.shape[0] // rows, group):
        part = [low[f % height, f // height].astype(f32) for f in range(g, g + group)]
        part = jnp.concatenate(part, axis=0).astype(bf16)
        first[g * rows : (g + group) * rows] = part[:, :cols]
        second[g * rows : (g + group) * rows] = part[:, cols:]
    second_turned = second[...].T

    sums = jnp.sum(squares[...], axis=0)
    lane = lax.broadcasted_iota(jnp.int32, sums.shape, 1)
    scales = []
    for k in range(2):
        total = jnp.sum(jnp.where(lane // 3 == k, sums, 0.0), axis=1, keepdims=True)
        scales.append(0.01 * lax.rsqrt(total / entries + 1e-06))

    sent = []
    for i in range(parts):
        at = pl.ds(i * span, span)
        codes = masters[i * per : (i + 1) * per]
        moved = jnp.dot(left[at], first[...], preferred_element_type=f32)
        kept = decoded(codes[:, :own].reshape(span, cols), REACH)
        near_query[at] = (kept - scales[0] * moved).astype(bf16)
        sent.append(pltpu.make_async_copy(near_query.at[at], query_copy.at[at], left_for.at[i, 0]))
        sent[-1].start()
        moved = jnp.dot(second_turned, right[:, at], preferred_element_type=f32)
        kept = decoded(codes[:, own:].reshape(span, cols).T, REACH)
        near_out[:, at] = (kept - scales[1] * moved).astype(bf16)
        sent.append(pltpu.make_async_copy(near_out.at[:, at], out_copy.at[:, at], left_for.at[i, 1]))
        sent[-1].start()
    for copy in own_copies:
        copy.wait()
    for k, (step, new) in enumerate(((first, query_new), (second, out_new))):
        moved = jnp.dot(near_own[k], step[...], preferred_element_type=f32)
        near_new[k] = near_master[k] - scales[k] * moved
        sent.append(pltpu.make_async_copy(near_new.at[k], new, own_left_for.at[k]))
        sent[-1].start()
    for copy in sent:
        copy.wait()


def far(value):
    return pltpu.with_memory_space_constraint(value, pltpu.HBM)


def body(
    saved_inputs,
    query_cotangent,
    attn_outputs,
    out_cotangent,
    left_factor,
    right_factor,
    query_master,
    out_master,
    first_moment,
    second_moment,
):
    depth = lax.axis_size("z")
    height = lax.axis_size("y")
    fs = depth * height
    tp = lax.axis_size("tp")
    own, rank_cols = left_factor.shape
    rows = first_moment.shape[1]
    cols = first_moment.shape[2]
    tokens = saved_inputs.shape[0]
    width = fs * own
    ranks = tp * rank_cols
    used = 2 * rank_cols
    kept = own * used // 128

    place = jnp.stack([lax.axis_index(FS), lax.axis_index("tp")]).astype(jnp.int32)
    packed, masters = pl.pallas_call(
        send_kernel,
        out_shape=(
            jax.ShapeDtypeStruct((depth, kept, 128), bf16),
            pltpu.HBM((2 * own, cols), bf16),
        ),
        in_specs=[pl.BlockSpec()] * 4,
        out_specs=(VMEM, VMEM),
        compiler_params=SMALL,
        cost_estimate=cost(1 << 16, 1 << 20),
    )(far(left_factor), far(right_factor), far(query_master), far(out_master.T))
    packed = pl.pallas_call(
        hold_kernel,
        out_shape=jax.ShapeDtypeStruct(packed.shape, bf16),
        in_specs=[ANY, ANY],
        out_specs=ANY,
        input_output_aliases={1: 0},
        compiler_params=SMALL,
        cost_estimate=LONG,
    )(far(masters), packed)
    masters = lax.all_gather(masters, FS)
    packed = lax.all_to_all(packed, "z", 0, 0)
    packed = pl.pallas_call(
        copies_kernel,
        out_shape=jax.ShapeDtypeStruct((height, depth, kept, 128), bf16),
        in_specs=[VMEM],
        out_specs=VMEM,
        compiler_params=SMALL,
        cost_estimate=cost(1 << 16, 1 << 20),
    )(packed)
    packed = lax.all_to_all(packed, "y", 0, 0)
    proj = pl.pallas_call(
        functools.partial(proj_kernel, used),
        out_shape=jax.ShapeDtypeStruct((used, tokens), bf16),
        in_specs=[VMEM] * 3,
        out_specs=VMEM,
        scratch_shapes=[pltpu.VMEM((width, 128), bf16)],
        compiler_params=SMALL,
        cost_estimate=cost(4 * tokens * width * 128, 8 << 20),
    )(packed, saved_inputs, out_cotangent)
    proj = lax.all_gather(proj, "tp", axis=0, tiled=True)

    partial = pl.pallas_call(
        functools.partial(grad_kernel, rank_cols),
        out_shape=pltpu.HBM((fs // 2, 4 * rows, cols), bf16),
        in_specs=[VMEM] * 3,
        out_specs=VMEM,
        compiler_params=SMALL,
        cost_estimate=cost(4 * ranks * tokens * cols, 2 << 20),
    )(proj, query_cotangent, attn_outputs)
    pieces = lax.all_to_all(partial.reshape(fs, 2 * rows, cols), FS, 0, 0)

    held = [packed]
    for step in range(1, tp // 2):
        held.append(lax.ppermute(packed, "tp", [((t + 2 * step) % tp, t) for t in range(tp)]))
    held = jnp.stack(held)
    other = lax.ppermute(held, "tp", [(t ^ 1, t) for t in range(tp)])

    first_new, second_new, low = pl.pallas_call(
        moment_kernel,
        out_shape=(
            jax.ShapeDtypeStruct(first_moment.shape, f32),
            jax.ShapeDtypeStruct(second_moment.shape, f32),
            pltpu.HBM((depth, rows, 2 * cols + 128), bf16),
        ),
        in_specs=[VMEM] * 3,
        out_specs=(VMEM, VMEM, VMEM),
        compiler_params=SMALL,
        cost_estimate=cost(1 << 20, 2 << 20),
    )(pieces, first_moment, second_moment)
    low = lax.all_to_all(low, "z", 0, 0)
    low = pl.pallas_call(
        spread_kernel,
        out_shape=pltpu.HBM((height, depth + 1, rows, 2 * cols), bf16),
        in_specs=[VMEM],
        out_specs=VMEM,
        compiler_params=SMALL,
        cost_estimate=cost(1 << 16, 1 << 20),
    )(low)
    low = lax.all_to_all(low, "y", 0, 0)

    span = width // 4
    per = span // own
    left, right, own_left, own_right = pl.pallas_call(
        functools.partial(prep_kernel, rank_cols),
        grid=(width // span,),
        out_shape=(
            pltpu.HBM((width, ranks), bf16),
            pltpu.HBM((ranks, width), bf16),
            pltpu.HBM((own, ranks), bf16),
            pltpu.HBM((own, ranks), bf16),
        ),
        in_specs=[
            SMEM,
            pl.BlockSpec((tp // 2, height, per // height, kept, 128), lambda i: (0, 0, i, 0, 0)),
            pl.BlockSpec((tp // 2, height, per // height, kept, 128), lambda i: (0, 0, i, 0, 0)),
        ],
        out_specs=(
            pl.BlockSpec((span, ranks), lambda i: (i, 0)),
            pl.BlockSpec((ranks, span), lambda i: (0, i)),
            pl.BlockSpec((own, ranks), lambda i: (0, 0)),
            pl.BlockSpec((own, ranks), lambda i: (0, 0)),
        ),
        scratch_shapes=[pltpu.VMEM((2, span, ranks), bf16)],
        compiler_params=SMALL,
        cost_estimate=cost(1 << 30, 30 << 20),
    )(place, far(held), far(other))

    low, masters = lax.optimization_barrier((low, masters))
    parts = width // span
    squares = pl.pallas_call(
        sums_kernel,
        out_shape=jax.ShapeDtypeStruct((tp, 1, 128), f32),
        in_specs=[VMEM],
        out_specs=VMEM,
        compiler_params=SMALL,
        cost_estimate=LONG,
    )(low)
    squares = lax.all_to_all(squares, "tp", 0, 0)

    query_copy, out_copy, query_new, out_new = pl.pallas_call(
        functools.partial(final_kernel, float(rows * fs * cols * tp), span),
        out_shape=(
            pltpu.HBM((width, cols), bf16),
            pltpu.HBM((cols, width), bf16),
            pltpu.HBM((own, cols), f32),
            pltpu.HBM((own, cols), f32),
        ),
        in_specs=[VMEM] * 5 + [ANY] * 4,
        out_specs=(ANY,) * 4,
        scratch_shapes=[
            pltpu.VMEM((width, cols), bf16),
            pltpu.VMEM((cols, width), bf16),
            pltpu.VMEM((2, own, ranks), bf16),
            pltpu.VMEM((2, own, cols), f32),
            pltpu.VMEM((2, own, cols), f32),
            pltpu.VMEM((ranks, cols), bf16),
            pltpu.VMEM((ranks, cols), bf16),
            pltpu.SemaphoreType.DMA((4,)),
            pltpu.SemaphoreType.DMA((parts, 2)),
            pltpu.SemaphoreType.DMA((2,)),
        ],
        compiler_params=SMALL,
        cost_estimate=cost(4 * width * ranks * cols, 20 << 20),
    )(
        squares,
        low,
        left,
        right,
        masters,
        far(own_left),
        far(own_right),
        far(query_master),
        far(out_master.T),
    )
    return (query_new, out_new.T, query_copy, out_copy, first_new, second_new)


def solution(mesh):
    finer = Mesh(mesh.devices.reshape(12, 8, 8), ("z", "y", "tp"))
    both = P(FS, "tp")
    moment = P(None, FS, "tp")

    return jax.shard_map(
        body,
        mesh=finer,
        in_specs=(P(FS, None), both, both, P(FS, None), both, both, both, P("tp", FS), moment, moment),
        out_specs=(both, P("tp", FS), P(None, "tp"), P("tp", None), moment, moment),
        check_vma=False,
    )
```

```python
import functools

import jax
import jax.numpy as jnp
from jax import lax
from jax.experimental import pallas as pl
from jax.experimental.pallas import tpu as pltpu
from jax.sharding import Mesh
from jax.sharding import PartitionSpec as P


bf16 = jnp.bfloat16
f32 = jnp.float32
FS = ("z", "y")
VMEM = pl.BlockSpec(memory_space=pltpu.VMEM)
ANY = pl.BlockSpec(memory_space=pl.ANY)
SMEM = pl.BlockSpec(memory_space=pltpu.SMEM)
REACH = 2.0**34
GRAD_REACH = 2.0**10
SMALL = pltpu.CompilerParams(vmem_limit_bytes=16 << 20)


def cost(flops, nbytes):
    return pl.CostEstimate(flops=flops, bytes_accessed=nbytes, transcendentals=0)


LONG = cost(1 << 35, 1 << 26)


def coded(value, reach):
    size = value * reach
    size = size * size
    size = size * size
    return jnp.where(value < 0.0, -size, size).astype(bf16)


def decoded(code, reach):
    wide = code.astype(f32)
    size = lax.rsqrt(lax.rsqrt(jnp.abs(wide))) * (1.0 / reach)
    return jnp.where(wide < 0.0, -size, size)


def send_kernel(left, right, query_master, out_master, out, masters):
    own = query_master.shape[0]
    masters[:own] = coded(query_master[...], REACH)
    masters[own:] = coded(out_master[...], REACH)
    both = jnp.concatenate([left[...].astype(f32), right[...].astype(f32)], axis=1)
    used = both.shape[1]
    free = 128 - used
    kept = out.shape[1]
    rest = both[kept:]
    tail = jnp.concatenate([rest[:, j : j + free] for j in range(0, used, free)], axis=0)
    packed = jnp.concatenate([both[:kept], tail], axis=1).astype(bf16)
    out[...] = jnp.broadcast_to(packed[None], out.shape)


def copies_kernel(packed, out):
    out[...] = jnp.broadcast_to(packed[...][None], out.shape)


def by_place(packed):
    height, depth = packed.shape[:2]
    return jnp.concatenate([packed[y, z][None] for z in range(depth) for y in range(height)], axis=0)


def hold_kernel(masters, packed, out):
    pass


def unpacked(packed, used):
    free = 128 - used
    parts = used // free
    height = packed.shape[1] // parts
    wide = packed.astype(f32)
    tail = [wide[:, j * height : (j + 1) * height, used:] for j in range(parts)]
    tail = jnp.concatenate(tail + [jnp.zeros_like(tail[0])], axis=2)
    return jnp.concatenate([wide, tail], axis=1)


def proj_kernel(used, packed, saved_inputs, out_cotangent, out, factors):
    depth = packed.shape[1]
    span = factors.shape[0] // depth
    for z in range(depth):
        block = unpacked(by_place(packed[:, z : z + 1]), used).reshape(span, 128)
        factors[z * span : (z + 1) * span] = block.astype(bf16)
    left = jnp.dot(saved_inputs[...], factors[...], preferred_element_type=f32)
    right = jnp.dot(out_cotangent[...], factors[...], preferred_element_type=f32)
    lane = lax.broadcasted_iota(jnp.int32, left.shape, 1)
    out[...] = jnp.where(lane < used // 2, left, right).T[:used].astype(bf16)


def grad_kernel(rank_cols, proj, query_cotangent, attn_outputs, out):
    cols = query_cotangent.shape[1]
    parts = []
    for k, other in enumerate((query_cotangent, attn_outputs)):
        starts = range(k * rank_cols, proj.shape[0], 2 * rank_cols)
        ranks = jnp.concatenate([proj[at : at + rank_cols] for at in starts], axis=0)
        parts.append(jnp.dot(ranks, other[...], preferred_element_type=f32).reshape(-1, 8, cols))
    first, second = parts
    both = jnp.concatenate([first[:, :4], second[:, :4], first[:, 4:], second[:, 4:]], axis=1)
    out[...] = coded(both, GRAD_REACH)


def in_three(total):
    parts = []
    for _ in range(3):
        parts.append(total.astype(bf16).astype(f32))
        total = total - parts[-1]
    return parts


def moment_kernel(pieces, first, second, first_new, second_new, low):
    rows = first.shape[1]
    grads = jnp.sum(decoded(pieces[...], GRAD_REACH), axis=0)
    new_first = 0.9 * jnp.concatenate([first[0], first[1]], axis=0) + 0.1 * grads
    new_second = 0.99 * jnp.concatenate([second[0], second[1]], axis=0) + 0.01 * grads * grads
    direction = new_first / (jnp.sqrt(new_second) + 1e-08)
    first_new[0] = new_first[:rows]
    first_new[1] = new_first[rows:]
    second_new[0] = new_second[:rows]
    second_new[1] = new_second[rows:]
    squares = direction * direction
    lane = lax.broadcasted_iota(jnp.int32, (rows, 128), 1)
    sums = jnp.zeros((rows, 128), f32)
    for k in range(2):
        total = jnp.sum(squares[k * rows : (k + 1) * rows], axis=(0, 1), keepdims=True)
        for part, value in enumerate(in_three(total)):
            sums = jnp.where(lane == 3 * k + part, value, sums)
    sent = jnp.concatenate([direction[:rows], direction[rows:], sums], axis=1).astype(bf16)
    low[...] = jnp.broadcast_to(sent[None], low.shape)


def prep_kernel(rank_cols, place, held, other, left, right, own_left, own_right, tile):
    own = own_left.shape[0]
    span = left.shape[0]
    chips = held.shape[0]
    blocks = [[unpacked(by_place(half[s]), 2 * rank_cols).reshape(span, 128) for s in range(chips)] for half in (held, other)]
    here = place[1] % 2 == 0
    by_core = [
        [jnp.where(here, near, far) for near, far in zip(blocks[core], blocks[1 - core])] for core in range(2)
    ]
    for chip in range(chips):

        @pl.when(place[1] // 2 == chip)
        def _():
            for k in range(2):
                at = slice(k * rank_cols, (k + 1) * rank_cols)
                side = [by_core[core][(s - chip) % chips][:, at] for s in range(chips) for core in range(2)]
                side = jnp.concatenate(side, axis=1).astype(bf16)
                tile[k] = side
    left[...] = tile[0]
    right[...] = tile[1].T

    @pl.when(pl.program_id(0) == place[0] // (span // own))
    def _():
        rows = pl.ds(pl.multiple_of(place[0] % (span // own) * own, own), own)
        own_left[...] = tile[0, rows]
        own_right[...] = tile[1, rows]


def decode_kernel(span, masters, out_all, near, near_out, arrived, left_for):
    own = near.shape[1]
    cols = near.shape[2]
    per = span // own
    parts = masters.shape[0] // per
    copies = []
    for i in range(parts):
        held = pl.ds(i * per, per)
        copies.append(pltpu.make_async_copy(masters.at[held, pl.ds(own, own)], near.at[held], arrived.at[i]))
        copies[-1].start()
    sent = []
    for i in range(parts):
        at = pl.ds(i * span, span)
        copies[i].wait()
        codes = near[i * per : (i + 1) * per].reshape(span, cols)
        near_out[:, at] = decoded(codes.T, REACH)
        sent.append(pltpu.make_async_copy(near_out.at[:, at], out_all.at[:, at], left_for.at[i]))
        sent[-1].start()
    for copy in sent:
        copy.wait()


def spread_kernel(low, out):
    depth, _, lanes = low.shape
    lanes = lanes - 128
    sums = jnp.sum(low[:, :, lanes:].astype(f32), axis=0)
    lane = lax.broadcasted_iota(jnp.int32, sums.shape, 1)
    squares = jnp.zeros(sums.shape, f32)
    for k in range(2):
        total = jnp.sum(jnp.where(lane // 3 == k, sums, 0.0)[:1], axis=1, keepdims=True)
        for part, value in enumerate(in_three(total)):
            squares = jnp.where(lane == 3 * k + part, value, squares)
    squares = jnp.concatenate([squares] * (lanes // 128), axis=1).astype(bf16)
    for y in range(out.shape[0]):
        out[y, :depth] = low[:, :, :lanes]
        out[y, depth] = squares


def sums_kernel(low, squares):
    depth = low.shape[1] - 1
    sums = jnp.sum(low[:, depth, :, :128].astype(f32), axis=0)[:1]
    squares[...] = jnp.broadcast_to(sums[None], squares.shape)


def final_kernel(
    entries,
    span,
    squares,
    low,
    left,
    right,
    masters,
    out_all,
    own_left,
    own_right,
    query_master,
    out_master,
    query_copy,
    out_copy,
    query_new,
    out_new,
    near_query,
    near_out,
    near_own,
    near_master,
    near_new,
    first,
    second,
    own_arrived,
    left_for,
    own_left_for,
):
    width = left.shape[0]
    cols = first.shape[1]
    own = query_master.shape[0]
    per = span // own
    parts = width // span
    ways = (
        (own_left, near_own.at[0]),
        (own_right, near_own.at[1]),
        (query_master, near_master.at[0]),
        (out_master, near_master.at[1]),
    )
    own_copies = [pltpu.make_async_copy(x, y, own_arrived.at[k]) for k, (x, y) in enumerate(ways)]
    for copy in own_copies:
        copy.start()

    height = low.shape[0]
    rows = low.shape[2]
    group = 16 // rows
    for g in range(0, first.shape[0] // rows, group):
        part = [low[f % height, f // height].astype(f32) for f in range(g, g + group)]
        part = jnp.concatenate(part, axis=0).astype(bf16)
        first[g * rows : (g + group) * rows] = part[:, :cols]
        second[g * rows : (g + group) * rows] = part[:, cols:]
    second_turned = second[...].T

    sums = jnp.sum(squares[...], axis=0)
    lane = lax.broadcasted_iota(jnp.int32, sums.shape, 1)
    scales = []
    for k in range(2):
        total = jnp.sum(jnp.where(lane // 3 == k, sums, 0.0), axis=1, keepdims=True)
        scales.append(0.01 * lax.rsqrt(total / entries + 1e-06))

    sent = []
    for i in range(parts):
        at = pl.ds(i * span, span)
        codes = masters[i * per : (i + 1) * per]
        moved = jnp.dot(left[at], first[...], preferred_element_type=f32)
        kept = decoded(codes[:, :own].reshape(span, cols), REACH)
        near_query[at] = (kept - scales[0] * moved).astype(bf16)
        sent.append(pltpu.make_async_copy(near_query.at[at], query_copy.at[at], left_for.at[i, 0]))
        sent[-1].start()
        moved = jnp.dot(second_turned, right[:, at], preferred_element_type=f32)
        near_out[:, at] = (out_all[:, at] - scales[1] * moved).astype(bf16)
        sent.append(pltpu.make_async_copy(near_out.at[:, at], out_copy.at[:, at], left_for.at[i, 1]))
        sent[-1].start()
    for copy in own_copies:
        copy.wait()
    for k, (step, new) in enumerate(((first, query_new), (second, out_new))):
        moved = jnp.dot(near_own[k], step[...], preferred_element_type=f32)
        near_new[k] = near_master[k] - scales[k] * moved
        sent.append(pltpu.make_async_copy(near_new.at[k], new, own_left_for.at[k]))
        sent[-1].start()
    for copy in sent:
        copy.wait()


def far(value):
    return pltpu.with_memory_space_constraint(value, pltpu.HBM)


def body(
    saved_inputs,
    query_cotangent,
    attn_outputs,
    out_cotangent,
    left_factor,
    right_factor,
    query_master,
    out_master,
    first_moment,
    second_moment,
):
    depth = lax.axis_size("z")
    height = lax.axis_size("y")
    fs = depth * height
    tp = lax.axis_size("tp")
    own, rank_cols = left_factor.shape
    rows = first_moment.shape[1]
    cols = first_moment.shape[2]
    tokens = saved_inputs.shape[0]
    width = fs * own
    ranks = tp * rank_cols
    used = 2 * rank_cols
    kept = own * used // 128

    place = jnp.stack([lax.axis_index(FS), lax.axis_index("tp")]).astype(jnp.int32)
    packed, masters = pl.pallas_call(
        send_kernel,
        out_shape=(
            jax.ShapeDtypeStruct((depth, kept, 128), bf16),
            pltpu.HBM((2 * own, cols), bf16),
        ),
        in_specs=[pl.BlockSpec()] * 4,
        out_specs=(VMEM, VMEM),
        compiler_params=SMALL,
        cost_estimate=cost(1 << 16, 1 << 20),
    )(far(left_factor), far(right_factor), far(query_master), far(out_master.T))
    packed = pl.pallas_call(
        hold_kernel,
        out_shape=jax.ShapeDtypeStruct(packed.shape, bf16),
        in_specs=[ANY, ANY],
        out_specs=ANY,
        input_output_aliases={1: 0},
        compiler_params=SMALL,
        cost_estimate=LONG,
    )(far(masters), packed)
    masters = lax.all_gather(masters, FS)
    packed = lax.all_to_all(packed, "z", 0, 0)
    packed = pl.pallas_call(
        copies_kernel,
        out_shape=jax.ShapeDtypeStruct((height, depth, kept, 128), bf16),
        in_specs=[VMEM],
        out_specs=VMEM,
        compiler_params=SMALL,
        cost_estimate=cost(1 << 16, 1 << 20),
    )(packed)
    packed = lax.all_to_all(packed, "y", 0, 0)
    proj = pl.pallas_call(
        functools.partial(proj_kernel, used),
        out_shape=jax.ShapeDtypeStruct((used, tokens), bf16),
        in_specs=[VMEM] * 3,
        out_specs=VMEM,
        scratch_shapes=[pltpu.VMEM((width, 128), bf16)],
        compiler_params=SMALL,
        cost_estimate=cost(4 * tokens * width * 128, 8 << 20),
    )(packed, saved_inputs, out_cotangent)
    proj = lax.all_gather(proj, "tp", axis=0, tiled=True)

    partial = pl.pallas_call(
        functools.partial(grad_kernel, rank_cols),
        out_shape=pltpu.HBM((fs // 2, 4 * rows, cols), bf16),
        in_specs=[VMEM] * 3,
        out_specs=VMEM,
        compiler_params=SMALL,
        cost_estimate=cost(4 * ranks * tokens * cols, 2 << 20),
    )(proj, query_cotangent, attn_outputs)
    pieces = lax.all_to_all(partial.reshape(fs, 2 * rows, cols), FS, 0, 0)

    held = [packed]
    for step in range(1, tp // 2):
        held.append(lax.ppermute(packed, "tp", [((t + 2 * step) % tp, t) for t in range(tp)]))
    held = jnp.stack(held)
    other = lax.ppermute(held, "tp", [(t ^ 1, t) for t in range(tp)])

    first_new, second_new, low = pl.pallas_call(
        moment_kernel,
        out_shape=(
            jax.ShapeDtypeStruct(first_moment.shape, f32),
            jax.ShapeDtypeStruct(second_moment.shape, f32),
            pltpu.HBM((depth, rows, 2 * cols + 128), bf16),
        ),
        in_specs=[VMEM] * 3,
        out_specs=(VMEM, VMEM, VMEM),
        compiler_params=SMALL,
        cost_estimate=cost(1 << 20, 2 << 20),
    )(pieces, first_moment, second_moment)
    low = lax.all_to_all(low, "z", 0, 0)
    low = pl.pallas_call(
        spread_kernel,
        out_shape=pltpu.HBM((height, depth + 1, rows, 2 * cols), bf16),
        in_specs=[VMEM],
        out_specs=VMEM,
        compiler_params=SMALL,
        cost_estimate=cost(1 << 16, 1 << 20),
    )(low)
    low = lax.all_to_all(low, "y", 0, 0)

    span = width // 4
    per = span // own
    left, right, own_left, own_right = pl.pallas_call(
        functools.partial(prep_kernel, rank_cols),
        grid=(width // span,),
        out_shape=(
            pltpu.HBM((width, ranks), bf16),
            pltpu.HBM((ranks, width), bf16),
            pltpu.HBM((own, ranks), bf16),
            pltpu.HBM((own, ranks), bf16),
        ),
        in_specs=[
            SMEM,
            pl.BlockSpec((tp // 2, height, per // height, kept, 128), lambda i: (0, 0, i, 0, 0)),
            pl.BlockSpec((tp // 2, height, per // height, kept, 128), lambda i: (0, 0, i, 0, 0)),
        ],
        out_specs=(
            pl.BlockSpec((span, ranks), lambda i: (i, 0)),
            pl.BlockSpec((ranks, span), lambda i: (0, i)),
            pl.BlockSpec((own, ranks), lambda i: (0, 0)),
            pl.BlockSpec((own, ranks), lambda i: (0, 0)),
        ),
        scratch_shapes=[pltpu.VMEM((2, span, ranks), bf16)],
        compiler_params=SMALL,
        cost_estimate=cost(1 << 30, 30 << 20),
    )(place, far(held), far(other))

    parts = width // span
    out_all = pl.pallas_call(
        functools.partial(decode_kernel, span),
        out_shape=pltpu.HBM((cols, width), f32),
        in_specs=[ANY],
        out_specs=ANY,
        scratch_shapes=[
            pltpu.VMEM((fs, own, cols), bf16),
            pltpu.VMEM((cols, width), f32),
            pltpu.SemaphoreType.DMA((parts,)),
            pltpu.SemaphoreType.DMA((parts,)),
        ],
        compiler_params=SMALL,
        cost_estimate=cost(1 << 28, 8 << 20),
    )(far(masters))
    squares = pl.pallas_call(
        sums_kernel,
        out_shape=jax.ShapeDtypeStruct((tp, 1, 128), f32),
        in_specs=[VMEM],
        out_specs=VMEM,
        compiler_params=SMALL,
        cost_estimate=LONG,
    )(low)
    squares = lax.all_to_all(squares, "tp", 0, 0)

    query_copy, out_copy, query_new, out_new = pl.pallas_call(
        functools.partial(final_kernel, float(rows * fs * cols * tp), span),
        out_shape=(
            pltpu.HBM((width, cols), bf16),
            pltpu.HBM((cols, width), bf16),
            pltpu.HBM((own, cols), f32),
            pltpu.HBM((own, cols), f32),
        ),
        in_specs=[VMEM] * 6 + [ANY] * 4,
        out_specs=(ANY,) * 4,
        scratch_shapes=[
            pltpu.VMEM((width, cols), bf16),
            pltpu.VMEM((cols, width), bf16),
            pltpu.VMEM((2, own, ranks), bf16),
            pltpu.VMEM((2, own, cols), f32),
            pltpu.VMEM((2, own, cols), f32),
            pltpu.VMEM((ranks, cols), bf16),
            pltpu.VMEM((ranks, cols), bf16),
            pltpu.SemaphoreType.DMA((4,)),
            pltpu.SemaphoreType.DMA((parts, 2)),
            pltpu.SemaphoreType.DMA((2,)),
        ],
        compiler_params=SMALL,
        cost_estimate=cost(4 * width * ranks * cols, 20 << 20),
    )(squares, low, left, right, masters, out_all, far(own_left), far(own_right), far(query_master), far(out_master.T))
    return (query_new, out_new.T, query_copy, out_copy, first_new, second_new)


def solution(mesh):
    finer = Mesh(mesh.devices.reshape(12, 8, 8), ("z", "y", "tp"))
    both = P(FS, "tp")
    moment = P(None, FS, "tp")

    return jax.shard_map(
        body,
        mesh=finer,
        in_specs=(P(FS, None), both, both, P(FS, None), both, both, both, P("tp", FS), moment, moment),
        out_specs=(both, P("tp", FS), P(None, "tp"), P("tp", None), moment, moment),
        check_vma=False,
    )
```

```python
import functools

import jax
import jax.numpy as jnp
from jax import lax
from jax.experimental import pallas as pl
from jax.experimental.pallas import tpu as pltpu
from jax.sharding import Mesh
from jax.sharding import PartitionSpec as P


bf16 = jnp.bfloat16
f32 = jnp.float32
FS = ("z", "y")
VMEM = pl.BlockSpec(memory_space=pltpu.VMEM)
ANY = pl.BlockSpec(memory_space=pl.ANY)
SMEM = pl.BlockSpec(memory_space=pltpu.SMEM)
REACH = 2.0**34
GRAD_REACH = 2.0**10
SMALL = pltpu.CompilerParams(vmem_limit_bytes=16 << 20)


def cost(flops, nbytes):
    return pl.CostEstimate(flops=flops, bytes_accessed=nbytes, transcendentals=0)


LONG = cost(1 << 35, 1 << 26)


def coded(value, reach):
    size = value * reach
    size = size * size
    size = size * size
    return jnp.where(value < 0.0, -size, size).astype(bf16)


def decoded(code, reach):
    wide = code.astype(f32)
    size = lax.rsqrt(lax.rsqrt(jnp.abs(wide))) * (1.0 / reach)
    return jnp.where(wide < 0.0, -size, size)


def send_kernel(left, right, query_master, out_master, out, masters):
    own = query_master.shape[0]
    masters[:own] = coded(query_master[...], REACH)
    masters[own:] = coded(out_master[...], REACH)
    both = jnp.concatenate([left[...].astype(f32), right[...].astype(f32)], axis=1)
    used = both.shape[1]
    free = 128 - used
    kept = out.shape[1]
    rest = both[kept:]
    tail = jnp.concatenate([rest[:, j : j + free] for j in range(0, used, free)], axis=0)
    packed = jnp.concatenate([both[:kept], tail], axis=1).astype(bf16)
    out[...] = jnp.broadcast_to(packed[None], out.shape)


def copies_kernel(packed, out):
    out[...] = jnp.broadcast_to(packed[...][None], out.shape)


def by_place(packed):
    height, depth = packed.shape[:2]
    return jnp.concatenate([packed[y, z][None] for z in range(depth) for y in range(height)], axis=0)


def hold_kernel(masters, packed, out):
    pass


def unpacked(packed, used):
    free = 128 - used
    parts = used // free
    height = packed.shape[1] // parts
    wide = packed.astype(f32)
    tail = [wide[:, j * height : (j + 1) * height, used:] for j in range(parts)]
    tail = jnp.concatenate(tail + [jnp.zeros_like(tail[0])], axis=2)
    return jnp.concatenate([wide, tail], axis=1)


def proj_kernel(used, packed, saved_inputs, out_cotangent, out, factors):
    depth = packed.shape[1]
    span = factors.shape[0] // depth
    for z in range(depth):
        block = unpacked(by_place(packed[:, z : z + 1]), used).reshape(span, 128)
        factors[z * span : (z + 1) * span] = block.astype(bf16)
    left = jnp.dot(saved_inputs[...], factors[...], preferred_element_type=f32)
    right = jnp.dot(out_cotangent[...], factors[...], preferred_element_type=f32)
    lane = lax.broadcasted_iota(jnp.int32, left.shape, 1)
    out[...] = jnp.where(lane < used // 2, left, right).T[:used].astype(bf16)


def grad_kernel(rank_cols, proj, query_cotangent, attn_outputs, out):
    cols = query_cotangent.shape[1]
    parts = []
    for k, other in enumerate((query_cotangent, attn_outputs)):
        starts = range(k * rank_cols, proj.shape[0], 2 * rank_cols)
        ranks = jnp.concatenate([proj[at : at + rank_cols] for at in starts], axis=0)
        share = jnp.dot(ranks, other[...], preferred_element_type=f32)
        parts.append(coded(share, GRAD_REACH).astype(f32).reshape(-1, 8, cols))
    first, second = parts
    both = jnp.concatenate([first[:, :4], second[:, :4], first[:, 4:], second[:, 4:]], axis=1)
    out[...] = both.astype(bf16)


def in_three(total):
    parts = []
    for _ in range(3):
        parts.append(total.astype(bf16).astype(f32))
        total = total - parts[-1]
    return parts


def moment_kernel(pieces, first, second, first_new, second_new, low):
    rows = first.shape[1]
    grads = 0.0
    for i in range(pieces.shape[0]):
        grads = grads + decoded(pieces[i], GRAD_REACH)
    new_first = 0.9 * jnp.concatenate([first[0], first[1]], axis=0) + 0.1 * grads
    new_second = 0.99 * jnp.concatenate([second[0], second[1]], axis=0) + 0.01 * grads * grads
    direction = new_first / (jnp.sqrt(new_second) + 1e-08)
    first_new[0] = new_first[:rows]
    first_new[1] = new_first[rows:]
    second_new[0] = new_second[:rows]
    second_new[1] = new_second[rows:]
    squares = direction * direction
    lane = lax.broadcasted_iota(jnp.int32, (rows, 128), 1)
    sums = jnp.zeros((rows, 128), f32)
    for k in range(2):
        total = jnp.sum(squares[k * rows : (k + 1) * rows], axis=(0, 1), keepdims=True)
        for part, value in enumerate(in_three(total)):
            sums = jnp.where(lane == 3 * k + part, value, sums)
    sent = jnp.concatenate([direction[:rows], direction[rows:], sums], axis=1).astype(bf16)
    low[...] = jnp.broadcast_to(sent[None], low.shape)


def prep_kernel(rank_cols, place, held, other, left, right, own_left, own_right, tile):
    own = own_left.shape[0]
    span = left.shape[0]
    chips = held.shape[0]
    blocks = [[unpacked(by_place(half[s]), 2 * rank_cols).reshape(span, 128) for s in range(chips)] for half in (held, other)]
    here = place[1] % 2 == 0
    by_core = [
        [jnp.where(here, near, far) for near, far in zip(blocks[core], blocks[1 - core])] for core in range(2)
    ]
    for chip in range(chips):

        @pl.when(place[1] // 2 == chip)
        def _():
            for k in range(2):
                at = slice(k * rank_cols, (k + 1) * rank_cols)
                side = [by_core[core][(s - chip) % chips][:, at] for s in range(chips) for core in range(2)]
                side = jnp.concatenate(side, axis=1).astype(bf16)
                tile[k] = side
    left[...] = tile[0]
    right[...] = tile[1].T

    @pl.when(pl.program_id(0) == place[0] // (span // own))
    def _():
        rows = pl.ds(pl.multiple_of(place[0] % (span // own) * own, own), own)
        own_left[...] = tile[0, rows]
        own_right[...] = tile[1, rows]


def spread_kernel(low, out):
    depth, _, lanes = low.shape
    lanes = lanes - 128
    sums = jnp.sum(low[:, :, lanes:].astype(f32), axis=0)
    lane = lax.broadcasted_iota(jnp.int32, sums.shape, 1)
    squares = jnp.zeros(sums.shape, f32)
    for k in range(2):
        total = jnp.sum(jnp.where(lane // 3 == k, sums, 0.0)[:1], axis=1, keepdims=True)
        for part, value in enumerate(in_three(total)):
            squares = jnp.where(lane == 3 * k + part, value, squares)
    squares = jnp.concatenate([squares] * (lanes // 128), axis=1).astype(bf16)
    for y in range(out.shape[0]):
        out[y, :depth] = low[:, :, :lanes]
        out[y, depth] = squares


def sums_kernel(low, squares):
    depth = low.shape[1] - 1
    sums = jnp.sum(low[:, depth, :, :128].astype(f32), axis=0)[:1]
    squares[...] = jnp.broadcast_to(sums[None], squares.shape)


def final_kernel(
    entries,
    span,
    squares,
    low,
    left,
    right,
    masters,
    own_left,
    own_right,
    query_master,
    out_master,
    query_copy,
    out_copy,
    query_new,
    out_new,
    near_query,
    near_out,
    near_own,
    near_master,
    near_new,
    first,
    second,
    own_arrived,
    left_for,
    own_left_for,
):
    width = left.shape[0]
    cols = first.shape[1]
    own = query_master.shape[0]
    per = span // own
    parts = width // span
    ways = (
        (own_left, near_own.at[0]),
        (own_right, near_own.at[1]),
        (query_master, near_master.at[0]),
        (out_master, near_master.at[1]),
    )
    own_copies = [pltpu.make_async_copy(x, y, own_arrived.at[k]) for k, (x, y) in enumerate(ways)]
    for copy in own_copies:
        copy.start()

    height = low.shape[0]
    rows = low.shape[2]
    group = 16 // rows
    for g in range(0, first.shape[0] // rows, group):
        part = [low[f % height, f // height].astype(f32) for f in range(g, g + group)]
        part = jnp.concatenate(part, axis=0).astype(bf16)
        first[g * rows : (g + group) * rows] = part[:, :cols]
        second[g * rows : (g + group) * rows] = part[:, cols:]
    second_turned = second[...].T

    sums = jnp.sum(squares[...], axis=0)
    lane = lax.broadcasted_iota(jnp.int32, sums.shape, 1)
    scales = []
    for k in range(2):
        total = jnp.sum(jnp.where(lane // 3 == k, sums, 0.0), axis=1, keepdims=True)
        scales.append(0.01 * lax.rsqrt(total / entries + 1e-06))

    sent = []
    for i in range(parts):
        at = pl.ds(i * span, span)
        codes = masters[i * per : (i + 1) * per]
        moved = jnp.dot(left[at], first[...], preferred_element_type=f32)
        kept = decoded(codes[:, :own].reshape(span, cols), REACH)
        near_query[at] = (kept - scales[0] * moved).astype(bf16)
        sent.append(pltpu.make_async_copy(near_query.at[at], query_copy.at[at], left_for.at[i, 0]))
        sent[-1].start()
        moved = jnp.dot(second_turned, right[:, at], preferred_element_type=f32)
        kept = decoded(codes[:, own:].reshape(span, cols).T, REACH)
        near_out[:, at] = (kept - scales[1] * moved).astype(bf16)
        sent.append(pltpu.make_async_copy(near_out.at[:, at], out_copy.at[:, at], left_for.at[i, 1]))
        sent[-1].start()
    for copy in own_copies:
        copy.wait()
    for k, (step, new) in enumerate(((first, query_new), (second, out_new))):
        moved = jnp.dot(near_own[k], step[...], preferred_element_type=f32)
        near_new[k] = near_master[k] - scales[k] * moved
        sent.append(pltpu.make_async_copy(near_new.at[k], new, own_left_for.at[k]))
        sent[-1].start()
    for copy in sent:
        copy.wait()


def far(value):
    return pltpu.with_memory_space_constraint(value, pltpu.HBM)


def body(
    saved_inputs,
    query_cotangent,
    attn_outputs,
    out_cotangent,
    left_factor,
    right_factor,
    query_master,
    out_master,
    first_moment,
    second_moment,
):
    depth = lax.axis_size("z")
    height = lax.axis_size("y")
    fs = depth * height
    tp = lax.axis_size("tp")
    own, rank_cols = left_factor.shape
    rows = first_moment.shape[1]
    cols = first_moment.shape[2]
    tokens = saved_inputs.shape[0]
    width = fs * own
    ranks = tp * rank_cols
    used = 2 * rank_cols
    kept = own * used // 128

    place = jnp.stack([lax.axis_index(FS), lax.axis_index("tp")]).astype(jnp.int32)
    packed, masters = pl.pallas_call(
        send_kernel,
        out_shape=(
            jax.ShapeDtypeStruct((depth, kept, 128), bf16),
            pltpu.HBM((2 * own, cols), bf16),
        ),
        in_specs=[pl.BlockSpec()] * 4,
        out_specs=(VMEM, VMEM),
        compiler_params=SMALL,
        cost_estimate=cost(1 << 16, 1 << 20),
    )(far(left_factor), far(right_factor), far(query_master), far(out_master.T))
    packed = pl.pallas_call(
        hold_kernel,
        out_shape=jax.ShapeDtypeStruct(packed.shape, bf16),
        in_specs=[ANY, ANY],
        out_specs=ANY,
        input_output_aliases={1: 0},
        compiler_params=SMALL,
        cost_estimate=LONG,
    )(far(masters), packed)
    masters = lax.all_gather(masters, FS)
    packed = lax.all_to_all(packed, "z", 0, 0)
    packed = pl.pallas_call(
        copies_kernel,
        out_shape=jax.ShapeDtypeStruct((height, depth, kept, 128), bf16),
        in_specs=[VMEM],
        out_specs=VMEM,
        compiler_params=SMALL,
        cost_estimate=cost(1 << 16, 1 << 20),
    )(packed)
    packed = lax.all_to_all(packed, "y", 0, 0)
    proj = pl.pallas_call(
        functools.partial(proj_kernel, used),
        out_shape=jax.ShapeDtypeStruct((used, tokens), bf16),
        in_specs=[VMEM] * 3,
        out_specs=VMEM,
        scratch_shapes=[pltpu.VMEM((width, 128), bf16)],
        compiler_params=SMALL,
        cost_estimate=cost(4 * tokens * width * 128, 8 << 20),
    )(packed, saved_inputs, out_cotangent)
    proj = lax.all_gather(proj, "tp", axis=0, tiled=True)

    partial = pl.pallas_call(
        functools.partial(grad_kernel, rank_cols),
        out_shape=pltpu.HBM((fs // 2, 4 * rows, cols), bf16),
        in_specs=[VMEM] * 3,
        out_specs=VMEM,
        compiler_params=SMALL,
        cost_estimate=cost(4 * ranks * tokens * cols, 2 << 20),
    )(proj, query_cotangent, attn_outputs)
    pieces = lax.all_to_all(partial.reshape(fs, 2 * rows, cols), FS, 0, 0)

    held = [packed]
    for step in range(1, tp // 2):
        held.append(lax.ppermute(packed, "tp", [((t + 2 * step) % tp, t) for t in range(tp)]))
    held = jnp.stack(held)
    other = lax.ppermute(held, "tp", [(t ^ 1, t) for t in range(tp)])

    first_new, second_new, low = pl.pallas_call(
        moment_kernel,
        out_shape=(
            jax.ShapeDtypeStruct(first_moment.shape, f32),
            jax.ShapeDtypeStruct(second_moment.shape, f32),
            pltpu.HBM((depth, rows, 2 * cols + 128), bf16),
        ),
        in_specs=[VMEM] * 3,
        out_specs=(VMEM, VMEM, VMEM),
        compiler_params=SMALL,
        cost_estimate=cost(1 << 20, 2 << 20),
    )(pieces, first_moment, second_moment)
    low = lax.all_to_all(low, "z", 0, 0)
    low = pl.pallas_call(
        spread_kernel,
        out_shape=pltpu.HBM((height, depth + 1, rows, 2 * cols), bf16),
        in_specs=[VMEM],
        out_specs=VMEM,
        compiler_params=SMALL,
        cost_estimate=cost(1 << 16, 1 << 20),
    )(low)
    low = lax.all_to_all(low, "y", 0, 0)

    span = width // 4
    per = span // own
    left, right, own_left, own_right = pl.pallas_call(
        functools.partial(prep_kernel, rank_cols),
        grid=(width // span,),
        out_shape=(
            pltpu.HBM((width, ranks), bf16),
            pltpu.HBM((ranks, width), bf16),
            pltpu.HBM((own, ranks), bf16),
            pltpu.HBM((own, ranks), bf16),
        ),
        in_specs=[
            SMEM,
            pl.BlockSpec((tp // 2, height, per // height, kept, 128), lambda i: (0, 0, i, 0, 0)),
            pl.BlockSpec((tp // 2, height, per // height, kept, 128), lambda i: (0, 0, i, 0, 0)),
        ],
        out_specs=(
            pl.BlockSpec((span, ranks), lambda i: (i, 0)),
            pl.BlockSpec((ranks, span), lambda i: (0, i)),
            pl.BlockSpec((own, ranks), lambda i: (0, 0)),
            pl.BlockSpec((own, ranks), lambda i: (0, 0)),
        ),
        scratch_shapes=[pltpu.VMEM((2, span, ranks), bf16)],
        compiler_params=SMALL,
        cost_estimate=cost(1 << 30, 30 << 20),
    )(place, far(held), far(other))

    low, masters = lax.optimization_barrier((low, masters))
    parts = width // span
    squares = pl.pallas_call(
        sums_kernel,
        out_shape=jax.ShapeDtypeStruct((tp, 1, 128), f32),
        in_specs=[VMEM],
        out_specs=VMEM,
        compiler_params=SMALL,
        cost_estimate=LONG,
    )(low)
    squares = lax.all_to_all(squares, "tp", 0, 0)

    query_copy, out_copy, query_new, out_new = pl.pallas_call(
        functools.partial(final_kernel, float(rows * fs * cols * tp), span),
        out_shape=(
            pltpu.HBM((width, cols), bf16),
            pltpu.HBM((cols, width), bf16),
            pltpu.HBM((own, cols), f32),
            pltpu.HBM((own, cols), f32),
        ),
        in_specs=[VMEM] * 5 + [ANY] * 4,
        out_specs=(ANY,) * 4,
        scratch_shapes=[
            pltpu.VMEM((width, cols), bf16),
            pltpu.VMEM((cols, width), bf16),
            pltpu.VMEM((2, own, ranks), bf16),
            pltpu.VMEM((2, own, cols), f32),
            pltpu.VMEM((2, own, cols), f32),
            pltpu.VMEM((ranks, cols), bf16),
            pltpu.VMEM((ranks, cols), bf16),
            pltpu.SemaphoreType.DMA((4,)),
            pltpu.SemaphoreType.DMA((parts, 2)),
            pltpu.SemaphoreType.DMA((2,)),
        ],
        compiler_params=SMALL,
        cost_estimate=cost(4 * width * ranks * cols, 20 << 20),
    )(
        squares,
        low,
        left,
        right,
        masters,
        far(own_left),
        far(own_right),
        far(query_master),
        far(out_master.T),
    )
    return (query_new, out_new.T, query_copy, out_copy, first_new, second_new)


def solution(mesh):
    finer = Mesh(mesh.devices.reshape(12, 8, 8), ("z", "y", "tp"))
    both = P(FS, "tp")
    moment = P(None, FS, "tp")

    return jax.shard_map(
        body,
        mesh=finer,
        in_specs=(P(FS, None), both, both, P(FS, None), both, both, both, P("tp", FS), moment, moment),
        out_specs=(both, P("tp", FS), P(None, "tp"), P("tp", None), moment, moment),
        check_vma=False,
    )
```

```python
import functools

import jax
import jax.numpy as jnp
from jax import lax
from jax.experimental import pallas as pl
from jax.experimental.pallas import tpu as pltpu
from jax.sharding import Mesh
from jax.sharding import PartitionSpec as P


bf16 = jnp.bfloat16
f32 = jnp.float32
FS = ("z", "y")
VMEM = pl.BlockSpec(memory_space=pltpu.VMEM)
ANY = pl.BlockSpec(memory_space=pl.ANY)
SMEM = pl.BlockSpec(memory_space=pltpu.SMEM)
ORDER = tuple(7 * a % 12 * 8 + 3 * b % 8 for a in range(12) for b in range(8))
REACH = 2.0**34
GRAD_REACH = 2.0**10
SMALL = pltpu.CompilerParams(vmem_limit_bytes=16 << 20)


def cost(flops, nbytes):
    return pl.CostEstimate(flops=flops, bytes_accessed=nbytes, transcendentals=0)


LONG = cost(1 << 35, 1 << 26)


def coded(value, reach):
    size = value * reach
    size = size * size
    size = size * size
    return jnp.where(value < 0.0, -size, size).astype(bf16)


def decoded(code, reach):
    wide = code.astype(f32)
    size = lax.rsqrt(lax.rsqrt(jnp.abs(wide))) * (1.0 / reach)
    return jnp.where(wide < 0.0, -size, size)


def send_kernel(left, right, query_master, out_master, out, masters):
    own = query_master.shape[0]
    masters[:own] = coded(query_master[...], REACH)
    masters[own:] = coded(out_master[...], REACH)
    both = jnp.concatenate([left[...].astype(f32), right[...].astype(f32)], axis=1)
    used = both.shape[1]
    free = 128 - used
    kept = out.shape[1]
    rest = both[kept:]
    tail = jnp.concatenate([rest[:, j : j + free] for j in range(0, used, free)], axis=0)
    packed = jnp.concatenate([both[:kept], tail], axis=1).astype(bf16)
    out[...] = jnp.broadcast_to(packed[None], out.shape)


def copies_kernel(packed, out):
    out[...] = jnp.broadcast_to(packed[...][None], out.shape)


def by_place(packed):
    height, depth = packed.shape[:2]
    return jnp.concatenate([packed[y, z][None] for z in range(depth) for y in range(height)], axis=0)


def hold_kernel(masters, packed, out):
    pass


def unpacked(packed, used):
    free = 128 - used
    parts = used // free
    height = packed.shape[1] // parts
    wide = packed.astype(f32)
    tail = [wide[:, j * height : (j + 1) * height, used:] for j in range(parts)]
    tail = jnp.concatenate(tail + [jnp.zeros_like(tail[0])], axis=2)
    return jnp.concatenate([wide, tail], axis=1)


def proj_kernel(used, packed, saved_inputs, out_cotangent, out, factors):
    depth = packed.shape[1]
    span = factors.shape[0] // depth
    for z in range(depth):
        block = unpacked(by_place(packed[:, z : z + 1]), used).reshape(span, 128)
        factors[z * span : (z + 1) * span] = block.astype(bf16)
    left = jnp.dot(saved_inputs[...], factors[...], preferred_element_type=f32)
    right = jnp.dot(out_cotangent[...], factors[...], preferred_element_type=f32)
    lane = lax.broadcasted_iota(jnp.int32, left.shape, 1)
    out[...] = jnp.where(lane < used // 2, left, right).T[:used].astype(bf16)


def grad_kernel(rank_cols, proj, query_cotangent, attn_outputs, out):
    cols = query_cotangent.shape[1]
    parts = []
    for k, other in enumerate((query_cotangent, attn_outputs)):
        starts = range(k * rank_cols, proj.shape[0], 2 * rank_cols)
        ranks = jnp.concatenate([proj[at : at + rank_cols] for at in starts], axis=0)
        share = jnp.dot(ranks, other[...], preferred_element_type=f32)
        parts.append(coded(share, GRAD_REACH).astype(f32).reshape(-1, 8, cols))
    first, second = parts
    both = jnp.concatenate([first[:, :4], second[:, :4], first[:, 4:], second[:, 4:]], axis=1)
    both = both.astype(bf16)
    for j, f in enumerate(ORDER):
        out[j] = both[f // 2, f % 2 * 8 : f % 2 * 8 + 8]


def in_three(total):
    parts = []
    for _ in range(3):
        parts.append(total.astype(bf16).astype(f32))
        total = total - parts[-1]
    return parts


def moment_kernel(pieces, first, second, first_new, second_new, low):
    rows = first.shape[1]
    grads = 0.0
    for i in range(pieces.shape[0]):
        grads = grads + decoded(pieces[i], GRAD_REACH)
    new_first = 0.9 * jnp.concatenate([first[0], first[1]], axis=0) + 0.1 * grads
    new_second = 0.99 * jnp.concatenate([second[0], second[1]], axis=0) + 0.01 * grads * grads
    direction = new_first / (jnp.sqrt(new_second) + 1e-08)
    first_new[0] = new_first[:rows]
    first_new[1] = new_first[rows:]
    second_new[0] = new_second[:rows]
    second_new[1] = new_second[rows:]
    squares = direction * direction
    lane = lax.broadcasted_iota(jnp.int32, (rows, 128), 1)
    sums = jnp.zeros((rows, 128), f32)
    for k in range(2):
        total = jnp.sum(squares[k * rows : (k + 1) * rows], axis=(0, 1), keepdims=True)
        for part, value in enumerate(in_three(total)):
            sums = jnp.where(lane == 3 * k + part, value, sums)
    sent = jnp.concatenate([direction[:rows], direction[rows:], sums], axis=1).astype(bf16)
    low[...] = jnp.broadcast_to(sent[None], low.shape)


def prep_kernel(rank_cols, place, held, other, left, right, own_left, own_right, tile):
    own = own_left.shape[0]
    span = left.shape[0]
    chips = held.shape[0]
    blocks = [[unpacked(by_place(half[s]), 2 * rank_cols).reshape(span, 128) for s in range(chips)] for half in (held, other)]
    here = place[1] % 2 == 0
    by_core = [
        [jnp.where(here, near, far) for near, far in zip(blocks[core], blocks[1 - core])] for core in range(2)
    ]
    for chip in range(chips):

        @pl.when(place[1] // 2 == chip)
        def _():
            for k in range(2):
                at = slice(k * rank_cols, (k + 1) * rank_cols)
                side = [by_core[core][(s - chip) % chips][:, at] for s in range(chips) for core in range(2)]
                side = jnp.concatenate(side, axis=1).astype(bf16)
                tile[k] = side
    left[...] = tile[0]
    right[...] = tile[1].T

    @pl.when(pl.program_id(0) == place[0] // (span // own))
    def _():
        rows = pl.ds(pl.multiple_of(place[0] % (span // own) * own, own), own)
        own_left[...] = tile[0, rows]
        own_right[...] = tile[1, rows]


def spread_kernel(low, out):
    depth, _, lanes = low.shape
    lanes = lanes - 128
    sums = jnp.sum(low[:, :, lanes:].astype(f32), axis=0)
    lane = lax.broadcasted_iota(jnp.int32, sums.shape, 1)
    squares = jnp.zeros(sums.shape, f32)
    for k in range(2):
        total = jnp.sum(jnp.where(lane // 3 == k, sums, 0.0)[:1], axis=1, keepdims=True)
        for part, value in enumerate(in_three(total)):
            squares = jnp.where(lane == 3 * k + part, value, squares)
    squares = jnp.concatenate([squares] * (lanes // 128), axis=1).astype(bf16)
    for y in range(out.shape[0]):
        out[y, :depth] = low[:, :, :lanes]
        out[y, depth] = squares


def sums_kernel(low, squares):
    depth = low.shape[1] - 1
    sums = jnp.sum(low[:, depth, :, :128].astype(f32), axis=0)[:1]
    squares[...] = jnp.broadcast_to(sums[None], squares.shape)


def final_kernel(
    entries,
    span,
    squares,
    low,
    left,
    right,
    masters,
    own_left,
    own_right,
    query_master,
    out_master,
    query_copy,
    out_copy,
    query_new,
    out_new,
    near_query,
    near_out,
    near_own,
    near_master,
    near_new,
    first,
    second,
    own_arrived,
    left_for,
    own_left_for,
):
    width = left.shape[0]
    cols = first.shape[1]
    own = query_master.shape[0]
    per = span // own
    parts = width // span
    ways = (
        (own_left, near_own.at[0]),
        (own_right, near_own.at[1]),
        (query_master, near_master.at[0]),
        (out_master, near_master.at[1]),
    )
    own_copies = [pltpu.make_async_copy(x, y, own_arrived.at[k]) for k, (x, y) in enumerate(ways)]
    for copy in own_copies:
        copy.start()

    height = low.shape[0]
    rows = low.shape[2]
    group = 16 // rows
    for g in range(0, first.shape[0] // rows, group):
        part = [low[f % height, f // height].astype(f32) for f in range(g, g + group)]
        part = jnp.concatenate(part, axis=0).astype(bf16)
        first[g * rows : (g + group) * rows] = part[:, :cols]
        second[g * rows : (g + group) * rows] = part[:, cols:]
    second_turned = second[...].T

    sums = jnp.sum(squares[...], axis=0)
    lane = lax.broadcasted_iota(jnp.int32, sums.shape, 1)
    scales = []
    for k in range(2):
        total = jnp.sum(jnp.where(lane // 3 == k, sums, 0.0), axis=1, keepdims=True)
        scales.append(0.01 * lax.rsqrt(total / entries + 1e-06))

    sent = []
    for i in range(parts):
        at = pl.ds(i * span, span)
        codes = masters[i * per : (i + 1) * per]
        moved = jnp.dot(left[at], first[...], preferred_element_type=f32)
        kept = decoded(codes[:, :own].reshape(span, cols), REACH)
        near_query[at] = (kept - scales[0] * moved).astype(bf16)
        sent.append(pltpu.make_async_copy(near_query.at[at], query_copy.at[at], left_for.at[i, 0]))
        sent[-1].start()
        moved = jnp.dot(second_turned, right[:, at], preferred_element_type=f32)
        kept = decoded(codes[:, own:].reshape(span, cols).T, REACH)
        near_out[:, at] = (kept - scales[1] * moved).astype(bf16)
        sent.append(pltpu.make_async_copy(near_out.at[:, at], out_copy.at[:, at], left_for.at[i, 1]))
        sent[-1].start()
    for copy in own_copies:
        copy.wait()
    for k, (step, new) in enumerate(((first, query_new), (second, out_new))):
        moved = jnp.dot(near_own[k], step[...], preferred_element_type=f32)
        near_new[k] = near_master[k] - scales[k] * moved
        sent.append(pltpu.make_async_copy(near_new.at[k], new, own_left_for.at[k]))
        sent[-1].start()
    for copy in sent:
        copy.wait()


def far(value):
    return pltpu.with_memory_space_constraint(value, pltpu.HBM)


def body(
    saved_inputs,
    query_cotangent,
    attn_outputs,
    out_cotangent,
    left_factor,
    right_factor,
    query_master,
    out_master,
    first_moment,
    second_moment,
):
    depth = lax.axis_size("z")
    height = lax.axis_size("y")
    fs = depth * height
    tp = lax.axis_size("tp")
    own, rank_cols = left_factor.shape
    rows = first_moment.shape[1]
    cols = first_moment.shape[2]
    tokens = saved_inputs.shape[0]
    width = fs * own
    ranks = tp * rank_cols
    used = 2 * rank_cols
    kept = own * used // 128

    place = jnp.stack([lax.axis_index(FS), lax.axis_index("tp")]).astype(jnp.int32)
    packed, masters = pl.pallas_call(
        send_kernel,
        out_shape=(
            jax.ShapeDtypeStruct((depth, kept, 128), bf16),
            pltpu.HBM((2 * own, cols), bf16),
        ),
        in_specs=[pl.BlockSpec()] * 4,
        out_specs=(VMEM, VMEM),
        compiler_params=SMALL,
        cost_estimate=cost(1 << 16, 1 << 20),
    )(far(left_factor), far(right_factor), far(query_master), far(out_master.T))
    packed = pl.pallas_call(
        hold_kernel,
        out_shape=jax.ShapeDtypeStruct(packed.shape, bf16),
        in_specs=[ANY, ANY],
        out_specs=ANY,
        input_output_aliases={1: 0},
        compiler_params=SMALL,
        cost_estimate=LONG,
    )(far(masters), packed)
    masters = lax.all_gather(masters, FS)
    packed = lax.all_to_all(packed, "z", 0, 0)
    packed = pl.pallas_call(
        copies_kernel,
        out_shape=jax.ShapeDtypeStruct((height, depth, kept, 128), bf16),
        in_specs=[VMEM],
        out_specs=VMEM,
        compiler_params=SMALL,
        cost_estimate=cost(1 << 16, 1 << 20),
    )(packed)
    packed = lax.all_to_all(packed, "y", 0, 0)
    proj = pl.pallas_call(
        functools.partial(proj_kernel, used),
        out_shape=jax.ShapeDtypeStruct((used, tokens), bf16),
        in_specs=[VMEM] * 3,
        out_specs=VMEM,
        scratch_shapes=[pltpu.VMEM((width, 128), bf16)],
        compiler_params=SMALL,
        cost_estimate=cost(4 * tokens * width * 128, 8 << 20),
    )(packed, saved_inputs, out_cotangent)
    proj = lax.all_gather(proj, "tp", axis=0, tiled=True)

    partial = pl.pallas_call(
        functools.partial(grad_kernel, rank_cols),
        out_shape=pltpu.HBM((fs, 2 * rows, cols), bf16),
        in_specs=[VMEM] * 3,
        out_specs=VMEM,
        compiler_params=SMALL,
        cost_estimate=cost(4 * ranks * tokens * cols, 2 << 20),
    )(proj, query_cotangent, attn_outputs)
    pieces = lax.all_to_all(partial, FS, 0, 0, axis_index_groups=[list(ORDER)])

    held = [packed]
    for step in range(1, tp // 2):
        held.append(lax.ppermute(packed, "tp", [((t + 2 * step) % tp, t) for t in range(tp)]))
    held = jnp.stack(held)
    other = lax.ppermute(held, "tp", [(t ^ 1, t) for t in range(tp)])

    first_new, second_new, low = pl.pallas_call(
        moment_kernel,
        out_shape=(
            jax.ShapeDtypeStruct(first_moment.shape, f32),
            jax.ShapeDtypeStruct(second_moment.shape, f32),
            pltpu.HBM((depth, rows, 2 * cols + 128), bf16),
        ),
        in_specs=[VMEM] * 3,
        out_specs=(VMEM, VMEM, VMEM),
        compiler_params=SMALL,
        cost_estimate=cost(1 << 20, 2 << 20),
    )(pieces, first_moment, second_moment)
    low = lax.all_to_all(low, "z", 0, 0)
    low = pl.pallas_call(
        spread_kernel,
        out_shape=pltpu.HBM((height, depth + 1, rows, 2 * cols), bf16),
        in_specs=[VMEM],
        out_specs=VMEM,
        compiler_params=SMALL,
        cost_estimate=cost(1 << 16, 1 << 20),
    )(low)
    low = lax.all_to_all(low, "y", 0, 0)

    span = width // 4
    per = span // own
    left, right, own_left, own_right = pl.pallas_call(
        functools.partial(prep_kernel, rank_cols),
        grid=(width // span,),
        out_shape=(
            pltpu.HBM((width, ranks), bf16),
            pltpu.HBM((ranks, width), bf16),
            pltpu.HBM((own, ranks), bf16),
            pltpu.HBM((own, ranks), bf16),
        ),
        in_specs=[
            SMEM,
            pl.BlockSpec((tp // 2, height, per // height, kept, 128), lambda i: (0, 0, i, 0, 0)),
            pl.BlockSpec((tp // 2, height, per // height, kept, 128), lambda i: (0, 0, i, 0, 0)),
        ],
        out_specs=(
            pl.BlockSpec((span, ranks), lambda i: (i, 0)),
            pl.BlockSpec((ranks, span), lambda i: (0, i)),
            pl.BlockSpec((own, ranks), lambda i: (0, 0)),
            pl.BlockSpec((own, ranks), lambda i: (0, 0)),
        ),
        scratch_shapes=[pltpu.VMEM((2, span, ranks), bf16)],
        compiler_params=SMALL,
        cost_estimate=cost(1 << 30, 30 << 20),
    )(place, far(held), far(other))

    low, masters = lax.optimization_barrier((low, masters))
    parts = width // span
    squares = pl.pallas_call(
        sums_kernel,
        out_shape=jax.ShapeDtypeStruct((tp, 1, 128), f32),
        in_specs=[VMEM],
        out_specs=VMEM,
        compiler_params=SMALL,
        cost_estimate=LONG,
    )(low)
    squares = lax.all_to_all(squares, "tp", 0, 0)

    query_copy, out_copy, query_new, out_new = pl.pallas_call(
        functools.partial(final_kernel, float(rows * fs * cols * tp), span),
        out_shape=(
            pltpu.HBM((width, cols), bf16),
            pltpu.HBM((cols, width), bf16),
            pltpu.HBM((own, cols), f32),
            pltpu.HBM((own, cols), f32),
        ),
        in_specs=[VMEM] * 5 + [ANY] * 4,
        out_specs=(ANY,) * 4,
        scratch_shapes=[
            pltpu.VMEM((width, cols), bf16),
            pltpu.VMEM((cols, width), bf16),
            pltpu.VMEM((2, own, ranks), bf16),
            pltpu.VMEM((2, own, cols), f32),
            pltpu.VMEM((2, own, cols), f32),
            pltpu.VMEM((ranks, cols), bf16),
            pltpu.VMEM((ranks, cols), bf16),
            pltpu.SemaphoreType.DMA((4,)),
            pltpu.SemaphoreType.DMA((parts, 2)),
            pltpu.SemaphoreType.DMA((2,)),
        ],
        compiler_params=SMALL,
        cost_estimate=cost(4 * width * ranks * cols, 20 << 20),
    )(
        squares,
        low,
        left,
        right,
        masters,
        far(own_left),
        far(own_right),
        far(query_master),
        far(out_master.T),
    )
    return (query_new, out_new.T, query_copy, out_copy, first_new, second_new)


def solution(mesh):
    finer = Mesh(mesh.devices.reshape(12, 8, 8), ("z", "y", "tp"))
    both = P(FS, "tp")
    moment = P(None, FS, "tp")

    return jax.shard_map(
        body,
        mesh=finer,
        in_specs=(P(FS, None), both, both, P(FS, None), both, both, both, P("tp", FS), moment, moment),
        out_specs=(both, P("tp", FS), P(None, "tp"), P("tp", None), moment, moment),
        check_vma=False,
    )
```

```python
import functools

import jax
import jax.numpy as jnp
from jax import lax
from jax.experimental import pallas as pl
from jax.experimental.pallas import tpu as pltpu
from jax.sharding import Mesh
from jax.sharding import PartitionSpec as P


bf16 = jnp.bfloat16
f32 = jnp.float32
FS = ("z", "y")
VMEM = pl.BlockSpec(memory_space=pltpu.VMEM)
ANY = pl.BlockSpec(memory_space=pl.ANY)
SMEM = pl.BlockSpec(memory_space=pltpu.SMEM)
ORDER = tuple(7 * a % 12 * 8 + 3 * b % 8 for a in range(12) for b in range(8))
Y_ORDER = tuple(3 * b % 8 for b in range(8))
Y_PLACE = tuple(Y_ORDER.index(y) for y in range(8))
REACH = 2.0**34
GRAD_REACH = 2.0**10
SMALL = pltpu.CompilerParams(vmem_limit_bytes=16 << 20)


def cost(flops, nbytes):
    return pl.CostEstimate(flops=flops, bytes_accessed=nbytes, transcendentals=0)


LONG = cost(1 << 35, 1 << 26)


def coded(value, reach):
    size = value * reach
    size = size * size
    size = size * size
    return jnp.where(value < 0.0, -size, size).astype(bf16)


def decoded(code, reach):
    wide = code.astype(f32)
    size = lax.rsqrt(lax.rsqrt(jnp.abs(wide))) * (1.0 / reach)
    return jnp.where(wide < 0.0, -size, size)


def send_kernel(left, right, query_master, out_master, out, masters):
    own = query_master.shape[0]
    masters[:own] = coded(query_master[...], REACH)
    masters[own:] = coded(out_master[...], REACH)
    both = jnp.concatenate([left[...].astype(f32), right[...].astype(f32)], axis=1)
    used = both.shape[1]
    free = 128 - used
    kept = out.shape[1]
    rest = both[kept:]
    tail = jnp.concatenate([rest[:, j : j + free] for j in range(0, used, free)], axis=0)
    packed = jnp.concatenate([both[:kept], tail], axis=1).astype(bf16)
    out[...] = jnp.broadcast_to(packed[None], out.shape)


def copies_kernel(packed, out):
    out[...] = jnp.broadcast_to(packed[...][None], out.shape)


def by_place(packed):
    return jnp.concatenate([packed[y, z][None] for z in range(packed.shape[1]) for y in Y_PLACE], axis=0)


def hold_kernel(masters, packed, out):
    pass


def unpacked(packed, used):
    free = 128 - used
    parts = used // free
    height = packed.shape[1] // parts
    wide = packed.astype(f32)
    tail = [wide[:, j * height : (j + 1) * height, used:] for j in range(parts)]
    tail = jnp.concatenate(tail + [jnp.zeros_like(tail[0])], axis=2)
    return jnp.concatenate([wide, tail], axis=1)


def proj_kernel(used, packed, saved_inputs, out_cotangent, out, factors):
    depth = packed.shape[1]
    span = factors.shape[0] // depth
    for z in range(depth):
        block = unpacked(by_place(packed[:, z : z + 1]), used).reshape(span, 128)
        factors[z * span : (z + 1) * span] = block.astype(bf16)
    left = jnp.dot(saved_inputs[...], factors[...], preferred_element_type=f32)
    right = jnp.dot(out_cotangent[...], factors[...], preferred_element_type=f32)
    lane = lax.broadcasted_iota(jnp.int32, left.shape, 1)
    out[...] = jnp.where(lane < used // 2, left, right).T[:used].astype(bf16)


def grad_kernel(rank_cols, proj, query_cotangent, attn_outputs, out):
    cols = query_cotangent.shape[1]
    parts = []
    for k, other in enumerate((query_cotangent, attn_outputs)):
        starts = range(k * rank_cols, proj.shape[0], 2 * rank_cols)
        ranks = jnp.concatenate([proj[at : at + rank_cols] for at in starts], axis=0)
        share = jnp.dot(ranks, other[...], preferred_element_type=f32)
        parts.append(coded(share, GRAD_REACH).astype(f32).reshape(-1, 8, cols))
    first, second = parts
    both = jnp.concatenate([first[:, :4], second[:, :4], first[:, 4:], second[:, 4:]], axis=1)
    both = both.astype(bf16)
    for j, f in enumerate(ORDER):
        out[j] = both[f // 2, f % 2 * 8 : f % 2 * 8 + 8]


def in_three(total):
    parts = []
    for _ in range(3):
        parts.append(total.astype(bf16).astype(f32))
        total = total - parts[-1]
    return parts


def moment_kernel(pieces, first, second, first_new, second_new, low):
    rows = first.shape[1]
    grads = 0.0
    for i in range(pieces.shape[0]):
        grads = grads + decoded(pieces[i], GRAD_REACH)
    new_first = 0.9 * jnp.concatenate([first[0], first[1]], axis=0) + 0.1 * grads
    new_second = 0.99 * jnp.concatenate([second[0], second[1]], axis=0) + 0.01 * grads * grads
    direction = new_first / (jnp.sqrt(new_second) + 1e-08)
    first_new[0] = new_first[:rows]
    first_new[1] = new_first[rows:]
    second_new[0] = new_second[:rows]
    second_new[1] = new_second[rows:]
    squares = direction * direction
    lane = lax.broadcasted_iota(jnp.int32, (rows, 128), 1)
    sums = jnp.zeros((rows, 128), f32)
    for k in range(2):
        total = jnp.sum(squares[k * rows : (k + 1) * rows], axis=(0, 1), keepdims=True)
        for part, value in enumerate(in_three(total)):
            sums = jnp.where(lane == 3 * k + part, value, sums)
    sent = jnp.concatenate([direction[:rows], direction[rows:], sums], axis=1).astype(bf16)
    low[...] = jnp.broadcast_to(sent[None], low.shape)


def prep_kernel(rank_cols, place, held, other, left, right, own_left, own_right, tile):
    own = own_left.shape[0]
    span = left.shape[0]
    chips = held.shape[0]
    blocks = [[unpacked(by_place(half[s]), 2 * rank_cols).reshape(span, 128) for s in range(chips)] for half in (held, other)]
    here = place[1] % 2 == 0
    by_core = [
        [jnp.where(here, near, far) for near, far in zip(blocks[core], blocks[1 - core])] for core in range(2)
    ]
    for chip in range(chips):

        @pl.when(place[1] // 2 == chip)
        def _():
            for k in range(2):
                at = slice(k * rank_cols, (k + 1) * rank_cols)
                side = [by_core[core][(s - chip) % chips][:, at] for s in range(chips) for core in range(2)]
                side = jnp.concatenate(side, axis=1).astype(bf16)
                tile[k] = side
    left[...] = tile[0]
    right[...] = tile[1].T

    @pl.when(pl.program_id(0) == place[0] // (span // own))
    def _():
        rows = pl.ds(pl.multiple_of(place[0] % (span // own) * own, own), own)
        own_left[...] = tile[0, rows]
        own_right[...] = tile[1, rows]


def spread_kernel(low, out):
    depth, _, lanes = low.shape
    lanes = lanes - 128
    sums = jnp.sum(low[:, :, lanes:].astype(f32), axis=0)
    lane = lax.broadcasted_iota(jnp.int32, sums.shape, 1)
    squares = jnp.zeros(sums.shape, f32)
    for k in range(2):
        total = jnp.sum(jnp.where(lane // 3 == k, sums, 0.0)[:1], axis=1, keepdims=True)
        for part, value in enumerate(in_three(total)):
            squares = jnp.where(lane == 3 * k + part, value, squares)
    squares = jnp.concatenate([squares] * (lanes // 128), axis=1).astype(bf16)
    for y in range(out.shape[0]):
        out[y, :depth] = low[:, :, :lanes]
        out[y, depth] = squares


def sums_kernel(low, squares):
    depth = low.shape[1] - 1
    sums = jnp.sum(low[:, depth, :, :128].astype(f32), axis=0)[:1]
    squares[...] = jnp.broadcast_to(sums[None], squares.shape)


def final_kernel(
    entries,
    span,
    squares,
    low,
    left,
    right,
    masters,
    own_left,
    own_right,
    query_master,
    out_master,
    query_copy,
    out_copy,
    query_new,
    out_new,
    near_query,
    near_out,
    near_own,
    near_master,
    near_new,
    first,
    second,
    own_arrived,
    left_for,
    own_left_for,
):
    width = left.shape[0]
    cols = first.shape[1]
    own = query_master.shape[0]
    per = span // own
    parts = width // span
    ways = (
        (own_left, near_own.at[0]),
        (own_right, near_own.at[1]),
        (query_master, near_master.at[0]),
        (out_master, near_master.at[1]),
    )
    own_copies = [pltpu.make_async_copy(x, y, own_arrived.at[k]) for k, (x, y) in enumerate(ways)]
    for copy in own_copies:
        copy.start()

    height = low.shape[0]
    rows = low.shape[2]
    group = 16 // rows
    for g in range(0, first.shape[0] // rows, group):
        part = [low[Y_PLACE[f % height], f // height].astype(f32) for f in range(g, g + group)]
        part = jnp.concatenate(part, axis=0).astype(bf16)
        first[g * rows : (g + group) * rows] = part[:, :cols]
        second[g * rows : (g + group) * rows] = part[:, cols:]
    second_turned = second[...].T

    sums = jnp.sum(squares[...], axis=0)
    lane = lax.broadcasted_iota(jnp.int32, sums.shape, 1)
    scales = []
    for k in range(2):
        total = jnp.sum(jnp.where(lane // 3 == k, sums, 0.0), axis=1, keepdims=True)
        scales.append(0.01 * lax.rsqrt(total / entries + 1e-06))

    sent = []
    for i in range(parts):
        at = pl.ds(i * span, span)
        codes = masters[i * per : (i + 1) * per]
        moved = jnp.dot(left[at], first[...], preferred_element_type=f32)
        kept = decoded(codes[:, :own].reshape(span, cols), REACH)
        near_query[at] = (kept - scales[0] * moved).astype(bf16)
        sent.append(pltpu.make_async_copy(near_query.at[at], query_copy.at[at], left_for.at[i, 0]))
        sent[-1].start()
        moved = jnp.dot(second_turned, right[:, at], preferred_element_type=f32)
        kept = decoded(codes[:, own:].reshape(span, cols).T, REACH)
        near_out[:, at] = (kept - scales[1] * moved).astype(bf16)
        sent.append(pltpu.make_async_copy(near_out.at[:, at], out_copy.at[:, at], left_for.at[i, 1]))
        sent[-1].start()
    for copy in own_copies:
        copy.wait()
    for k, (step, new) in enumerate(((first, query_new), (second, out_new))):
        moved = jnp.dot(near_own[k], step[...], preferred_element_type=f32)
        near_new[k] = near_master[k] - scales[k] * moved
        sent.append(pltpu.make_async_copy(near_new.at[k], new, own_left_for.at[k]))
        sent[-1].start()
    for copy in sent:
        copy.wait()


def far(value):
    return pltpu.with_memory_space_constraint(value, pltpu.HBM)


def body(
    saved_inputs,
    query_cotangent,
    attn_outputs,
    out_cotangent,
    left_factor,
    right_factor,
    query_master,
    out_master,
    first_moment,
    second_moment,
):
    depth = lax.axis_size("z")
    height = lax.axis_size("y")
    fs = depth * height
    tp = lax.axis_size("tp")
    own, rank_cols = left_factor.shape
    rows = first_moment.shape[1]
    cols = first_moment.shape[2]
    tokens = saved_inputs.shape[0]
    width = fs * own
    ranks = tp * rank_cols
    used = 2 * rank_cols
    kept = own * used // 128

    place = jnp.stack([lax.axis_index(FS), lax.axis_index("tp")]).astype(jnp.int32)
    packed, masters = pl.pallas_call(
        send_kernel,
        out_shape=(
            jax.ShapeDtypeStruct((depth, kept, 128), bf16),
            pltpu.HBM((2 * own, cols), bf16),
        ),
        in_specs=[pl.BlockSpec()] * 4,
        out_specs=(VMEM, VMEM),
        compiler_params=SMALL,
        cost_estimate=cost(1 << 16, 1 << 20),
    )(far(left_factor), far(right_factor), far(query_master), far(out_master.T))
    packed = pl.pallas_call(
        hold_kernel,
        out_shape=jax.ShapeDtypeStruct(packed.shape, bf16),
        in_specs=[ANY, ANY],
        out_specs=ANY,
        input_output_aliases={1: 0},
        compiler_params=SMALL,
        cost_estimate=LONG,
    )(far(masters), packed)
    masters = lax.all_gather(masters, FS)
    packed = lax.all_to_all(packed, "z", 0, 0)
    packed = pl.pallas_call(
        copies_kernel,
        out_shape=jax.ShapeDtypeStruct((height, depth, kept, 128), bf16),
        in_specs=[VMEM],
        out_specs=VMEM,
        compiler_params=SMALL,
        cost_estimate=cost(1 << 16, 1 << 20),
    )(packed)
    packed = lax.all_to_all(packed, "y", 0, 0, axis_index_groups=[list(Y_ORDER)])
    proj = pl.pallas_call(
        functools.partial(proj_kernel, used),
        out_shape=jax.ShapeDtypeStruct((used, tokens), bf16),
        in_specs=[VMEM] * 3,
        out_specs=VMEM,
        scratch_shapes=[pltpu.VMEM((width, 128), bf16)],
        compiler_params=SMALL,
        cost_estimate=cost(4 * tokens * width * 128, 8 << 20),
    )(packed, saved_inputs, out_cotangent)
    proj = lax.all_gather(proj, "tp", axis=0, tiled=True)

    partial = pl.pallas_call(
        functools.partial(grad_kernel, rank_cols),
        out_shape=pltpu.HBM((fs, 2 * rows, cols), bf16),
        in_specs=[VMEM] * 3,
        out_specs=VMEM,
        compiler_params=SMALL,
        cost_estimate=cost(4 * ranks * tokens * cols, 2 << 20),
    )(proj, query_cotangent, attn_outputs)
    pieces = lax.all_to_all(partial, FS, 0, 0, axis_index_groups=[list(ORDER)])

    held = [packed]
    for step in range(1, tp // 2):
        held.append(lax.ppermute(packed, "tp", [((t + 2 * step) % tp, t) for t in range(tp)]))
    held = jnp.stack(held)
    other = lax.ppermute(held, "tp", [(t ^ 1, t) for t in range(tp)])

    first_new, second_new, low = pl.pallas_call(
        moment_kernel,
        out_shape=(
            jax.ShapeDtypeStruct(first_moment.shape, f32),
            jax.ShapeDtypeStruct(second_moment.shape, f32),
            pltpu.HBM((depth, rows, 2 * cols + 128), bf16),
        ),
        in_specs=[VMEM] * 3,
        out_specs=(VMEM, VMEM, VMEM),
        compiler_params=SMALL,
        cost_estimate=cost(1 << 20, 2 << 20),
    )(pieces, first_moment, second_moment)
    low = lax.all_to_all(low, "z", 0, 0)
    low = pl.pallas_call(
        spread_kernel,
        out_shape=pltpu.HBM((height, depth + 1, rows, 2 * cols), bf16),
        in_specs=[VMEM],
        out_specs=VMEM,
        compiler_params=SMALL,
        cost_estimate=cost(1 << 16, 1 << 20),
    )(low)
    low = lax.all_to_all(low, "y", 0, 0, axis_index_groups=[list(Y_ORDER)])

    span = width // 4
    per = span // own
    left, right, own_left, own_right = pl.pallas_call(
        functools.partial(prep_kernel, rank_cols),
        grid=(width // span,),
        out_shape=(
            pltpu.HBM((width, ranks), bf16),
            pltpu.HBM((ranks, width), bf16),
            pltpu.HBM((own, ranks), bf16),
            pltpu.HBM((own, ranks), bf16),
        ),
        in_specs=[
            SMEM,
            pl.BlockSpec((tp // 2, height, per // height, kept, 128), lambda i: (0, 0, i, 0, 0)),
            pl.BlockSpec((tp // 2, height, per // height, kept, 128), lambda i: (0, 0, i, 0, 0)),
        ],
        out_specs=(
            pl.BlockSpec((span, ranks), lambda i: (i, 0)),
            pl.BlockSpec((ranks, span), lambda i: (0, i)),
            pl.BlockSpec((own, ranks), lambda i: (0, 0)),
            pl.BlockSpec((own, ranks), lambda i: (0, 0)),
        ),
        scratch_shapes=[pltpu.VMEM((2, span, ranks), bf16)],
        compiler_params=SMALL,
        cost_estimate=cost(1 << 30, 30 << 20),
    )(place, far(held), far(other))

    low, masters = lax.optimization_barrier((low, masters))
    parts = width // span
    squares = pl.pallas_call(
        sums_kernel,
        out_shape=jax.ShapeDtypeStruct((tp, 1, 128), f32),
        in_specs=[VMEM],
        out_specs=VMEM,
        compiler_params=SMALL,
        cost_estimate=LONG,
    )(low)
    squares = lax.all_to_all(squares, "tp", 0, 0)

    query_copy, out_copy, query_new, out_new = pl.pallas_call(
        functools.partial(final_kernel, float(rows * fs * cols * tp), span),
        out_shape=(
            pltpu.HBM((width, cols), bf16),
            pltpu.HBM((cols, width), bf16),
            pltpu.HBM((own, cols), f32),
            pltpu.HBM((own, cols), f32),
        ),
        in_specs=[VMEM] * 5 + [ANY] * 4,
        out_specs=(ANY,) * 4,
        scratch_shapes=[
            pltpu.VMEM((width, cols), bf16),
            pltpu.VMEM((cols, width), bf16),
            pltpu.VMEM((2, own, ranks), bf16),
            pltpu.VMEM((2, own, cols), f32),
            pltpu.VMEM((2, own, cols), f32),
            pltpu.VMEM((ranks, cols), bf16),
            pltpu.VMEM((ranks, cols), bf16),
            pltpu.SemaphoreType.DMA((4,)),
            pltpu.SemaphoreType.DMA((parts, 2)),
            pltpu.SemaphoreType.DMA((2,)),
        ],
        compiler_params=SMALL,
        cost_estimate=cost(4 * width * ranks * cols, 20 << 20),
    )(
        squares,
        low,
        left,
        right,
        masters,
        far(own_left),
        far(own_right),
        far(query_master),
        far(out_master.T),
    )
    return (query_new, out_new.T, query_copy, out_copy, first_new, second_new)


def solution(mesh):
    finer = Mesh(mesh.devices.reshape(12, 8, 8), ("z", "y", "tp"))
    both = P(FS, "tp")
    moment = P(None, FS, "tp")

    return jax.shard_map(
        body,
        mesh=finer,
        in_specs=(P(FS, None), both, both, P(FS, None), both, both, both, P("tp", FS), moment, moment),
        out_specs=(both, P("tp", FS), P(None, "tp"), P("tp", None), moment, moment),
        check_vma=False,
    )
```

```python
import functools

import jax
import jax.numpy as jnp
from jax import lax
from jax.experimental import pallas as pl
from jax.experimental.pallas import tpu as pltpu
from jax.sharding import Mesh
from jax.sharding import PartitionSpec as P


bf16 = jnp.bfloat16
f32 = jnp.float32
FS = ("z", "y")
VMEM = pl.BlockSpec(memory_space=pltpu.VMEM)
ANY = pl.BlockSpec(memory_space=pl.ANY)
SMEM = pl.BlockSpec(memory_space=pltpu.SMEM)
ORDER = tuple(7 * a % 12 * 8 + (3 * b + 5 * a) % 8 for b in range(8) for a in range(12))
Y_ORDER = tuple(3 * b % 8 for b in range(8))
Y_PLACE = tuple(Y_ORDER.index(y) for y in range(8))
Z_ORDER = tuple(7 * a % 12 for a in range(12))
Z_PLACE = tuple(Z_ORDER.index(z) for z in range(12))
REACH = 2.0**34
GRAD_REACH = 2.0**10
SMALL = pltpu.CompilerParams(vmem_limit_bytes=16 << 20)


def cost(flops, nbytes):
    return pl.CostEstimate(flops=flops, bytes_accessed=nbytes, transcendentals=0)


LONG = cost(1 << 35, 1 << 26)


def coded(value, reach):
    size = value * reach
    size = size * size
    size = size * size
    return jnp.where(value < 0.0, -size, size).astype(bf16)


def decoded(code, reach):
    wide = code.astype(f32)
    size = lax.rsqrt(lax.rsqrt(jnp.abs(wide))) * (1.0 / reach)
    return jnp.where(wide < 0.0, -size, size)


def send_kernel(left, right, query_master, out_master, out, masters):
    own = query_master.shape[0]
    masters[:own] = coded(query_master[...], REACH)
    masters[own:] = coded(out_master[...], REACH)
    both = jnp.concatenate([left[...].astype(f32), right[...].astype(f32)], axis=1)
    used = both.shape[1]
    free = 128 - used
    kept = out.shape[1]
    rest = both[kept:]
    tail = jnp.concatenate([rest[:, j : j + free] for j in range(0, used, free)], axis=0)
    packed = jnp.concatenate([both[:kept], tail], axis=1).astype(bf16)
    out[...] = jnp.broadcast_to(packed[None], out.shape)


def copies_kernel(packed, out):
    out[...] = jnp.broadcast_to(packed[...][None], out.shape)


def by_place(packed):
    return jnp.concatenate([packed[y, z][None] for z in range(packed.shape[1]) for y in Y_PLACE], axis=0)


def hold_kernel(masters, packed, out):
    pass


def unpacked(packed, used):
    free = 128 - used
    parts = used // free
    height = packed.shape[1] // parts
    wide = packed.astype(f32)
    tail = [wide[:, j * height : (j + 1) * height, used:] for j in range(parts)]
    tail = jnp.concatenate(tail + [jnp.zeros_like(tail[0])], axis=2)
    return jnp.concatenate([wide, tail], axis=1)


def proj_kernel(used, packed, saved_inputs, out_cotangent, out, factors):
    depth = packed.shape[1]
    span = factors.shape[0] // depth
    for z in range(depth):
        block = unpacked(by_place(packed[:, z : z + 1]), used).reshape(span, 128)
        factors[z * span : (z + 1) * span] = block.astype(bf16)
    left = jnp.dot(saved_inputs[...], factors[...], preferred_element_type=f32)
    right = jnp.dot(out_cotangent[...], factors[...], preferred_element_type=f32)
    lane = lax.broadcasted_iota(jnp.int32, left.shape, 1)
    out[...] = jnp.where(lane < used // 2, left, right).T[:used].astype(bf16)


def grad_kernel(rank_cols, proj, query_cotangent, attn_outputs, out):
    cols = query_cotangent.shape[1]
    parts = []
    for k, other in enumerate((query_cotangent, attn_outputs)):
        starts = range(k * rank_cols, proj.shape[0], 2 * rank_cols)
        ranks = jnp.concatenate([proj[at : at + rank_cols] for at in starts], axis=0)
        share = jnp.dot(ranks, other[...], preferred_element_type=f32)
        parts.append(coded(share, GRAD_REACH).astype(f32).reshape(-1, 8, cols))
    first, second = parts
    both = jnp.concatenate([first[:, :4], second[:, :4], first[:, 4:], second[:, 4:]], axis=1)
    both = both.astype(bf16)
    for j, f in enumerate(ORDER):
        out[j] = both[f // 2, f % 2 * 8 : f % 2 * 8 + 8]


def in_three(total):
    parts = []
    for _ in range(3):
        parts.append(total.astype(bf16).astype(f32))
        total = total - parts[-1]
    return parts


def moment_kernel(pieces, first, second, first_new, second_new, low):
    rows = first.shape[1]
    grads = 0.0
    for i in range(pieces.shape[0]):
        grads = grads + decoded(pieces[i], GRAD_REACH)
    new_first = 0.9 * jnp.concatenate([first[0], first[1]], axis=0) + 0.1 * grads
    new_second = 0.99 * jnp.concatenate([second[0], second[1]], axis=0) + 0.01 * grads * grads
    direction = new_first / (jnp.sqrt(new_second) + 1e-08)
    first_new[0] = new_first[:rows]
    first_new[1] = new_first[rows:]
    second_new[0] = new_second[:rows]
    second_new[1] = new_second[rows:]
    squares = direction * direction
    lane = lax.broadcasted_iota(jnp.int32, (rows, 128), 1)
    sums = jnp.zeros((rows, 128), f32)
    for k in range(2):
        total = jnp.sum(squares[k * rows : (k + 1) * rows], axis=(0, 1), keepdims=True)
        for part, value in enumerate(in_three(total)):
            sums = jnp.where(lane == 3 * k + part, value, sums)
    sent = jnp.concatenate([direction[:rows], direction[rows:], sums], axis=1).astype(bf16)
    low[...] = jnp.broadcast_to(sent[None], low.shape)


def prep_kernel(rank_cols, place, held, other, left, right, own_left, own_right, tile):
    own = own_left.shape[0]
    span = left.shape[0]
    chips = held.shape[0]
    blocks = [[unpacked(by_place(half[s]), 2 * rank_cols).reshape(span, 128) for s in range(chips)] for half in (held, other)]
    here = place[1] % 2 == 0
    by_core = [
        [jnp.where(here, near, far) for near, far in zip(blocks[core], blocks[1 - core])] for core in range(2)
    ]
    for chip in range(chips):

        @pl.when(place[1] // 2 == chip)
        def _():
            for k in range(2):
                at = slice(k * rank_cols, (k + 1) * rank_cols)
                side = [by_core[core][(s - chip) % chips][:, at] for s in range(chips) for core in range(2)]
                side = jnp.concatenate(side, axis=1).astype(bf16)
                tile[k] = side
    left[...] = tile[0]
    right[...] = tile[1].T

    @pl.when(pl.program_id(0) == place[0] // (span // own))
    def _():
        rows = pl.ds(pl.multiple_of(place[0] % (span // own) * own, own), own)
        own_left[...] = tile[0, rows]
        own_right[...] = tile[1, rows]


def spread_kernel(low, out):
    depth, _, lanes = low.shape
    lanes = lanes - 128
    sums = jnp.sum(low[:, :, lanes:].astype(f32), axis=0)
    lane = lax.broadcasted_iota(jnp.int32, sums.shape, 1)
    squares = jnp.zeros(sums.shape, f32)
    for k in range(2):
        total = jnp.sum(jnp.where(lane // 3 == k, sums, 0.0)[:1], axis=1, keepdims=True)
        for part, value in enumerate(in_three(total)):
            squares = jnp.where(lane == 3 * k + part, value, squares)
    squares = jnp.concatenate([squares] * (lanes // 128), axis=1).astype(bf16)
    for y in range(out.shape[0]):
        out[y, :depth] = low[:, :, :lanes]
        out[y, depth] = squares


def sums_kernel(low, squares):
    depth = low.shape[1] - 1
    sums = jnp.sum(low[:, depth, :, :128].astype(f32), axis=0)[:1]
    squares[...] = jnp.broadcast_to(sums[None], squares.shape)


def final_kernel(
    entries,
    span,
    squares,
    low,
    left,
    right,
    masters,
    own_left,
    own_right,
    query_master,
    out_master,
    query_copy,
    out_copy,
    query_new,
    out_new,
    near_query,
    near_out,
    near_own,
    near_master,
    near_new,
    first,
    second,
    own_arrived,
    left_for,
    own_left_for,
):
    width = left.shape[0]
    cols = first.shape[1]
    own = query_master.shape[0]
    per = span // own
    parts = width // span
    ways = (
        (own_left, near_own.at[0]),
        (own_right, near_own.at[1]),
        (query_master, near_master.at[0]),
        (out_master, near_master.at[1]),
    )
    own_copies = [pltpu.make_async_copy(x, y, own_arrived.at[k]) for k, (x, y) in enumerate(ways)]
    for copy in own_copies:
        copy.start()

    height = low.shape[0]
    rows = low.shape[2]
    group = 16 // rows
    for g in range(0, first.shape[0] // rows, group):
        part = [low[Y_PLACE[f % height], Z_PLACE[f // height]].astype(f32) for f in range(g, g + group)]
        part = jnp.concatenate(part, axis=0).astype(bf16)
        first[g * rows : (g + group) * rows] = part[:, :cols]
        second[g * rows : (g + group) * rows] = part[:, cols:]
    second_turned = second[...].T

    sums = jnp.sum(squares[...], axis=0)
    lane = lax.broadcasted_iota(jnp.int32, sums.shape, 1)
    scales = []
    for k in range(2):
        total = jnp.sum(jnp.where(lane // 3 == k, sums, 0.0), axis=1, keepdims=True)
        scales.append(0.01 * lax.rsqrt(total / entries + 1e-06))

    sent = []
    for i in range(parts):
        at = pl.ds(i * span, span)
        codes = masters[i * per : (i + 1) * per]
        moved = jnp.dot(left[at], first[...], preferred_element_type=f32)
        kept = decoded(codes[:, :own].reshape(span, cols), REACH)
        near_query[at] = (kept - scales[0] * moved).astype(bf16)
        sent.append(pltpu.make_async_copy(near_query.at[at], query_copy.at[at], left_for.at[i, 0]))
        sent[-1].start()
        moved = jnp.dot(second_turned, right[:, at], preferred_element_type=f32)
        kept = decoded(codes[:, own:].reshape(span, cols).T, REACH)
        near_out[:, at] = (kept - scales[1] * moved).astype(bf16)
        sent.append(pltpu.make_async_copy(near_out.at[:, at], out_copy.at[:, at], left_for.at[i, 1]))
        sent[-1].start()
    for copy in own_copies:
        copy.wait()
    for k, (step, new) in enumerate(((first, query_new), (second, out_new))):
        moved = jnp.dot(near_own[k], step[...], preferred_element_type=f32)
        near_new[k] = near_master[k] - scales[k] * moved
        sent.append(pltpu.make_async_copy(near_new.at[k], new, own_left_for.at[k]))
        sent[-1].start()
    for copy in sent:
        copy.wait()


def far(value):
    return pltpu.with_memory_space_constraint(value, pltpu.HBM)


def body(
    saved_inputs,
    query_cotangent,
    attn_outputs,
    out_cotangent,
    left_factor,
    right_factor,
    query_master,
    out_master,
    first_moment,
    second_moment,
):
    depth = lax.axis_size("z")
    height = lax.axis_size("y")
    fs = depth * height
    tp = lax.axis_size("tp")
    own, rank_cols = left_factor.shape
    rows = first_moment.shape[1]
    cols = first_moment.shape[2]
    tokens = saved_inputs.shape[0]
    width = fs * own
    ranks = tp * rank_cols
    used = 2 * rank_cols
    kept = own * used // 128

    place = jnp.stack([lax.axis_index(FS), lax.axis_index("tp")]).astype(jnp.int32)
    packed, masters = pl.pallas_call(
        send_kernel,
        out_shape=(
            jax.ShapeDtypeStruct((depth, kept, 128), bf16),
            pltpu.HBM((2 * own, cols), bf16),
        ),
        in_specs=[pl.BlockSpec()] * 4,
        out_specs=(VMEM, VMEM),
        compiler_params=SMALL,
        cost_estimate=cost(1 << 16, 1 << 20),
    )(far(left_factor), far(right_factor), far(query_master), far(out_master.T))
    packed = pl.pallas_call(
        hold_kernel,
        out_shape=jax.ShapeDtypeStruct(packed.shape, bf16),
        in_specs=[ANY, ANY],
        out_specs=ANY,
        input_output_aliases={1: 0},
        compiler_params=SMALL,
        cost_estimate=LONG,
    )(far(masters), packed)
    masters = lax.all_gather(masters, FS)
    packed = lax.all_to_all(packed, "z", 0, 0)
    packed = pl.pallas_call(
        copies_kernel,
        out_shape=jax.ShapeDtypeStruct((height, depth, kept, 128), bf16),
        in_specs=[VMEM],
        out_specs=VMEM,
        compiler_params=SMALL,
        cost_estimate=cost(1 << 16, 1 << 20),
    )(packed)
    packed = lax.all_to_all(packed, "y", 0, 0, axis_index_groups=[list(Y_ORDER)])
    proj = pl.pallas_call(
        functools.partial(proj_kernel, used),
        out_shape=jax.ShapeDtypeStruct((used, tokens), bf16),
        in_specs=[VMEM] * 3,
        out_specs=VMEM,
        scratch_shapes=[pltpu.VMEM((width, 128), bf16)],
        compiler_params=SMALL,
        cost_estimate=cost(4 * tokens * width * 128, 8 << 20),
    )(packed, saved_inputs, out_cotangent)
    proj = lax.all_gather(proj, "tp", axis=0, tiled=True)

    partial = pl.pallas_call(
        functools.partial(grad_kernel, rank_cols),
        out_shape=pltpu.HBM((fs, 2 * rows, cols), bf16),
        in_specs=[VMEM] * 3,
        out_specs=VMEM,
        compiler_params=SMALL,
        cost_estimate=cost(4 * ranks * tokens * cols, 2 << 20),
    )(proj, query_cotangent, attn_outputs)
    pieces = lax.all_to_all(partial, FS, 0, 0, axis_index_groups=[list(ORDER)])

    held = [packed]
    for step in range(1, tp // 2):
        held.append(lax.ppermute(packed, "tp", [((t + 2 * step) % tp, t) for t in range(tp)]))
    held = jnp.stack(held)
    other = lax.ppermute(held, "tp", [(t ^ 1, t) for t in range(tp)])

    first_new, second_new, low = pl.pallas_call(
        moment_kernel,
        out_shape=(
            jax.ShapeDtypeStruct(first_moment.shape, f32),
            jax.ShapeDtypeStruct(second_moment.shape, f32),
            pltpu.HBM((depth, rows, 2 * cols + 128), bf16),
        ),
        in_specs=[VMEM] * 3,
        out_specs=(VMEM, VMEM, VMEM),
        compiler_params=SMALL,
        cost_estimate=cost(1 << 20, 2 << 20),
    )(pieces, first_moment, second_moment)
    low = lax.all_to_all(low, "z", 0, 0, axis_index_groups=[list(Z_ORDER)])
    low = pl.pallas_call(
        spread_kernel,
        out_shape=pltpu.HBM((height, depth + 1, rows, 2 * cols), bf16),
        in_specs=[VMEM],
        out_specs=VMEM,
        compiler_params=SMALL,
        cost_estimate=cost(1 << 16, 1 << 20),
    )(low)
    low = lax.all_to_all(low, "y", 0, 0, axis_index_groups=[list(Y_ORDER)])

    span = width // 4
    per = span // own
    left, right, own_left, own_right = pl.pallas_call(
        functools.partial(prep_kernel, rank_cols),
        grid=(width // span,),
        out_shape=(
            pltpu.HBM((width, ranks), bf16),
            pltpu.HBM((ranks, width), bf16),
            pltpu.HBM((own, ranks), bf16),
            pltpu.HBM((own, ranks), bf16),
        ),
        in_specs=[
            SMEM,
            pl.BlockSpec((tp // 2, height, per // height, kept, 128), lambda i: (0, 0, i, 0, 0)),
            pl.BlockSpec((tp // 2, height, per // height, kept, 128), lambda i: (0, 0, i, 0, 0)),
        ],
        out_specs=(
            pl.BlockSpec((span, ranks), lambda i: (i, 0)),
            pl.BlockSpec((ranks, span), lambda i: (0, i)),
            pl.BlockSpec((own, ranks), lambda i: (0, 0)),
            pl.BlockSpec((own, ranks), lambda i: (0, 0)),
        ),
        scratch_shapes=[pltpu.VMEM((2, span, ranks), bf16)],
        compiler_params=SMALL,
        cost_estimate=cost(1 << 30, 30 << 20),
    )(place, far(held), far(other))

    low, masters = lax.optimization_barrier((low, masters))
    parts = width // span
    squares = pl.pallas_call(
        sums_kernel,
        out_shape=jax.ShapeDtypeStruct((tp, 1, 128), f32),
        in_specs=[VMEM],
        out_specs=VMEM,
        compiler_params=SMALL,
        cost_estimate=LONG,
    )(low)
    squares = lax.all_to_all(squares, "tp", 0, 0)

    query_copy, out_copy, query_new, out_new = pl.pallas_call(
        functools.partial(final_kernel, float(rows * fs * cols * tp), span),
        out_shape=(
            pltpu.HBM((width, cols), bf16),
            pltpu.HBM((cols, width), bf16),
            pltpu.HBM((own, cols), f32),
            pltpu.HBM((own, cols), f32),
        ),
        in_specs=[VMEM] * 5 + [ANY] * 4,
        out_specs=(ANY,) * 4,
        scratch_shapes=[
            pltpu.VMEM((width, cols), bf16),
            pltpu.VMEM((cols, width), bf16),
            pltpu.VMEM((2, own, ranks), bf16),
            pltpu.VMEM((2, own, cols), f32),
            pltpu.VMEM((2, own, cols), f32),
            pltpu.VMEM((ranks, cols), bf16),
            pltpu.VMEM((ranks, cols), bf16),
            pltpu.SemaphoreType.DMA((4,)),
            pltpu.SemaphoreType.DMA((parts, 2)),
            pltpu.SemaphoreType.DMA((2,)),
        ],
        compiler_params=SMALL,
        cost_estimate=cost(4 * width * ranks * cols, 20 << 20),
    )(
        squares,
        low,
        left,
        right,
        masters,
        far(own_left),
        far(own_right),
        far(query_master),
        far(out_master.T),
    )
    return (query_new, out_new.T, query_copy, out_copy, first_new, second_new)


def solution(mesh):
    finer = Mesh(mesh.devices.reshape(12, 8, 8), ("z", "y", "tp"))
    both = P(FS, "tp")
    moment = P(None, FS, "tp")

    return jax.shard_map(
        body,
        mesh=finer,
        in_specs=(P(FS, None), both, both, P(FS, None), both, both, both, P("tp", FS), moment, moment),
        out_specs=(both, P("tp", FS), P(None, "tp"), P("tp", None), moment, moment),
        check_vma=False,
    )
```
